32 devices in a mesh: sp: 8 (over z, y), tp: 4 (over x, core).
Axes of the slice: x: 2, y: 2, z: 4, core: 2. Of those that a mesh axis runs over, the one named last changes fastest.
Arguments:
- residual: bfloat16 [8192, 2048], P(('sp', 'tp')), may hold values from -6 to 6
- first_group_queries: bfloat16 [8192, 1024], P('sp', 'tp'), may hold values from -6 to 6
- first_group_keys: bfloat16 [8192, 1024], P('sp', 'tp'), may hold values from -6 to 6
- second_group_queries: bfloat16 [8192, 512], P('sp', 'tp'), may hold values from -6 to 6
- second_group_keys: bfloat16 [8192, 512], P('sp', 'tp'), may hold values from -6 to 6
- primary_retain_switch_inputs: bfloat16 [8192, 1024], P('sp', 'tp'), may hold values from -12 to 16
- secondary_retain_switch_inputs: bfloat16 [8192, 512], P('sp', 'tp'), may hold values from -12 to 16
- timestep_fading_exponent: float32 [8192], P('sp'), may hold values from -2.1 to 0
- values: bfloat16 [2, 8192, 1024], P(None, 'sp', 'tp'), may hold values from -6 to 6
- output_gate_logits: bfloat16 [2, 8192, 1024], P(None, 'sp', 'tp'), may hold values from -6 to 6
- head_norm_gains: float32 [2, 1024], P(None, 'tp'), may hold values from 0.1 to 1.9
- output_projection: bfloat16 [2, 1024, 2048], P(None, 'tp'), may hold values from -0.125 to 0.125
- feedforward_norm_gain: float32 [2048], replicated, may hold values from 0.1 to 1.9
- gate_projection: bfloat16 [2048, 6144], P('sp', 'tp'), may hold values from -0.125 to 0.125
- up_projection: bfloat16 [2048, 6144], P('sp', 'tp'), may hold values from -0.125 to 0.125
- down_projection: bfloat16 [6144, 2048], P('tp', 'sp'), may hold values from -0.078125 to 0.078125
Outputs:
- layer_out: bfloat16 [8192, 2048], P(('sp', 'tp'))
The draws below stay inside these ranges and needn't reach their ends.
All inputs are finite; a program needn't handle non-finite values.
Results may differ from the reference program's by a relative error of at most 0.018.
Values may be sent and summed in bfloat16 or wider, within the bound.
A program may use at most 128 MiB of HBM per device.

```python
import jax
import jax.numpy as jnp
from jax import lax

D = 2048
HEADS = 8
FIRST_KEY_SIZE = 128
SECOND_KEY_SIZE = 64
DV = 128
FF = 6144
BLOCK = 64
SEQ = 8192
N_TP = 4


def forget_draw(base_key, key_width):
    key_rank, key_factor, key_channel, key_jitter, key_long, key_level = jax.random.split(base_key, 6)
    ranking = jax.random.permutation(key_rank, HEADS)
    fast_count = HEADS // 2
    long_share = 0.5
    fast_mask = jnp.repeat((ranking < fast_count).astype(jnp.float32), key_width)
    slow_level = jnp.log(SEQ / 3.2)
    fast_level = -jnp.log(jnp.exp(16.0 / (0.6 * BLOCK)) - 1.0)
    long_mask = (jax.random.uniform(key_long, (HEADS * key_width,), jnp.float32) < long_share).astype(jnp.float32)
    spread_level = jax.random.uniform(key_level, (HEADS * key_width,), jnp.float32, jnp.log(4.0), slow_level)
    slow_channel = long_mask * slow_level + (1.0 - long_mask) * spread_level
    base_level = fast_mask * fast_level + (1.0 - fast_mask) * slow_channel
    factor = jax.random.uniform(key_factor, (SEQ // BLOCK, 1), jnp.float32, 0.0, jnp.log(4.0))
    factor = jnp.repeat(factor, BLOCK, axis=0)
    channel = jnp.clip(0.5 * jax.random.normal(key_channel, (1, HEADS * key_width), jnp.float32), -1.5, 1.5)
    jitter = jnp.clip(0.8 * jax.random.normal(key_jitter, (SEQ, HEADS * key_width), jnp.float32), -3.2, 3.2)
    result = base_level[None, :] - factor + channel + jitter
    return result.astype(jnp.bfloat16)


def draw_primary_retain_switch_inputs(key, part):
    return forget_draw(jax.random.fold_in(key, 11), FIRST_KEY_SIZE)


def draw_secondary_retain_switch_inputs(key, part):
    return forget_draw(jax.random.fold_in(key, 23), SECOND_KEY_SIZE)


def draw_timestep_fading_exponent(key, part):
    key_spot, key_loss = jax.random.split(jax.random.fold_in(key, 37))
    positions = jax.random.randint(key_spot, (3,), 0, SEQ)
    losses = jax.random.uniform(key_loss, (3,), jnp.float32, jnp.log(0.5), jnp.log(0.8))
    hits = jnp.arange(SEQ)[:, None] == positions[None, :]
    return jnp.sum(jnp.where(hits, losses[None, :], 0.0), axis=1).astype(jnp.float32)


def block_scale(stream_key, dims, shards, smallest, top_value):
    factor_of = 1.0
    for dim, shards_of in shards:
        draws = jax.random.uniform(jax.random.fold_in(jax.random.fold_in(stream_key, 6), dim), (shards_of,), jnp.float32, smallest / len(shards), top_value / len(shards))
        factor_of = factor_of * jnp.repeat(jnp.exp(draws), dims[dim] // shards_of).reshape((-1,) + (1,) * (len(dims) - 1 - dim))
    return factor_of


def scatter_about(key, shape, scale, limit, pieces=(), kind=jnp.bfloat16):
    entries = scale * jax.random.normal(key, shape, jnp.float32)
    if pieces:
        entries = entries * block_scale(key, shape, pieces, -0.22, 0.18)
    return jnp.clip(entries, -limit, limit).astype(kind)


def setup_inputs(seed: int = 0) -> dict:
    streams_of = jax.random.split(jax.random.key(seed), 17)
    return {
        "residual": scatter_about(streams_of[0], (SEQ, D), 1.0, 6.0, ((0, 32),)),
        "first_group_queries": scatter_about(streams_of[1], (SEQ, HEADS * FIRST_KEY_SIZE), 1.0, 6.0, ((0, 8), (1, 4))),
        "first_group_keys": scatter_about(streams_of[2], (SEQ, HEADS * FIRST_KEY_SIZE), 1.0, 6.0, ((0, 8), (1, 4))),
        "second_group_queries": scatter_about(streams_of[3], (SEQ, HEADS * SECOND_KEY_SIZE), 1.0, 6.0, ((0, 8), (1, 4))),
        "second_group_keys": scatter_about(streams_of[4], (SEQ, HEADS * SECOND_KEY_SIZE), 1.0, 6.0, ((0, 8), (1, 4))),
        "primary_retain_switch_inputs": draw_primary_retain_switch_inputs(jax.random.fold_in(streams_of[16], 71), 0),
        "secondary_retain_switch_inputs": draw_secondary_retain_switch_inputs(jax.random.fold_in(streams_of[16], 71), 0),
        "timestep_fading_exponent": draw_timestep_fading_exponent(jax.random.fold_in(streams_of[16], 71), 0),
        "values": scatter_about(streams_of[8], (2, SEQ, HEADS * DV), 1.0, 6.0, ((1, 8), (2, 4))),
        "output_gate_logits": scatter_about(streams_of[9], (2, SEQ, HEADS * DV), 1.0, 6.0, ((1, 8), (2, 4))),
        "head_norm_gains": jnp.clip(1.0 + 0.18 * jax.random.normal(streams_of[10], (2, HEADS * DV), jnp.float32), 0.1, 1.9),
        "output_projection": scatter_about(streams_of[11], (2, HEADS * DV, D), (2 * HEADS * DV) ** -0.5, 0.125, ((1, 4),)),
        "feedforward_norm_gain": jnp.clip(1.0 + 0.18 * jax.random.normal(streams_of[12], (D,), jnp.float32), 0.1, 1.9),
        "gate_projection": scatter_about(streams_of[13], (D, FF), D ** -0.5, 0.125, ((0, 8), (1, 4))),
        "up_projection": scatter_about(streams_of[14], (D, FF), D ** -0.5, 0.125, ((0, 8), (1, 4))),
        "down_projection": scatter_about(streams_of[15], (FF, D), FF ** -0.5, 0.078125, ((0, 4), (1, 8))),
    }


EPS = 1e-06
SOFTNESS_SCALE = 16.0
highest_precision = lax.Precision.HIGHEST

def blocks(source, block_count, head_count, key_width):
    return source.astype(jnp.float32).reshape(block_count, BLOCK, head_count, key_width).transpose(0, 2, 1, 3)

def mechanism(query_matrix_rows, key_matrix_rows, value_matrix_rows, decay_logarithm, key_width):
    block_count = query_matrix_rows.shape[0] // BLOCK
    query_blocks = blocks(query_matrix_rows, block_count, HEADS, key_width) * key_width ** (-0.5)
    key_blocks = blocks(key_matrix_rows, block_count, HEADS, key_width)
    value_blocks = blocks(value_matrix_rows, block_count, HEADS, DV)
    decay_blocks = jnp.cumsum(blocks(decay_logarithm, block_count, HEADS, key_width), axis=2)
    causal = jnp.tril(jnp.ones((BLOCK, BLOCK), dtype=bool))

    def advance(running_state, inputs):
        query_piece, key_piece, value_piece, decay_piece = inputs
        spread_log = decay_piece[:, :, None, :] - decay_piece[:, None, :, :]
        decay_grid = jnp.exp(jnp.where(causal[None, :, :, None], spread_log, -jnp.inf))
        scores = lax.optimization_barrier(jnp.sum(query_piece[:, :, None, :] * key_piece[:, None, :, :] * decay_grid, axis=-1))
        block_result = jnp.einsum('hij,hjv->hiv', scores, value_piece, precision=highest_precision)
        block_result = block_result + jnp.einsum('rus,rsp->rup', query_piece * jnp.exp(decay_piece), running_state, precision=highest_precision)
        final_log_decay = decay_piece[:, -1:, :]
        running_state = jnp.exp(final_log_decay[:, 0, :])[:, :, None] * running_state + jnp.einsum('qxe,qxt->qet', key_piece * jnp.exp(final_log_decay - decay_piece), value_piece, precision=highest_precision)
        return (running_state, block_result)
    zero_state = jnp.zeros((HEADS, key_width, DV), jnp.float32)
    _, outputs = lax.scan(advance, zero_state, (query_blocks, key_blocks, value_blocks, decay_blocks))
    return outputs.transpose(0, 2, 1, 3).reshape(query_matrix_rows.shape[0], HEADS, DV)

def gate_heads(head_out, gate_rows, gain_row):
    inverse = lax.rsqrt(lax.optimization_barrier(jnp.mean(head_out * head_out, axis=-1, keepdims=True)) + EPS)
    normed = (head_out * inverse).reshape(head_out.shape[0], -1) * gain_row
    return (jax.nn.silu(gate_rows.astype(jnp.float32)) * normed).astype(jnp.bfloat16)

def grouped_product(left_sides, right_sides):
    portion = left_sides[0].shape[1] // N_TP
    row_count = left_sides[0].shape[0]
    col_count = right_sides[0].shape[1]

    def add_group(group_index, summed):
        offset = (group_index * portion).astype(jnp.int32)
        partial_value = jnp.zeros((row_count, col_count), jnp.float32)
        for left_side, right_side in zip(left_sides, right_sides):
            partial_value = partial_value + jnp.dot(lax.dynamic_slice_in_dim(left_side, offset, portion, 1), lax.dynamic_slice_in_dim(right_side, offset, portion, 0), preferred_element_type=jnp.float32)
        rounded = lax.optimization_barrier(partial_value.astype(jnp.bfloat16))
        return summed + rounded.astype(jnp.float32)
    return lax.fori_loop(0, N_TP, add_group, jnp.zeros((row_count, col_count), jnp.float32))

def row_norm(source, gain_row):
    widened = source.astype(jnp.float32)
    inverse = lax.rsqrt(lax.optimization_barrier(jnp.mean(widened * widened, axis=-1, keepdims=True)) + EPS)
    return (widened * inverse * gain_row).astype(jnp.bfloat16)

def reference(residual, first_group_queries, first_group_keys, second_group_queries, second_group_keys, primary_retain_switch_inputs, secondary_retain_switch_inputs, timestep_fading_exponent, values, output_gate_logits, head_norm_gains, output_projection, feedforward_norm_gain, gate_projection, up_projection, down_projection):
    primary_fading_exponent = jax.nn.log_sigmoid(primary_retain_switch_inputs.astype(jnp.float32)) / SOFTNESS_SCALE + timestep_fading_exponent[:, None]
    secondary_fading_exponent = jax.nn.log_sigmoid(secondary_retain_switch_inputs.astype(jnp.float32)) / SOFTNESS_SCALE + timestep_fading_exponent[:, None]
    heads_a = mechanism(first_group_queries, first_group_keys, values[0], primary_fading_exponent, FIRST_KEY_SIZE)
    heads_b = mechanism(second_group_queries, second_group_keys, values[1], secondary_fading_exponent, SECOND_KEY_SIZE)
    gated_a = gate_heads(heads_a, output_gate_logits[0], head_norm_gains[0])
    gated_b = gate_heads(heads_b, output_gate_logits[1], head_norm_gains[1])
    attention = grouped_product((gated_a, gated_b), (output_projection[0], output_projection[1]))
    mid_rows = (residual.astype(jnp.float32) + attention).astype(jnp.bfloat16)
    normed = row_norm(mid_rows, feedforward_norm_gain)
    gate_sum = jnp.dot(normed, gate_projection, preferred_element_type=jnp.float32)
    up_sum = jnp.dot(normed, up_projection, preferred_element_type=jnp.float32)
    hidden = (jax.nn.silu(gate_sum) * up_sum).astype(jnp.bfloat16)
    down_sum = grouped_product((hidden,), (down_projection,))
    return (mid_rows.astype(jnp.float32) + down_sum).astype(jnp.bfloat16)
```

```python
import functools

import jax
import jax.numpy as jnp
from jax import lax
from jax.experimental import pallas as pl
from jax.experimental.pallas import tpu as pltpu
from jax.sharding import PartitionSpec as P

FIRST_KEY_SIZE = 128
SECOND_KEY_SIZE = 64
DV = 128
CHUNK = 128
MIDDLE = CHUNK // 2 - 1
PAD = 16
MESH = pl.DeviceIdType.MESH

EPS = 1e-06
SOFTNESS_SCALE = 16.0
VMEM_BYTES = 66_000_000

def dot(a, b, dims):
    return lax.dot_general(a, b, (dims, ((), ())), preferred_element_type=jnp.float32)


def positions():
    row = lax.broadcasted_iota(jnp.int32, (CHUNK, CHUNK), 0)
    column = lax.broadcasted_iota(jnp.int32, (CHUNK, CHUNK), 1)
    return row, column


def fading_sums(fading_row):
    row, column = positions()
    as_column = jnp.sum(jnp.where(row == column, fading_row, 0.0), axis=1, keepdims=True)
    column_sums = jnp.sum(jnp.where(column <= row, fading_row, 0.0), axis=1, keepdims=True)
    row_sums = jnp.sum(jnp.where(row <= column, as_column, 0.0), axis=0, keepdims=True)
    return column_sums, row_sums


def channel_sums(switches):
    row, column = positions()
    x = switches.astype(jnp.float32)
    logs = (jnp.minimum(x, 0.0) - jnp.log1p(jnp.exp(-jnp.abs(x)))) * (1.0 / SOFTNESS_SCALE)
    lower = (column <= row).astype(jnp.bfloat16)
    high = logs.astype(jnp.bfloat16)
    low = (logs - high.astype(jnp.float32)).astype(jnp.bfloat16)
    return dot(lower, high, ((1,), (0,))) + dot(lower, low, ((1,), (0,)))


def lanes_of(head, width, key_width):
    lane = lax.broadcasted_iota(jnp.int32, (1, width), 1)
    return (lane >= head * key_width) & (lane < (head + 1) * key_width)


def advanced(state, inverse_keys, weighted, sums, total_fading, key_width):
    width = state.shape[1]
    end, middle = sums[CHUNK - 1 :, :], sums[MIDDLE : MIDDLE + 1, :]
    head_count = width // key_width
    if key_width % 128 == 0:
        added = jnp.concatenate(
            [
                dot(
                    weighted[:, h * DV : (h + 1) * DV],
                    inverse_keys[:, h * key_width : (h + 1) * key_width],
                    ((0,), (0,)),
                )
                for h in range(head_count)
            ],
            axis=1,
        )
    else:
        added = jnp.zeros((DV, width), jnp.float32)
        for h in range(head_count):
            product = dot(weighted[:, h * DV : (h + 1) * DV], inverse_keys, ((0,), (0,)))
            added = jnp.where(lanes_of(h, width, key_width), product, added)
    return jnp.exp(end + total_fading) * state + jnp.exp(end - middle) * added


def remote(source, target, send, receive, device):
    return pltpu.make_async_remote_copy(
        src_ref=source,
        dst_ref=target,
        send_sem=send,
        recv_sem=receive,
        device_id=device,
        device_id_type=MESH,
    )


def rows_at(index, count):
    return pl.ds(pl.multiple_of(index * count, count), count)


class Ring:
    def __init__(self, peers, place, tp_place, gate, up, down, gate_sems, down_sems):
        self.peers, self.tp_place = peers, tp_place
        self.gate, self.up, self.down = gate, up, down
        self.gate_sems, self.down_sems = gate_sems, down_sems
        self.position = jnp.where(place % 2 == 0, place // 2, peers - 1 - place // 2)
        self.full = (peers - 1) // 2
        self.hops = peers // 2
        self.beyond = (self.origin(0, -1), self.origin(1, -1))
        self.waited = set()
        self.issued = 0
        self.events = ([], [])
        for way in (0, 1):
            for matrix, count in ((0, 4), (1, 2)):
                for hop in range(1, self.hops + 1):
                    for piece in self.carried(way, hop, count):
                        self.events[way].append((matrix, hop, piece))

    def origin(self, way, distance):
        place = (self.position + (distance if way else -distance) + 2 * self.peers) % self.peers
        return jnp.where(place < (self.peers + 1) // 2, 2 * place, 2 * (self.peers - 1 - place) + 1)

    def carried(self, way, hop, count):
        if hop <= self.full:
            return range(count)
        return range(count // 2, count) if way else range(count // 2)

    def piece(self, matrix, origin, piece):
        if matrix:
            half = self.down.shape[1] // 2
            return self.down.at[origin, pl.ds(piece * half, half), :]
        half = self.gate.shape[0] // self.peers // 2
        return (self.up if piece // 2 else self.gate).at[rows_at(origin * 2 + piece % 2, half), :]

    def copy(self, way, matrix, hop, piece, distance):
        ref = self.piece(matrix, self.origin(way, distance), piece)
        send, receive = self.down_sems if matrix else self.gate_sems
        at = (way, hop - 1, piece)
        return remote(ref, ref, send.at[at], receive.at[at], (self.beyond[way], self.tp_place))

    def arrive(self, way, matrix, hop, piece):
        if (way, matrix, hop, piece) not in self.waited:
            self.waited.add((way, matrix, hop, piece))
            self.copy(way, matrix, hop, piece, hop).wait_recv()

    def pump(self, until):
        until = len(self.events[0]) if until is None else (until * len(self.events[0]) + 20) // 21
        while self.issued < until:
            for way in (0, 1):
                matrix, hop, piece = self.events[way][self.issued]
                if hop > 1:
                    self.arrive(way, matrix, hop - 1, piece)
                self.copy(way, matrix, hop, piece, hop - 1).start()
            self.issued += 1

    def arrive_gates(self):
        for hop in range(1, self.hops + 1):
            for way in (0, 1):
                for piece in self.carried(way, hop, 4):
                    self.arrive(way, 0, hop, piece)

    def finish(self):
        for way in (0, 1):
            for matrix, hop, piece in self.events[way]:
                self.copy(way, matrix, hop, piece, hop - 1).wait_send()


def layer_kernel(
    n_sp,
    n_tp,
    residual_hbm,
    qa_hbm,
    qb_hbm,
    ka_hbm,
    kb_hbm,
    sa_hbm,
    sb_hbm,
    values_hbm,
    gates_hbm,
    projection_hbm,
    gate_hbm,
    up_hbm,
    down_hbm,
    fading,
    gains,
    row_gain,
    mid,
    down_sum,
    residual,
    qa,
    qb,
    ka,
    kb,
    sa,
    sb,
    values,
    gates,
    projection,
    gate_full,
    up_full,
    down_full,
    sums_a,
    sums_b,
    before_a,
    before_b,
    starts,
    heads,
    state_a,
    state_b,
    decay,
    packs,
    pair_got,
    later_got,
    terms,
    partner_terms,
    cross_terms,
    cross_got,
    own_sum,
    all_rows,
    hidden,
    stage,
    stage_partner,
    stage_cross,
    stage_got,
    load_sems,
    gate_send,
    gate_receive,
    down_send,
    down_receive,
    pair_sems,
    later_send,
    later_receive,
    terms_send,
    terms_receive,
    cross_send,
    cross_receive,
    rows_send,
    rows_receive,
    passed_send,
    passed_receive,
    half_send,
    half_receive,
    last_send,
    last_receive,
):
    place, tp_place = lax.axis_index("sp"), lax.axis_index("tp")
    chip, core = tp_place // 2, tp_place % 2
    chips = n_tp // 2
    partner = (place, 2 * chip + 1 - core)
    rows, own_rows = qa.shape[0], residual.shape[0]
    chunks, units = rows // CHUNK, own_rows // CHUNK
    width_a, width_b = ka.shape[1], kb.shape[1]
    width = width_a + width_b
    groups = (
        (qa, ka, sa, sums_a, before_a, state_a, FIRST_KEY_SIZE, 0),
        (qb, kb, sb, sums_b, before_b, state_b, SECOND_KEY_SIZE, width_a),
    )
    inner = gate_hbm.shape[0]

    barrier = pltpu.get_barrier_semaphore()
    for k in range(1, n_sp):
        pl.semaphore_signal(
            barrier, inc=1, device_id=((place + k) % n_sp, tp_place), device_id_type=MESH
        )
    for k in range(1, n_tp):
        pl.semaphore_signal(
            barrier, inc=1, device_id=(place, (tp_place + k) % n_tp), device_id_type=MESH
        )

    loads = [
        (gate_hbm, gate_full.at[rows_at(place, inner), :]),
        (up_hbm, up_full.at[rows_at(place, inner), :]),
        (ka_hbm, ka),
        (kb_hbm, kb),
        (sa_hbm, sa),
        (sb_hbm, sb),
        (values_hbm, values),
        (qa_hbm, qa),
        (qb_hbm, qb),
        (down_hbm, down_full.at[place]),
        (projection_hbm, projection),
        (gates_hbm, gates),
        (residual_hbm, residual),
    ]
    loads = [pltpu.make_async_copy(a, b, load_sems.at[i]) for i, (a, b) in enumerate(loads)]
    for load in loads:
        load.start()
    ring = Ring(
        n_sp,
        place,
        tp_place,
        gate_full,
        up_full,
        down_full,
        (gate_send, gate_receive),
        (down_send, down_receive),
    )
    state_a[...] = jnp.zeros_like(state_a)
    state_b[...] = jnp.zeros_like(state_b)
    decay[...] = jnp.zeros_like(decay)
    loads[0].wait()
    loads[1].wait()
    pl.semaphore_wait(barrier, n_sp + n_tp - 2)
    ring.pump(1)
    for load in loads[2:7]:
        load.wait()

    @pl.loop(0, chunks)
    def _(i):
        here = rows_at(i, CHUNK)
        column_sums, _ = fading_sums(fading[i])
        total_fading = column_sums[CHUNK - 1 :, :]
        later = jnp.exp(total_fading - column_sums)
        for group, (_, keys, switches, kept, before, state, key_width, start) in enumerate(groups):
            mine = slice(start, start + keys.shape[1])
            sums = channel_sums(switches[here, :])
            kept[here, :] = sums
            middle = sums[MIDDLE : MIDDLE + 1, :]
            inverse_keys = (keys[here, :].astype(jnp.float32) * jnp.exp(middle - sums)).astype(jnp.bfloat16)
            keys[here, :] = inverse_keys
            before[i] = (state[...] * jnp.exp(middle)).astype(jnp.bfloat16)
            starts[i, :, mine] = jnp.exp(decay[:1, mine] + middle)
            weighted = (values[group, here, :].astype(jnp.float32) * later).astype(jnp.bfloat16)
            state[...] = advanced(state[...], inverse_keys, weighted, sums, total_fading, key_width)
            decay[:, mine] += sums[CHUNK - 1 :, :] + total_fading

    def pack(slot, first, second, factor):
        packs[slot, :DV, :width_a] = first.astype(jnp.bfloat16)
        packs[slot, :DV, width_a:] = second.astype(jnp.bfloat16)
        packs[slot, DV:, :] = jnp.broadcast_to(factor, (PAD, width)).astype(jnp.bfloat16)

    whole_decay = jnp.exp(decay[:1, :])
    pack(0, state_a[...], state_b[...], whole_decay)
    odd = place % 2
    mate = place + 1 - 2 * odd
    pair = remote(packs.at[0], pair_got, pair_sems.at[0], pair_sems.at[1], (mate, tp_place))
    pair.start()
    pair.wait_recv()
    got = pair_got[...].astype(jnp.float32)
    got_a, got_b, got_decay = got[:DV, :width_a], got[:DV, width_a:], got[DV : DV + 1, :]
    is_odd = odd == 1
    pair_a = jnp.where(
        is_odd,
        whole_decay[:, :width_a] * got_a + state_a[...],
        got_decay[:, :width_a] * state_a[...] + got_a,
    )
    pair_b = jnp.where(
        is_odd,
        whole_decay[:, width_a:] * got_b + state_b[...],
        got_decay[:, width_a:] * state_b[...] + got_b,
    )
    pack(1, pair_a, pair_b, whole_decay * got_decay)
    pairs, pair_place = n_sp // 2, place // 2

    def to_later(k):
        return remote(
            packs.at[1],
            later_got.at[k - 1],
            later_send.at[k - 1],
            later_receive.at[k - 1],
            ((place + 2 * k) % n_sp, tp_place),
        )

    for k in range(1, pairs):

        @pl.when(pair_place + k < pairs)
        def _():
            to_later(k).start()

    ring.pump(4)
    loads[7].wait()
    loads[8].wait()

    row, column = positions()
    causal = column <= row

    @pl.loop(0, chunks)
    def _(i):
        here = rows_at(i, CHUNK)
        column_sums, row_sums = fading_sums(fading[i])
        since_start = jnp.exp(column_sums)
        between = jnp.where(causal, jnp.exp(jnp.minimum(column_sums - row_sums, 0.0)), 0.0)
        for group, (queries, keys, _, kept, before, _, key_width, _) in enumerate(groups):
            sums = kept[here, :]
            middle = sums[MIDDLE : MIDDLE + 1, :]
            spread = queries[here, :].astype(jnp.float32) * (jnp.exp(sums - middle) * key_width**-0.5)
            scaled = spread.astype(jnp.bfloat16)
            queries[here, :] = (spread * since_start).astype(jnp.bfloat16)
            inverse_keys = keys[here, :]
            local = before[i]
            for h in range(keys.shape[1] // key_width):
                if key_width % 128 == 0:
                    mine = slice(h * key_width, (h + 1) * key_width)
                    q, k, s = scaled[:, mine], inverse_keys[:, mine], local[:, mine]
                else:
                    q = jnp.where(lanes_of(h, keys.shape[1], key_width), scaled, jnp.zeros_like(scaled))
                    k, s = inverse_keys, local
                scores = jnp.where(causal, dot(q, k, ((1,), (1,))) * between, 0.0).astype(jnp.bfloat16)
                head = dot(scores, values[group, here, h * DV : (h + 1) * DV], ((1,), (0,)))
                heads[group, here, h * DV : (h + 1) * DV] = head + since_start * dot(q, s, ((1,), (1,)))

    ring.pump(6)
    state_a[...] = jnp.zeros_like(state_a)
    state_b[...] = jnp.zeros_like(state_b)
    for k in range(pairs - 1, 0, -1):

        @pl.when(pair_place >= k)
        def _():
            to_later(k).wait_recv()
            part = later_got[k - 1].astype(jnp.float32)
            factor = part[DV : DV + 1, :]
            state_a[...] = factor[:, :width_a] * state_a[...] + part[:DV, :width_a]
            state_b[...] = factor[:, width_a:] * state_b[...] + part[:DV, width_a:]

    state_a[...] = jnp.where(is_odd, got_decay[:, :width_a] * state_a[...] + got_a, state_a[...])
    state_b[...] = jnp.where(is_odd, got_decay[:, width_a:] * state_b[...] + got_b, state_b[...])
    for load in loads[9:]:
        load.wait()

    def attend(i):
        here = rows_at(i, CHUNK)
        pieces = []
        for group, (queries, _, _, _, _, state, key_width, start) in enumerate(groups):
            key_lanes = queries.shape[1]
            earlier = (state[...] * starts[i, :, start : start + key_lanes]).astype(jnp.bfloat16)
            scaled = queries[here, :]
            for h in range(key_lanes // key_width):
                lanes = slice(h * DV, (h + 1) * DV)
                if key_width % 128 == 0:
                    mine = slice(h * key_width, (h + 1) * key_width)
                    q, s = scaled[:, mine], earlier[:, mine]
                else:
                    q = jnp.where(lanes_of(h, key_lanes, key_width), scaled, jnp.zeros_like(scaled))
                    s = earlier
                head = heads[group, here, lanes] + dot(q, s, ((1,), (1,)))
                inverse = lax.rsqrt(jnp.mean(head * head, axis=-1, keepdims=True) + EPS)
                gate = gates[group, here, lanes].astype(jnp.float32)
                silu = gate / (1.0 + jnp.exp(-gate))
                pieces.append((silu * (head * inverse * gains[group : group + 1, lanes])).astype(jnp.bfloat16))
        return dot(jnp.concatenate(pieces, axis=1), projection[...], ((1,), (0,)))

    def chip_at(k):
        return (chip + 1 + k) % chips

    def terms_copy(slot):
        return remote(
            terms.at[slot], partner_terms.at[slot], terms_send.at[slot], terms_receive.at[slot], partner
        )

    def cross_copy(j, u):
        slot = j * units + u
        return remote(
            cross_terms.at[slot],
            cross_got.at[slot],
            cross_send.at[slot],
            cross_receive.at[slot],
            (place, 2 * chip_at(j) + core),
        )

    @pl.loop(0, chips * units)
    def _(k):
        other, u = chip_at(k // units), k % units
        slot = other * units + u
        terms[slot] = attend((2 * other + 1 - core) * units + u).astype(jnp.bfloat16)
        terms_copy(slot).start()

    @pl.loop(0, (chips - 1) * units)
    def _(k):
        j, u = k // units, k % units
        other = chip_at(j)
        slot = other * units + u
        total = attend((2 * other + core) * units + u)
        terms_copy(slot).wait_recv()
        cross_terms[k] = (total + partner_terms[slot].astype(jnp.float32)).astype(jnp.bfloat16)
        cross_copy(j, u).start()

    @pl.loop(0, units)
    def _(u):
        slot = chip * units + u
        total = attend((2 * chip + core) * units + u)
        terms_copy(slot).wait_recv()
        own_sum[u] = total + partner_terms[slot].astype(jnp.float32)

    ring.pump(8)

    def own_at(owner, u):
        return all_rows.at[rows_at(owner * units + u, CHUNK), :]

    def rows_copy(j, u, owner):
        slot = j * units + u
        ref = own_at(owner, u)
        return remote(
            ref, ref, rows_send.at[slot], rows_receive.at[slot], (place, 2 * chip_at(j) + core)
        )

    def passed_copy(j, u, owner):
        slot = j * units + u
        ref = own_at(owner, u)
        return remote(ref, ref, passed_send.at[slot], passed_receive.at[slot], partner)

    def sender_chip(j):
        return (chip - 1 - j + chips) % chips

    for u in range(units):
        here = slice(u * CHUNK, (u + 1) * CHUNK)
        total = residual[here, :].astype(jnp.float32) + own_sum[u]
        for j in range(chips - 1):
            cross_copy(j, u).wait_recv()
            total = total + cross_got[j * units + u].astype(jnp.float32)
        rounded = total.astype(jnp.bfloat16)
        mid[here, :] = rounded
        widened = rounded.astype(jnp.float32)
        inverse = lax.rsqrt(jnp.mean(widened * widened, axis=-1, keepdims=True) + EPS)
        all_rows[rows_at(tp_place * units + u, CHUNK), :] = (widened * inverse * row_gain[...]).astype(jnp.bfloat16)
        for j in range(chips - 1):
            rows_copy(j, u, tp_place).start()
        passed_copy(chips - 1, u, tp_place).start()
    ring.pump(10)
    for u in range(units):
        for j in range(chips - 1):
            rows_copy(j, u, 2 * sender_chip(j) + core).wait_recv()
            passed_copy(j, u, 2 * sender_chip(j) + core).start()
    for u in range(units):
        for j in range(chips):
            passed_copy(j, u, 2 * sender_chip(j) + 1 - core).wait_recv()
    ring.pump(16)
    ring.arrive_gates()

    ff = hidden.shape[1]
    tile = 256
    tiles = ff // tile

    def first_half(n):
        lanes = rows_at(n, tile)
        everything = all_rows[...]
        gate_sum = dot(everything, gate_full[:, lanes], ((1,), (0,)))
        up_sum = dot(everything, up_full[:, lanes], ((1,), (0,)))
        hidden[:, lanes] = (gate_sum / (1.0 + jnp.exp(-gate_sum)) * up_sum).astype(jnp.bfloat16)

    pl.loop(0, tiles // 2)(first_half)
    ring.pump(17)
    pl.loop(tiles // 2, tiles)(first_half)
    ring.pump(18)

    columns = down_hbm.shape[1]

    def half_copy(b):
        return remote(
            stage.at[b, :, 1 - core], stage_partner.at[b], half_send.at[b], half_receive.at[b], partner
        )

    def last_copy(b, j):
        slot = b * max(chips - 1, 1) + j
        return remote(
            stage_cross.at[slot],
            stage_got.at[slot],
            last_send.at[slot],
            last_receive.at[slot],
            (place, 2 * chip_at(j) + core),
        )

    def multiply(b, origin):
        product = dot(hidden[...], down_full[origin], ((1,), (0,))).astype(jnp.bfloat16)
        stage[b] = product.reshape(chips, 2, own_rows, columns)
        half_copy(b).start()

    def combine(b):
        half_copy(b).wait_recv()
        for j in range(chips - 1):
            other = chip_at(j)
            both = stage[b, other, core].astype(jnp.float32) + stage_partner[b, other].astype(jnp.float32)
            stage_cross[b * max(chips - 1, 1) + j] = both.astype(jnp.bfloat16)
            last_copy(b, j).start()

    def close(b, origin):
        total = stage[b, chip, core].astype(jnp.float32) + stage_partner[b, chip].astype(jnp.float32)
        for j in range(chips - 1):
            last_copy(b, j).wait_recv()
            total = total + stage_got[b * max(chips - 1, 1) + j].astype(jnp.float32)
        down_sum[origin] = total

    blocks = [(0, 0)]
    for hop in range(1, ring.hops + 1):
        blocks += [(way, hop) for way in ((0, 1) if hop <= ring.full else (0,))]
    origins = [ring.origin(way, hop) for way, hop in blocks]
    for b, (way, hop) in enumerate(blocks):
        if hop:
            for side in (0, 1) if hop > ring.full else (way,):
                for piece in ring.carried(side, hop, 2):
                    ring.arrive(side, 1, hop, piece)
        multiply(b, origins[b])
        ring.pump({1: 19, 3: 20, 5: 21}.get(b * 8 // n_sp, 0))
        if b >= 1:
            combine(b - 1)
        if b >= 2:
            close(b - 2, origins[b - 2])
    ring.pump(None)
    combine(len(blocks) - 1)
    if len(blocks) > 1:
        close(len(blocks) - 2, origins[-2])
    close(len(blocks) - 1, origins[-1])

    ring.finish()
    pair.wait_send()
    for k in range(1, pairs):

        @pl.when(pair_place + k < pairs)
        def _():
            to_later(k).wait_send()

    for slot in range(chips * units):
        terms_copy(slot).wait_send()
    for u in range(units):
        for j in range(chips - 1):
            cross_copy(j, u).wait_send()
            rows_copy(j, u, tp_place).wait_send()
        for j in range(chips):
            passed_copy(j, u, tp_place).wait_send()
    for b in range(len(blocks)):
        half_copy(b).wait_send()
        for j in range(chips - 1):
            last_copy(b, j).wait_send()


def per_device(
    residual,
    first_group_queries,
    first_group_keys,
    second_group_queries,
    second_group_keys,
    primary_retain_switch_inputs,
    secondary_retain_switch_inputs,
    timestep_fading_exponent,
    values,
    output_gate_logits,
    head_norm_gains,
    output_projection,
    feedforward_norm_gain,
    gate_projection,
    up_projection,
    down_projection,
):
    n_sp, n_tp = lax.axis_size("sp"), lax.axis_size("tp")
    rows, own_rows = first_group_queries.shape[0], residual.shape[0]
    features = residual.shape[1]
    chunks, units, chips = rows // CHUNK, own_rows // CHUNK, n_tp // 2
    width_a, width_b = first_group_keys.shape[1], second_group_keys.shape[1]
    width = width_a + width_b
    value_width = values.shape[2]
    inner, ff = gate_projection.shape
    columns = down_projection.shape[1]
    hops, crossings = n_sp // 2, max(chips - 1, 1)
    projection = output_projection.reshape(-1, features)
    in_hbm = [
        residual,
        first_group_queries,
        second_group_queries,
        first_group_keys,
        second_group_keys,
        primary_retain_switch_inputs,
        secondary_retain_switch_inputs,
        values,
        output_gate_logits,
        projection,
        gate_projection,
        up_projection,
        down_projection,
    ]
    in_vmem = [
        timestep_fading_exponent.reshape(chunks, 1, CHUNK),
        head_norm_gains,
        feedforward_norm_gain.reshape(1, features),
    ]

    def bf16(*shape):
        return pltpu.VMEM(shape, jnp.bfloat16)

    def f32(*shape):
        return pltpu.VMEM(shape, jnp.float32)

    def sems(*shape):
        return pltpu.SemaphoreType.DMA(shape)

    scratch = [pltpu.VMEM(a.shape, a.dtype) for a in in_hbm[:10]]
    scratch += [bf16(n_sp * inner, ff), bf16(n_sp * inner, ff), bf16(n_sp, ff, columns)]
    scratch += [f32(rows, width_a), f32(rows, width_b)]
    scratch += [bf16(chunks, DV, width_a), bf16(chunks, DV, width_b), f32(chunks, 1, width)]
    scratch += [f32(2, rows, value_width), f32(DV, width_a), f32(DV, width_b), f32(8, width)]
    scratch += [bf16(2, DV + PAD, width), bf16(DV + PAD, width), bf16(max(n_sp // 2 - 1, 1), DV + PAD, width)]
    scratch += [bf16(chips * units, CHUNK, features)] * 2
    scratch += [bf16(crossings * units, CHUNK, features)] * 2
    scratch += [f32(units, CHUNK, features), bf16(rows, features), bf16(rows, ff)]
    scratch += [bf16(n_sp, chips, 2, own_rows, columns), bf16(n_sp, chips, own_rows, columns)]
    scratch += [bf16(n_sp * crossings, own_rows, columns)] * 2
    scratch += [sems(len(in_hbm))]
    scratch += [sems(2, hops, 4), sems(2, hops, 4), sems(2, hops, 2), sems(2, hops, 2)]
    scratch += [sems(2), sems(max(n_sp // 2 - 1, 1)), sems(max(n_sp // 2 - 1, 1))]
    scratch += [sems(chips * units)] * 2
    scratch += [sems(crossings * units)] * 4
    scratch += [sems(chips * units)] * 2
    scratch += [sems(n_sp)] * 2
    scratch += [sems(n_sp * crossings)] * 2
    mid, down_sum = pl.pallas_call(
        functools.partial(layer_kernel, n_sp, n_tp),
        in_specs=[pl.BlockSpec(memory_space=pl.ANY)] * len(in_hbm)
        + [pl.BlockSpec(memory_space=pltpu.VMEM)] * len(in_vmem),
        out_specs=[pl.BlockSpec(memory_space=pltpu.VMEM)] * 2,
        out_shape=[
            jax.ShapeDtypeStruct((own_rows, features), jnp.bfloat16),
            jax.ShapeDtypeStruct((n_sp, own_rows, columns), jnp.float32),
        ],
        scratch_shapes=scratch,
        compiler_params=pltpu.CompilerParams(
            collective_id=0, has_side_effects=True, vmem_limit_bytes=VMEM_BYTES
        ),
        name="layer",
    )(*in_hbm, *in_vmem)
    added = down_sum.transpose(1, 0, 2).reshape(own_rows, features)
    return (mid.astype(jnp.float32) + added).astype(jnp.bfloat16)


def solution(mesh):
    return jax.shard_map(
        per_device,
        mesh=mesh,
        in_specs=(
            P(("sp", "tp"), None),
            P("sp", "tp"),
            P("sp", "tp"),
            P("sp", "tp"),
            P("sp", "tp"),
            P("sp", "tp"),
            P("sp", "tp"),
            P("sp"),
            P(None, "sp", "tp"),
            P(None, "sp", "tp"),
            P(None, "tp"),
            P(None, "tp", None),
            P(),
            P("sp", "tp"),
            P("sp", "tp"),
            P("tp", "sp"),
        ),
        out_specs=P(("sp", "tp"), None),
        check_vma=False,
    )
```

```python
import functools

import jax
import jax.numpy as jnp
from jax import lax
from jax.experimental import pallas as pl
from jax.experimental.pallas import tpu as pltpu
from jax.sharding import PartitionSpec as P

FIRST_KEY_SIZE = 128
SECOND_KEY_SIZE = 64
DV = 128
CHUNK = 128
MIDDLE = CHUNK // 2 - 1
PAD = 16
MESH = pl.DeviceIdType.MESH

EPS = 1e-06
SOFTNESS_SCALE = 16.0
VMEM_BYTES = 66_000_000
DEPTH = 4

def dot(a, b, dims):
    return lax.dot_general(a, b, (dims, ((), ())), preferred_element_type=jnp.float32)


def positions():
    row = lax.broadcasted_iota(jnp.int32, (CHUNK, CHUNK), 0)
    column = lax.broadcasted_iota(jnp.int32, (CHUNK, CHUNK), 1)
    return row, column


def fading_sums(fading_row):
    row, column = positions()
    as_column = jnp.sum(jnp.where(row == column, fading_row, 0.0), axis=1, keepdims=True)
    column_sums = jnp.sum(jnp.where(column <= row, fading_row, 0.0), axis=1, keepdims=True)
    row_sums = jnp.sum(jnp.where(row <= column, as_column, 0.0), axis=0, keepdims=True)
    return column_sums, row_sums


def channel_sums(switches):
    row, column = positions()
    x = switches.astype(jnp.float32)
    logs = (jnp.minimum(x, 0.0) - jnp.log1p(jnp.exp(-jnp.abs(x)))) * (1.0 / SOFTNESS_SCALE)
    lower = (column <= row).astype(jnp.bfloat16)
    high = logs.astype(jnp.bfloat16)
    low = (logs - high.astype(jnp.float32)).astype(jnp.bfloat16)
    return dot(lower, high, ((1,), (0,))) + dot(lower, low, ((1,), (0,)))


def lanes_of(head, width, key_width):
    lane = lax.broadcasted_iota(jnp.int32, (1, width), 1)
    return (lane >= head * key_width) & (lane < (head + 1) * key_width)


def advanced(state, inverse_keys, weighted, sums, total_fading, key_width):
    width = state.shape[1]
    end, middle = sums[CHUNK - 1 :, :], sums[MIDDLE : MIDDLE + 1, :]
    head_count = width // key_width
    if key_width % 128 == 0:
        added = jnp.concatenate(
            [
                dot(
                    weighted[:, h * DV : (h + 1) * DV],
                    inverse_keys[:, h * key_width : (h + 1) * key_width],
                    ((0,), (0,)),
                )
                for h in range(head_count)
            ],
            axis=1,
        )
    else:
        added = jnp.zeros((DV, width), jnp.float32)
        for h in range(head_count):
            product = dot(weighted[:, h * DV : (h + 1) * DV], inverse_keys, ((0,), (0,)))
            added = jnp.where(lanes_of(h, width, key_width), product, added)
    return jnp.exp(end + total_fading) * state + jnp.exp(end - middle) * added


def remote(source, target, send, receive, device):
    return pltpu.make_async_remote_copy(
        src_ref=source,
        dst_ref=target,
        send_sem=send,
        recv_sem=receive,
        device_id=device,
        device_id_type=MESH,
    )


def rows_at(index, count):
    return pl.ds(pl.multiple_of(index * count, count), count)


class Line:
    def __init__(self, pairs, place, tp_place, whole, shards, sems, mate_sems):
        self.pairs, self.place, self.tp_place = pairs, place, tp_place
        self.pair, self.side = place // 2, place % 2
        self.gate, self.up, self.down = whole
        self.shards = shards
        self.sems, self.mate_sems = sems, mate_sems
        self.inner, self.half = shards[0].shape[0], shards[2].shape[0] // 2
        self.waited = set()
        self.issued = 0
        self.events = [
            (matrix, hop, piece)
            for matrix, count in ((0, 4), (1, 2))
            for hop in range(1, pairs)
            for piece in range(count)
        ]

    def shard(self, kind, side):
        half = rows_at(side, self.half)
        return self.shards[kind].at[half, :] if kind == 2 else self.shards[kind].at[:, half]

    def landing(self, kind, origin):
        if kind == 2:
            return self.down.at[origin]
        return (self.up if kind else self.gate).at[rows_at(origin, self.inner), :]

    def own(self, kind):
        return self.shard(kind, self.side), self.landing(kind, self.place)

    def mate_copy(self, kind):
        return remote(
            self.shard(kind, 1 - self.side),
            self.landing(kind, self.place),
            self.mate_sems[0].at[kind],
            self.mate_sems[1].at[kind],
            (self.place + 1 - 2 * self.side, self.tp_place),
        )

    def arrive_mate(self, kind):
        if ("mate", kind) not in self.waited:
            self.waited.add(("mate", kind))
            self.mate_copy(kind).wait_recv()

    def reaches(self, way, distance):
        return self.pair + distance < self.pairs if way else self.pair >= distance

    def copy(self, way, matrix, hop, piece, distance):
        pair = (self.pair + (distance if way else -distance) + self.pairs) % self.pairs
        if matrix:
            ref = self.landing(2, 2 * pair + piece)
        else:
            ref = self.landing(piece % 2, 2 * pair + (self.side if piece < 2 else 1 - self.side))
        send, receive = self.sems[matrix]
        at = (way, hop - 1, piece)
        beyond = (self.place + (-2 if way else 2) + 2 * self.pairs) % (2 * self.pairs)
        return remote(ref, ref, send.at[at], receive.at[at], (beyond, self.tp_place))

    def arrive(self, way, matrix, hop, piece):
        if (way, matrix, hop, piece) not in self.waited:
            self.waited.add((way, matrix, hop, piece))

            @pl.when(self.reaches(way, hop))
            def _():
                self.copy(way, matrix, hop, piece, hop).wait_recv()

    def passes(self, way, hop):
        return self.reaches(way, hop - 1) & self.reaches(1 - way, 1)

    def pump(self, until):
        until = len(self.events) if until is None else (until * len(self.events) + 17) // 18
        while self.issued < until:
            matrix, hop, piece = self.events[self.issued]
            if hop == 1 and (matrix or piece >= 2):
                self.arrive_mate(2 if matrix else piece % 2)
            for way in (0, 1):
                if hop > 1:
                    self.arrive(way, matrix, hop - 1, piece)

                @pl.when(self.passes(way, hop))
                def _():
                    self.copy(way, matrix, hop, piece, hop - 1).start()

            self.issued += 1

    def arrive_gates(self):
        for hop in range(1, self.pairs):
            for piece in range(4):
                for way in (0, 1):
                    self.arrive(way, 0, hop, piece)

    def nth(self, q):
        low, high = self.pair, self.pairs - 1 - self.pair
        both = jnp.minimum(low, high)
        near = self.pair + ((q // 2) if q % 2 == 0 else -((q + 1) // 2))
        far = jnp.where(low > high, self.pair - (q - both), self.pair + (q - both))
        return jnp.where(q <= 2 * both, near, far)

    def finish(self):
        for kind in range(3):
            self.mate_copy(kind).wait_send()
        for matrix, hop, piece in self.events:
            for way in (0, 1):

                @pl.when(self.passes(way, hop))
                def _():
                    self.copy(way, matrix, hop, piece, hop - 1).wait_send()


def layer_kernel(
    n_sp,
    n_tp,
    residual_hbm,
    qa_hbm,
    qb_hbm,
    ka_hbm,
    kb_hbm,
    sa_hbm,
    sb_hbm,
    values_hbm,
    gates_hbm,
    projection_hbm,
    gate_hbm,
    up_hbm,
    down_hbm,
    fading,
    gains,
    row_gain,
    *others,
):
    outs, scratch = (others[:1], others[1:]) if down_hbm.shape[1] % 128 == 0 else (others[:2], others[2:])
    layer_body(
        n_sp,
        n_tp,
        (
            residual_hbm,
            qa_hbm,
            qb_hbm,
            ka_hbm,
            kb_hbm,
            sa_hbm,
            sb_hbm,
            values_hbm,
            gates_hbm,
            projection_hbm,
            gate_hbm,
            up_hbm,
            down_hbm,
        ),
        fading,
        gains,
        row_gain,
        outs,
        *scratch,
    )


def layer_body(
    n_sp,
    n_tp,
    in_hbm,
    fading,
    gains,
    row_gain,
    outs,
    residual,
    qa,
    qb,
    ka,
    kb,
    sa,
    sb,
    values,
    gates,
    projection,
    gate_full,
    up_full,
    down_full,
    sums_a,
    sums_b,
    before_a,
    before_b,
    starts,
    heads,
    state_a,
    state_b,
    decay,
    packs,
    pair_got,
    later_got,
    terms,
    partner_terms,
    cross_terms,
    cross_got,
    own_sum,
    all_rows,
    hidden,
    stage,
    stage_partner,
    stage_cross,
    stage_got,
    mid,
    result,
    load_sems,
    mate_send,
    mate_receive,
    gate_send,
    gate_receive,
    down_send,
    down_receive,
    pair_sems,
    later_send,
    later_receive,
    terms_send,
    terms_receive,
    cross_send,
    cross_receive,
    rows_send,
    rows_receive,
    passed_send,
    passed_receive,
    half_send,
    half_receive,
    last_send,
    last_receive,
    out_sems,
):
    residual_hbm, qa_hbm, qb_hbm, ka_hbm, kb_hbm, sa_hbm, sb_hbm, values_hbm, gates_hbm, projection_hbm = in_hbm[:10]
    shards = in_hbm[10:]
    place, tp_place = lax.axis_index("sp"), lax.axis_index("tp")
    chip, core = tp_place // 2, tp_place % 2
    chips = n_tp // 2
    partner = (place, 2 * chip + 1 - core)
    rows, own_rows = qa.shape[0], residual.shape[0]
    chunks, units = rows // CHUNK, own_rows // CHUNK
    width_a, width_b = ka.shape[1], kb.shape[1]
    width = width_a + width_b
    groups = (
        (qa, ka, sa, sums_a, before_a, state_a, FIRST_KEY_SIZE, 0),
        (qb, kb, sb, sums_b, before_b, state_b, SECOND_KEY_SIZE, width_a),
    )
    odd = place % 2
    mate = place + 1 - 2 * odd
    pairs, pair_place = n_sp // 2, place // 2
    line = Line(
        pairs,
        place,
        tp_place,
        (gate_full, up_full, down_full),
        shards,
        ((gate_send, gate_receive), (down_send, down_receive)),
        (mate_send, mate_receive),
    )

    barrier = pltpu.get_barrier_semaphore()
    for k in range(1, n_sp):
        pl.semaphore_signal(
            barrier, inc=1, device_id=((place + k) % n_sp, tp_place), device_id_type=MESH
        )
    for k in range(1, n_tp):
        pl.semaphore_signal(
            barrier, inc=1, device_id=(place, (tp_place + k) % n_tp), device_id_type=MESH
        )

    for k in range(1, chips):
        pl.semaphore_signal(
            barrier,
            inc=1,
            device_id=(mate, 2 * ((chip + k) % chips) + core),
            device_id_type=MESH,
        )

    loads = [
        line.own(0),
        line.own(1),
        (ka_hbm, ka),
        (kb_hbm, kb),
        (sa_hbm, sa),
        (sb_hbm, sb),
        (values_hbm, values),
        (qa_hbm, qa),
        (qb_hbm, qb),
        line.own(2),
        (projection_hbm, projection),
        (gates_hbm, gates),
        (residual_hbm, residual),
    ]
    loads = [pltpu.make_async_copy(a, b, load_sems.at[i]) for i, (a, b) in enumerate(loads)]
    for load in loads:
        load.start()
    state_a[...] = jnp.zeros_like(state_a)
    state_b[...] = jnp.zeros_like(state_b)
    decay[...] = jnp.zeros_like(decay)
    loads[0].wait()
    loads[1].wait()
    pl.semaphore_wait(barrier, n_sp + n_tp + chips - 3)
    line.mate_copy(0).start()
    line.pump(1)
    for load in loads[2:7]:
        load.wait()

    @pl.loop(0, chunks)
    def _(i):
        here = rows_at(i, CHUNK)
        column_sums, _ = fading_sums(fading[i])
        total_fading = column_sums[CHUNK - 1 :, :]
        later = jnp.exp(total_fading - column_sums)
        for group, (_, keys, switches, kept, before, state, key_width, start) in enumerate(groups):
            mine = slice(start, start + keys.shape[1])
            sums = channel_sums(switches[here, :])
            kept[here, :] = sums
            middle = sums[MIDDLE : MIDDLE + 1, :]
            inverse_keys = (keys[here, :].astype(jnp.float32) * jnp.exp(middle - sums)).astype(jnp.bfloat16)
            keys[here, :] = inverse_keys
            before[i] = (state[...] * jnp.exp(middle)).astype(jnp.bfloat16)
            starts[i, :, mine] = jnp.exp(decay[:1, mine] + middle)
            weighted = (values[group, here, :].astype(jnp.float32) * later).astype(jnp.bfloat16)
            state[...] = advanced(state[...], inverse_keys, weighted, sums, total_fading, key_width)
            decay[:, mine] += sums[CHUNK - 1 :, :] + total_fading

    def pack(slot, first, second, factor):
        packs[slot, :DV, :width_a] = first.astype(jnp.bfloat16)
        packs[slot, :DV, width_a:] = second.astype(jnp.bfloat16)
        packs[slot, DV:, :] = jnp.broadcast_to(factor, (PAD, width)).astype(jnp.bfloat16)

    whole_decay = jnp.exp(decay[:1, :])
    pack(0, state_a[...], state_b[...], whole_decay)
    pair = remote(packs.at[0], pair_got, pair_sems.at[0], pair_sems.at[1], (mate, tp_place))
    pair.start()
    line.mate_copy(1).start()
    pair.wait_recv()
    got = pair_got[...].astype(jnp.float32)
    got_a, got_b, got_decay = got[:DV, :width_a], got[:DV, width_a:], got[DV : DV + 1, :]
    is_odd = odd == 1
    pair_a = jnp.where(
        is_odd,
        whole_decay[:, :width_a] * got_a + state_a[...],
        got_decay[:, :width_a] * state_a[...] + got_a,
    )
    pair_b = jnp.where(
        is_odd,
        whole_decay[:, width_a:] * got_b + state_b[...],
        got_decay[:, width_a:] * state_b[...] + got_b,
    )
    pack(1, pair_a, pair_b, whole_decay * got_decay)

    def to_later(k):
        return remote(
            packs.at[1],
            later_got.at[k - 1],
            later_send.at[k - 1],
            later_receive.at[k - 1],
            ((place + 2 * k) % n_sp, tp_place),
        )

    for k in range(1, pairs):

        @pl.when(pair_place + k < pairs)
        def _():
            to_later(k).start()

    line.mate_copy(2).start()
    loads[9].wait()
    line.pump(3)
    loads[7].wait()
    loads[8].wait()

    row, column = positions()
    causal = column <= row

    @pl.loop(0, chunks)
    def _(i):
        here = rows_at(i, CHUNK)
        column_sums, row_sums = fading_sums(fading[i])
        since_start = jnp.exp(column_sums)
        between = jnp.where(causal, jnp.exp(jnp.minimum(column_sums - row_sums, 0.0)), 0.0)
        for group, (queries, keys, _, kept, before, _, key_width, _) in enumerate(groups):
            sums = kept[here, :]
            middle = sums[MIDDLE : MIDDLE + 1, :]
            spread = queries[here, :].astype(jnp.float32) * (jnp.exp(sums - middle) * key_width**-0.5)
            scaled = spread.astype(jnp.bfloat16)
            queries[here, :] = (spread * since_start).astype(jnp.bfloat16)
            inverse_keys = keys[here, :]
            local = before[i]
            for h in range(keys.shape[1] // key_width):
                if key_width % 128 == 0:
                    mine = slice(h * key_width, (h + 1) * key_width)
                    q, k, s = scaled[:, mine], inverse_keys[:, mine], local[:, mine]
                else:
                    q = jnp.where(lanes_of(h, keys.shape[1], key_width), scaled, jnp.zeros_like(scaled))
                    k, s = inverse_keys, local
                scores = jnp.where(causal, dot(q, k, ((1,), (1,))) * between, 0.0).astype(jnp.bfloat16)
                head = dot(scores, values[group, here, h * DV : (h + 1) * DV], ((1,), (0,)))
                heads[group, here, h * DV : (h + 1) * DV] = head + since_start * dot(q, s, ((1,), (1,)))

    state_a[...] = jnp.zeros_like(state_a)
    state_b[...] = jnp.zeros_like(state_b)
    for k in range(pairs - 1, 0, -1):

        @pl.when(pair_place >= k)
        def _():
            to_later(k).wait_recv()
            part = later_got[k - 1].astype(jnp.float32)
            factor = part[DV : DV + 1, :]
            state_a[...] = factor[:, :width_a] * state_a[...] + part[:DV, :width_a]
            state_b[...] = factor[:, width_a:] * state_b[...] + part[:DV, width_a:]

    state_a[...] = jnp.where(is_odd, got_decay[:, :width_a] * state_a[...] + got_a, state_a[...])
    state_b[...] = jnp.where(is_odd, got_decay[:, width_a:] * state_b[...] + got_b, state_b[...])
    for load in loads[10:]:
        load.wait()

    def attend(i):
        here = rows_at(i, CHUNK)
        pieces = []
        for group, (queries, _, _, _, _, state, key_width, start) in enumerate(groups):
            key_lanes = queries.shape[1]
            earlier = (state[...] * starts[i, :, start : start + key_lanes]).astype(jnp.bfloat16)
            scaled = queries[here, :]
            for h in range(key_lanes // key_width):
                lanes = slice(h * DV, (h + 1) * DV)
                if key_width % 128 == 0:
                    mine = slice(h * key_width, (h + 1) * key_width)
                    q, s = scaled[:, mine], earlier[:, mine]
                else:
                    q = jnp.where(lanes_of(h, key_lanes, key_width), scaled, jnp.zeros_like(scaled))
                    s = earlier
                head = heads[group, here, lanes] + dot(q, s, ((1,), (1,)))
                inverse = lax.rsqrt(jnp.mean(head * head, axis=-1, keepdims=True) + EPS)
                gate = gates[group, here, lanes].astype(jnp.float32)
                silu = gate / (1.0 + jnp.exp(-gate))
                pieces.append((silu * (head * inverse * gains[group : group + 1, lanes])).astype(jnp.bfloat16))
        return dot(jnp.concatenate(pieces, axis=1), projection[...], ((1,), (0,)))

    def chip_at(k):
        return (chip + 1 + k) % chips

    def terms_copy(slot):
        return remote(
            terms.at[slot], partner_terms.at[slot], terms_send.at[slot], terms_receive.at[slot], partner
        )

    def cross_copy(j, u):
        slot = j * units + u
        return remote(
            cross_terms.at[slot],
            cross_got.at[slot],
            cross_send.at[slot],
            cross_receive.at[slot],
            (place, 2 * chip_at(j) + core),
        )

    @pl.loop(0, chips * units)
    def _(k):
        other, u = chip_at(k // units), k % units
        slot = other * units + u
        terms[slot] = attend((2 * other + 1 - core) * units + u).astype(jnp.bfloat16)
        terms_copy(slot).start()

    @pl.loop(0, (chips - 1) * units)
    def _(k):
        j, u = k // units, k % units
        other = chip_at(j)
        slot = other * units + u
        total = attend((2 * other + core) * units + u)
        terms_copy(slot).wait_recv()
        cross_terms[k] = (total + partner_terms[slot].astype(jnp.float32)).astype(jnp.bfloat16)
        cross_copy(j, u).start()

    @pl.loop(0, units)
    def _(u):
        slot = chip * units + u
        total = attend((2 * chip + core) * units + u)
        terms_copy(slot).wait_recv()
        own_sum[u] = total + partner_terms[slot].astype(jnp.float32)

    line.pump(6)

    peers = [(dy, dx) for dy in (0, 1) for dx in range(chips) if dy or dx]

    def device_at(dy, dx):
        return (mate if dy else place, 2 * ((chip + dx) % chips) + core)

    def owner_at(dy, dx, of_core):
        side = 1 - odd if dy else odd
        return side * n_tp + 2 * ((chip - dx + chips) % chips) + of_core

    def own_at(owner, u):
        return all_rows.at[rows_at(owner * units + u, CHUNK), :]

    def rows_copy(k, u, owner):
        slot = k * units + u
        ref = own_at(owner, u)
        return remote(ref, ref, rows_send.at[slot], rows_receive.at[slot], device_at(*peers[k]))

    def passed_copy(k, u, owner):
        slot = k * units + u
        ref = own_at(owner, u)
        return remote(ref, ref, passed_send.at[slot], passed_receive.at[slot], partner)

    mine = owner_at(0, 0, core)
    for u in range(units):
        here = slice(u * CHUNK, (u + 1) * CHUNK)
        total = residual[here, :].astype(jnp.float32) + own_sum[u]
        for j in range(chips - 1):
            cross_copy(j, u).wait_recv()
            total = total + cross_got[j * units + u].astype(jnp.float32)
        rounded = total.astype(jnp.bfloat16)
        mid[here, :] = rounded
        widened = rounded.astype(jnp.float32)
        inverse = lax.rsqrt(jnp.mean(widened * widened, axis=-1, keepdims=True) + EPS)
        all_rows[rows_at(mine * units + u, CHUNK), :] = (widened * inverse * row_gain[...]).astype(jnp.bfloat16)
        for k in range(len(peers)):
            rows_copy(k, u, mine).start()
        passed_copy(len(peers), u, mine).start()
    line.pump(8)
    for u in range(units):
        for k, peer in enumerate(peers):
            rows_copy(k, u, owner_at(*peer, core)).wait_recv()
            passed_copy(k, u, owner_at(*peer, core)).start()
        line.pump(10 + 2 * u)
    for u in range(units):
        for k, peer in enumerate(peers + [(0, 0)]):
            passed_copy(k, u, owner_at(*peer, 1 - core)).wait_recv()
    line.pump(14)
    line.arrive_gates()
    ff = hidden.shape[1]
    tile = 256 if ff % 256 == 0 else 128
    tiles = ff // tile
    bands = 2 * chips
    band = 2 * own_rows

    def first_half(n):
        lanes = rows_at(n // bands, tile)
        here = rows_at(n % bands, band)
        gate_sum = dot(all_rows[here, :], gate_full[:, lanes], ((1,), (0,)))
        up_sum = dot(all_rows[here, :], up_full[:, lanes], ((1,), (0,)))
        hidden[here, lanes] = (gate_sum / (1.0 + jnp.exp(-gate_sum)) * up_sum).astype(jnp.bfloat16)

    pl.loop(0, tiles * bands * 2 // 3)(first_half)
    line.pump(15)
    pl.loop(tiles * bands * 2 // 3, tiles * bands)(first_half)

    columns = shards[2].shape[1]
    direct = columns % 128 == 0
    count = len(peers)

    def half_copy(b):
        return remote(
            stage.at[b % DEPTH, :, 1 - core], stage_partner.at[b], half_send.at[b], half_receive.at[b], partner
        )

    def last_copy(b, k):
        slot = b * count + k
        return remote(
            stage_cross.at[b % DEPTH * count + k],
            stage_got.at[slot],
            last_send.at[slot],
            last_receive.at[slot],
            device_at(*peers[k]),
        )

    def out_copy(b, origin):
        lanes = rows_at(origin, columns)
        done = (mid.at[:, lanes], outs[0].at[:, lanes]) if direct else (result.at[b], outs[1].at[origin])
        return pltpu.make_async_copy(*done, out_sems.at[b])

    def multiply(b, origin):
        if b >= DEPTH:
            half_copy(b - DEPTH).wait_send()

        @pl.loop(0, bands)
        def _(g):
            product = dot(hidden[rows_at(g, band), :], down_full[origin], ((1,), (0,))).astype(jnp.bfloat16)
            stage[b % DEPTH, g] = product.reshape(2, own_rows, columns)

        half_copy(b).start()

    def combine(b):
        half_copy(b).wait_recv()
        for k, (dy, dx) in enumerate(peers):
            if b >= DEPTH:
                last_copy(b - DEPTH, k).wait_send()
            band_at = (1 - odd if dy else odd) * chips + (chip + dx) % chips
            both = stage[b % DEPTH, band_at, core].astype(jnp.float32) + stage_partner[b, band_at].astype(jnp.float32)
            stage_cross[b % DEPTH * count + k] = both.astype(jnp.bfloat16)
            last_copy(b, k).start()

    def close(b, origin):
        band_at = odd * chips + chip
        total = stage[b % DEPTH, band_at, core].astype(jnp.float32) + stage_partner[b, band_at].astype(jnp.float32)
        for k in range(count):
            last_copy(b, k).wait_recv()
            total = total + stage_got[b * count + k].astype(jnp.float32)
        if direct:
            lanes = rows_at(origin, columns)
            mid[:, lanes] = (mid[:, lanes].astype(jnp.float32) + total).astype(jnp.bfloat16)
        else:
            result[b] = total
        out_copy(b, origin).start()

    origins = [2 * line.nth(b // 2) + b % 2 for b in range(n_sp)]
    for b in range(n_sp):
        if b >= 2:
            line.arrive(0, 1, b // 2, b % 2)
            line.arrive(1, 1, b // 2, b % 2)
        multiply(b, origins[b])
        if b >= 1:
            combine(b - 1)
        line.pump({1: 16, 3: 17, 4: 18}.get(b * 8 // n_sp, 0))
        if b >= 3:
            close(b - 3, origins[b - 3])
    line.pump(None)
    combine(n_sp - 1)
    for b in range(max(n_sp - 3, 0), n_sp):
        close(b, origins[b])
    for b in range(n_sp):
        out_copy(b, origins[b]).wait()
    if not direct:
        pltpu.sync_copy(mid, outs[0])

    line.finish()
    pair.wait_send()
    for k in range(1, pairs):

        @pl.when(pair_place + k < pairs)
        def _():
            to_later(k).wait_send()

    for slot in range(chips * units):
        terms_copy(slot).wait_send()
    for u in range(units):
        for j in range(chips - 1):
            cross_copy(j, u).wait_send()
        for k in range(count):
            rows_copy(k, u, mine).wait_send()
        for k in range(count + 1):
            passed_copy(k, u, mine).wait_send()
    for b in range(max(n_sp - DEPTH, 0), n_sp):
        half_copy(b).wait_send()
        for k in range(count):
            last_copy(b, k).wait_send()


def per_device(
    residual,
    first_group_queries,
    first_group_keys,
    second_group_queries,
    second_group_keys,
    primary_retain_switch_inputs,
    secondary_retain_switch_inputs,
    timestep_fading_exponent,
    values,
    output_gate_logits,
    head_norm_gains,
    output_projection,
    feedforward_norm_gain,
    gate_projection,
    up_projection,
    down_projection,
):
    n_sp, n_tp = lax.axis_size("sp"), lax.axis_size("tp")
    rows, own_rows = first_group_queries.shape[0], residual.shape[0]
    features = residual.shape[1]
    chunks, units, chips = rows // CHUNK, own_rows // CHUNK, n_tp // 2
    width_a, width_b = first_group_keys.shape[1], second_group_keys.shape[1]
    width = width_a + width_b
    value_width = values.shape[2]
    inner, ff = gate_projection.shape
    columns = down_projection.shape[1]
    pairs, crossings, peers = n_sp // 2, max(chips - 1, 1), 2 * chips - 1
    direct = columns % 128 == 0
    projection = output_projection.reshape(-1, features)
    in_hbm = [
        residual,
        first_group_queries,
        second_group_queries,
        first_group_keys,
        second_group_keys,
        primary_retain_switch_inputs,
        secondary_retain_switch_inputs,
        values,
        output_gate_logits,
        projection,
        gate_projection,
        up_projection,
        down_projection,
    ]
    in_vmem = [
        timestep_fading_exponent.reshape(chunks, 1, CHUNK),
        head_norm_gains,
        feedforward_norm_gain.reshape(1, features),
    ]

    def bf16(*shape):
        return pltpu.VMEM(shape, jnp.bfloat16)

    def f32(*shape):
        return pltpu.VMEM(shape, jnp.float32)

    def sems(*shape):
        return pltpu.SemaphoreType.DMA(shape)

    scratch = [pltpu.VMEM(a.shape, a.dtype) for a in in_hbm[:10]]
    scratch += [bf16(n_sp * inner, ff // 2)] * 2 + [bf16(n_sp, ff // 2, columns)]
    scratch += [f32(rows, width_a), f32(rows, width_b)]
    scratch += [bf16(chunks, DV, width_a), bf16(chunks, DV, width_b), f32(chunks, 1, width)]
    scratch += [f32(2, rows, value_width), f32(DV, width_a), f32(DV, width_b), f32(8, width)]
    scratch += [bf16(2, DV + PAD, width), bf16(DV + PAD, width), bf16(max(n_sp // 2 - 1, 1), DV + PAD, width)]
    scratch += [bf16(chips * units, CHUNK, features)] * 2
    scratch += [bf16(crossings * units, CHUNK, features)] * 2
    scratch += [f32(units, CHUNK, features), bf16(2 * rows, features), bf16(2 * rows, ff // 2)]
    scratch += [bf16(DEPTH, 2 * chips, 2, own_rows, columns), bf16(n_sp, 2 * chips, own_rows, columns)]
    scratch += [bf16(DEPTH * peers, own_rows, columns), bf16(n_sp * peers, own_rows, columns)]
    scratch += [bf16(own_rows, features), f32(*((8, 128) if direct else (n_sp, own_rows, columns)))]
    scratch += [sems(len(in_hbm)), sems(3), sems(3)]
    scratch += [sems(2, max(pairs - 1, 1), 4)] * 2 + [sems(2, max(pairs - 1, 1), 2)] * 2
    scratch += [sems(2), sems(max(n_sp // 2 - 1, 1)), sems(max(n_sp // 2 - 1, 1))]
    scratch += [sems(chips * units)] * 2
    scratch += [sems(crossings * units)] * 2
    scratch += [sems(peers * units)] * 2
    scratch += [sems((peers + 1) * units)] * 2
    scratch += [sems(n_sp)] * 2
    scratch += [sems(n_sp * peers)] * 2
    scratch += [sems(n_sp)]
    row_shape = jax.ShapeDtypeStruct((own_rows, features), jnp.bfloat16)
    sums_shape = jax.ShapeDtypeStruct((n_sp, own_rows, columns), jnp.float32)
    outs = [row_shape] if direct else [row_shape, sums_shape]
    outs = pl.pallas_call(
        functools.partial(layer_kernel, n_sp, n_tp),
        in_specs=[pl.BlockSpec(memory_space=pl.ANY)] * len(in_hbm)
        + [pl.BlockSpec(memory_space=pltpu.VMEM)] * len(in_vmem),
        out_specs=[pl.BlockSpec(memory_space=pl.ANY)] * len(outs),
        out_shape=outs,
        scratch_shapes=scratch,
        compiler_params=pltpu.CompilerParams(
            collective_id=0, has_side_effects=True, vmem_limit_bytes=VMEM_BYTES
        ),
        name="layer",
    )(*in_hbm, *in_vmem)
    if direct:
        return outs[0]
    added = outs[1].transpose(1, 0, 2).reshape(own_rows, features)
    return (outs[0].astype(jnp.float32) + added).astype(jnp.bfloat16)


def solution(mesh):
    return jax.shard_map(
        per_device,
        mesh=mesh,
        in_specs=(
            P(("sp", "tp"), None),
            P("sp", "tp"),
            P("sp", "tp"),
            P("sp", "tp"),
            P("sp", "tp"),
            P("sp", "tp"),
            P("sp", "tp"),
            P("sp"),
            P(None, "sp", "tp"),
            P(None, "sp", "tp"),
            P(None, "tp"),
            P(None, "tp", None),
            P(),
            P("sp", "tp"),
            P("sp", "tp"),
            P("tp", "sp"),
        ),
        out_specs=P(("sp", "tp"), None),
        check_vma=False,
    )
```

```python
import functools

import jax
import jax.numpy as jnp
from jax import lax
from jax.experimental import pallas as pl
from jax.experimental.pallas import tpu as pltpu
from jax.sharding import PartitionSpec as P

FIRST_KEY_SIZE = 128
SECOND_KEY_SIZE = 64
DV = 128
CHUNK = 128
MIDDLE = CHUNK // 2 - 1
PAD = 16
MESH = pl.DeviceIdType.MESH

EPS = 1e-06
SOFTNESS_SCALE = 16.0
VMEM_BYTES = 62_000_000
DEPTH = 4
EARLY = (1,)

def dot(a, b, dims):
    return lax.dot_general(a, b, (dims, ((), ())), preferred_element_type=jnp.float32)


def positions():
    row = lax.broadcasted_iota(jnp.int32, (CHUNK, CHUNK), 0)
    column = lax.broadcasted_iota(jnp.int32, (CHUNK, CHUNK), 1)
    return row, column


def fading_sums(fading_row):
    row, column = positions()
    as_column = jnp.sum(jnp.where(row == column, fading_row, 0.0), axis=1, keepdims=True)
    column_sums = jnp.sum(jnp.where(column <= row, fading_row, 0.0), axis=1, keepdims=True)
    row_sums = jnp.sum(jnp.where(row <= column, as_column, 0.0), axis=0, keepdims=True)
    return column_sums, row_sums


def channel_sums(switches):
    row, column = positions()
    x = switches.astype(jnp.float32)
    logs = (jnp.minimum(x, 0.0) - jnp.log1p(jnp.exp(-jnp.abs(x)))) * (1.0 / SOFTNESS_SCALE)
    lower = (column <= row).astype(jnp.bfloat16)
    high = logs.astype(jnp.bfloat16)
    low = (logs - high.astype(jnp.float32)).astype(jnp.bfloat16)
    return dot(lower, high, ((1,), (0,))) + dot(lower, low, ((1,), (0,)))


def lanes_of(head, width, key_width):
    lane = lax.broadcasted_iota(jnp.int32, (1, width), 1)
    return (lane >= head * key_width) & (lane < (head + 1) * key_width)


def advanced(state, inverse_keys, weighted, sums, total_fading, key_width):
    width = state.shape[1]
    end, middle = sums[CHUNK - 1 :, :], sums[MIDDLE : MIDDLE + 1, :]
    head_count = width // key_width
    if key_width % 128 == 0:
        added = jnp.concatenate(
            [
                dot(
                    weighted[:, h * DV : (h + 1) * DV],
                    inverse_keys[:, h * key_width : (h + 1) * key_width],
                    ((0,), (0,)),
                )
                for h in range(head_count)
            ],
            axis=1,
        )
    else:
        added = jnp.zeros((DV, width), jnp.float32)
        for h in range(head_count):
            product = dot(weighted[:, h * DV : (h + 1) * DV], inverse_keys, ((0,), (0,)))
            added = jnp.where(lanes_of(h, width, key_width), product, added)
    return jnp.exp(end + total_fading) * state + jnp.exp(end - middle) * added


def remote(source, target, send, receive, device):
    return pltpu.make_async_remote_copy(
        src_ref=source,
        dst_ref=target,
        send_sem=send,
        recv_sem=receive,
        device_id=device,
        device_id_type=MESH,
    )


def rows_at(index, count):
    return pl.ds(pl.multiple_of(index * count, count), count)


class Line:
    def __init__(self, pairs, place, tp_place, whole, shards, sems, mate_sems):
        self.pairs, self.place, self.tp_place = pairs, place, tp_place
        self.pair, self.side = place // 2, place % 2
        self.gate, self.up, self.down = whole
        self.shards = shards
        self.sems, self.mate_sems = sems, mate_sems
        self.inner, self.half = shards[0].shape[0], shards[2].shape[0] // 2
        self.waited = set()
        self.issued = [0, 0]
        self.split = self.down.shape[2] % 256 == 0
        self.events = [
            (matrix, hop, piece)
            for matrix in (0, 1)
            for hop in range(1, pairs)
            for piece in self.pieces(matrix, hop)
        ]

    def pieces(self, matrix, hop):
        if not matrix:
            return range(4)
        return (0, 2, 3) if hop == self.pairs - 1 and self.split else (0, 1)

    def shard(self, kind, side):
        half = rows_at(side, self.half)
        return self.shards[kind].at[half, :] if kind == 2 else self.shards[kind].at[:, half]

    def landing(self, kind, origin):
        if kind == 2:
            return self.down.at[origin]
        return (self.up if kind else self.gate).at[rows_at(origin, self.inner), :]

    def own(self, kind):
        return self.shard(kind, self.side), self.landing(kind, self.place)

    def mate_copy(self, kind):
        return remote(
            self.shard(kind, 1 - self.side),
            self.landing(kind, self.place),
            self.mate_sems[0].at[kind],
            self.mate_sems[1].at[kind],
            (self.place + 1 - 2 * self.side, self.tp_place),
        )

    def arrive_mate(self, kind):
        if ("mate", kind) not in self.waited:
            self.waited.add(("mate", kind))
            self.mate_copy(kind).wait_recv()

    def reaches(self, way, distance):
        return self.pair + distance < self.pairs if way else self.pair >= distance

    def copy(self, way, matrix, hop, piece, distance):
        pair = (self.pair + (distance if way else -distance) + self.pairs) % self.pairs
        if matrix and piece >= 2:
            half = self.down.shape[2] // 2
            ref = self.down.at[2 * pair + 1, :, pl.ds((piece - 2) * half, half)]
        elif matrix:
            ref = self.landing(2, 2 * pair + piece)
        else:
            ref = self.landing(piece % 2, 2 * pair + (self.side if piece < 2 else 1 - self.side))
        send, receive = self.sems[matrix]
        at = (way, hop - 1, piece)
        beyond = (self.place + (-2 if way else 2) + 2 * self.pairs) % (2 * self.pairs)
        return remote(ref, ref, send.at[at], receive.at[at], (beyond, self.tp_place))

    def arrive(self, way, matrix, hop, piece):
        if (way, matrix, hop, piece) not in self.waited:
            self.waited.add((way, matrix, hop, piece))

            @pl.when(self.reaches(way, hop))
            def _():
                self.copy(way, matrix, hop, piece, hop).wait_recv()

    def passes(self, way, hop):
        return self.reaches(way, hop - 1) & self.reaches(1 - way, 1)

    def pump(self, until, ways=(0, 1)):
        count = 6 * (self.pairs - 1)
        until = len(self.events) if until >= 18 else (until * count + 17) // 18
        for way in ways:
            for matrix, hop, piece in self.events[self.issued[way] : until]:
                if hop == 1 and (matrix or piece >= 2):
                    self.arrive_mate(2 if matrix else piece % 2)
                if hop > 1:
                    self.arrive(way, matrix, hop - 1, 1 if matrix and piece else piece)

                @pl.when(self.passes(way, hop))
                def _():
                    self.copy(way, matrix, hop, piece, hop - 1).start()

            self.issued[way] = max(until, self.issued[way])

    def arrive_gates(self, until):
        for hop in range(1, until + 1):
            for piece in range(4):
                for way in (0, 1):
                    self.arrive(way, 0, hop, piece)

    def nth(self, q):
        low, high = self.pair, self.pairs - 1 - self.pair
        both = jnp.minimum(low, high)
        near = self.pair + ((q // 2) if q % 2 == 0 else -((q + 1) // 2))
        far = jnp.where(low > high, self.pair - (q - both), self.pair + (q - both))
        return jnp.where(q <= 2 * both, near, far)

    def finish(self):
        for kind in range(3):
            self.mate_copy(kind).wait_send()
        for matrix, hop, piece in self.events:
            for way in (0, 1):

                @pl.when(self.passes(way, hop))
                def _():
                    self.copy(way, matrix, hop, piece, hop - 1).wait_send()


def layer_kernel(
    n_sp,
    n_tp,
    residual_hbm,
    qa_hbm,
    qb_hbm,
    ka_hbm,
    kb_hbm,
    sa_hbm,
    sb_hbm,
    values_hbm,
    gates_hbm,
    projection_hbm,
    gate_hbm,
    up_hbm,
    down_hbm,
    fading,
    gains,
    row_gain,
    *others,
):
    outs, scratch = (others[:1], others[1:]) if down_hbm.shape[1] % 128 == 0 else (others[:2], others[2:])
    layer_body(
        n_sp,
        n_tp,
        (
            residual_hbm,
            qa_hbm,
            qb_hbm,
            ka_hbm,
            kb_hbm,
            sa_hbm,
            sb_hbm,
            values_hbm,
            gates_hbm,
            projection_hbm,
            gate_hbm,
            up_hbm,
            down_hbm,
        ),
        fading,
        gains,
        row_gain,
        outs,
        *scratch,
    )


def layer_body(
    n_sp,
    n_tp,
    in_hbm,
    fading,
    gains,
    row_gain,
    outs,
    gate_full,
    up_full,
    down_full,
    state_a,
    state_b,
    decay,
    packs,
    pair_got,
    later_got,
    terms,
    partner_terms,
    cross_terms,
    cross_got,
    all_rows,
    hidden,
    stage,
    stage_partner,
    stage_cross,
    stage_got,
    mid,
    load_sems,
    mate_send,
    mate_receive,
    gate_send,
    gate_receive,
    down_send,
    down_receive,
    pair_sems,
    later_send,
    later_receive,
    terms_send,
    terms_receive,
    cross_send,
    cross_receive,
    rows_send,
    rows_receive,
    passed_send,
    passed_receive,
    half_send,
    half_receive,
    last_send,
    last_receive,
):
    residual_hbm, qa_hbm, qb_hbm, ka_hbm, kb_hbm, sa_hbm, sb_hbm, values_hbm, gates_hbm, projection_hbm = in_hbm[:10]
    shards = in_hbm[10:]
    place, tp_place = lax.axis_index("sp"), lax.axis_index("tp")
    chip, core = tp_place // 2, tp_place % 2
    chips = n_tp // 2
    partner = (place, 2 * chip + 1 - core)
    rows, own_rows = qa_hbm.shape[0], residual_hbm.shape[0]
    chunks, units = rows // CHUNK, own_rows // CHUNK
    width_a, width_b = ka_hbm.shape[1], kb_hbm.shape[1]
    width = width_a + width_b
    odd = place % 2
    mate = place + 1 - 2 * odd
    pairs, pair_place = n_sp // 2, place // 2
    line = Line(
        pairs,
        place,
        tp_place,
        (gate_full, up_full, down_full),
        shards,
        ((gate_send, gate_receive), (down_send, down_receive)),
        (mate_send, mate_receive),
    )

    barrier = pltpu.get_barrier_semaphore()
    for k in range(1, n_sp):
        pl.semaphore_signal(
            barrier, inc=1, device_id=((place + k) % n_sp, tp_place), device_id_type=MESH
        )
    for k in range(1, n_tp):
        pl.semaphore_signal(
            barrier, inc=1, device_id=(place, (tp_place + k) % n_tp), device_id_type=MESH
        )

    for k in range(1, chips):
        pl.semaphore_signal(
            barrier,
            inc=1,
            device_id=(mate, 2 * ((chip + k) % chips) + core),
            device_id_type=MESH,
        )

    def pair_copy():
        return remote(packs.at[0], pair_got, pair_sems.at[0], pair_sems.at[1], (mate, tp_place))

    def to_later(k, slot=1):
        return remote(
            packs.at[slot],
            later_got.at[k - 1],
            later_send.at[k - 1],
            later_receive.at[k - 1],
            ((place + 2 * k) % n_sp, tp_place),
        )

    def chip_at(k):
        return (chip + 1 + k) % chips

    def terms_copy(slot):
        return remote(
            terms.at[slot], partner_terms.at[slot], terms_send.at[slot], terms_receive.at[slot], partner
        )

    def cross_copy(j, u):
        slot = j * units + u
        return remote(
            cross_terms.at[slot],
            cross_got.at[slot],
            cross_send.at[slot],
            cross_receive.at[slot],
            (place, 2 * chip_at(j) + core),
        )

    peers = [(dy, dx) for dy in (0, 1) for dx in range(chips) if dy or dx]

    def device_at(dy, dx):
        return (mate if dy else place, 2 * ((chip + dx) % chips) + core)

    def owner_at(dy, dx, of_core):
        side = 1 - odd if dy else odd
        return side * n_tp + 2 * ((chip - dx + chips) % chips) + of_core

    def own_at(owner, u):
        return all_rows.at[rows_at(owner * units + u, CHUNK), :]

    def rows_copy(k, u, owner):
        slot = k * units + u
        ref = own_at(owner, u)
        return remote(ref, ref, rows_send.at[slot], rows_receive.at[slot], device_at(*peers[k]))

    def passed_copy(k, u, owner):
        slot = k * units + u
        ref = own_at(owner, u)
        return remote(ref, ref, passed_send.at[slot], passed_receive.at[slot], partner)

    mine = owner_at(0, 0, core)
    def attention(
        residual,
        qa,
        qb,
        ka,
        kb,
        sa,
        sb,
        values,
        gates,
        projection,
        sums_a,
        sums_b,
        before_a,
        before_b,
        starts,
        heads,
        own_sum,
    ):
        groups = (
            (qa, ka, sa, sums_a, before_a, state_a, FIRST_KEY_SIZE, 0),
            (qb, kb, sb, sums_b, before_b, state_b, SECOND_KEY_SIZE, width_a),
        )

        loads = [
            line.own(0),
            line.own(1),
            (ka_hbm, ka),
            (kb_hbm, kb),
            (sa_hbm, sa),
            (sb_hbm, sb),
            (values_hbm, values),
            (qa_hbm, qa),
            (qb_hbm, qb),
            line.own(2),
            (projection_hbm, projection),
            (gates_hbm, gates),
            (residual_hbm, residual),
        ]
        loads = [pltpu.make_async_copy(a, b, load_sems.at[i]) for i, (a, b) in enumerate(loads)]
        for load in loads:
            load.start()
        state_a[...] = jnp.zeros_like(state_a)
        state_b[...] = jnp.zeros_like(state_b)
        decay[...] = jnp.zeros_like(decay)
        loads[0].wait()
        loads[1].wait()
        pl.semaphore_wait(barrier, n_sp + n_tp + chips - 3)
        line.pump(1)
        for load in loads[2:7]:
            load.wait()

        @pl.loop(0, chunks)
        def _(i):
            here = rows_at(i, CHUNK)
            column_sums, _ = fading_sums(fading[i])
            total_fading = column_sums[CHUNK - 1 :, :]
            later = jnp.exp(total_fading - column_sums)
            for group, (_, keys, switches, kept, before, state, key_width, start) in enumerate(groups):
                mine = slice(start, start + keys.shape[1])
                sums = channel_sums(switches[here, :])
                kept[here, :] = sums
                middle = sums[MIDDLE : MIDDLE + 1, :]
                inverse_keys = (keys[here, :].astype(jnp.float32) * jnp.exp(middle - sums)).astype(jnp.bfloat16)
                keys[here, :] = inverse_keys
                before[i] = (state[...] * jnp.exp(middle)).astype(jnp.bfloat16)
                starts[i, :, mine] = jnp.exp(decay[:1, mine] + middle)
                weighted = (values[group, here, :].astype(jnp.float32) * later).astype(jnp.bfloat16)
                state[...] = advanced(state[...], inverse_keys, weighted, sums, total_fading, key_width)
                decay[:, mine] += sums[CHUNK - 1 :, :] + total_fading

        def pack(slot, first, second, factor):
            packs[slot, :DV, :width_a] = first.astype(jnp.bfloat16)
            packs[slot, :DV, width_a:] = second.astype(jnp.bfloat16)
            packs[slot, DV:, :] = jnp.broadcast_to(factor, (PAD, width)).astype(jnp.bfloat16)

        whole_decay = jnp.exp(decay[:1, :])
        pack(0, state_a[...], state_b[...], whole_decay)
        pair_copy().start()
        line.mate_copy(0).start()
        line.mate_copy(1).start()
        line.pump(2, EARLY)
        pair_copy().wait_recv()
        got = pair_got[...].astype(jnp.float32)
        got_a, got_b, got_decay = got[:DV, :width_a], got[:DV, width_a:], got[DV : DV + 1, :]
        is_odd = odd == 1
        pair_a = jnp.where(
            is_odd,
            whole_decay[:, :width_a] * got_a + state_a[...],
            got_decay[:, :width_a] * state_a[...] + got_a,
        )
        pair_b = jnp.where(
            is_odd,
            whole_decay[:, width_a:] * got_b + state_b[...],
            got_decay[:, width_a:] * state_b[...] + got_b,
        )
        pack(1, pair_a, pair_b, whole_decay * got_decay)
        for k in range(1, pairs):

            @pl.when(pair_place + k < pairs - 1)
            def _():
                to_later(k).start()

        line.mate_copy(2).start()
        loads[9].wait()
        line.pump(2)
        loads[7].wait()
        loads[8].wait()

        row, column = positions()
        causal = column <= row

        @pl.loop(0, chunks)
        def _(i):
            here = rows_at(i, CHUNK)
            column_sums, row_sums = fading_sums(fading[i])
            since_start = jnp.exp(column_sums)
            between = jnp.where(causal, jnp.exp(jnp.minimum(column_sums - row_sums, 0.0)), 0.0)
            for group, (queries, keys, _, kept, before, _, key_width, _) in enumerate(groups):
                sums = kept[here, :]
                middle = sums[MIDDLE : MIDDLE + 1, :]
                spread = queries[here, :].astype(jnp.float32) * (jnp.exp(sums - middle) * key_width**-0.5)
                scaled = spread.astype(jnp.bfloat16)
                queries[here, :] = (spread * since_start).astype(jnp.bfloat16)
                inverse_keys = keys[here, :]
                local = before[i]
                for h in range(keys.shape[1] // key_width):
                    if key_width % 128 == 0:
                        mine = slice(h * key_width, (h + 1) * key_width)
                        q, k, s = scaled[:, mine], inverse_keys[:, mine], local[:, mine]
                    else:
                        q = jnp.where(lanes_of(h, keys.shape[1], key_width), scaled, jnp.zeros_like(scaled))
                        k, s = inverse_keys, local
                    scores = jnp.where(causal, dot(q, k, ((1,), (1,))) * between, 0.0).astype(jnp.bfloat16)
                    head = dot(scores, values[group, here, h * DV : (h + 1) * DV], ((1,), (0,)))
                    heads[group, here, h * DV : (h + 1) * DV] = head + since_start * dot(q, s, ((1,), (1,)))

        state_a[...] = jnp.zeros_like(state_a)
        state_b[...] = jnp.zeros_like(state_b)

        def follow(slot):
            part = slot[...].astype(jnp.float32)
            factor = part[DV : DV + 1, :]
            state_a[...] = factor[:, :width_a] * state_a[...] + part[:DV, :width_a]
            state_b[...] = factor[:, width_a:] * state_b[...] + part[:DV, width_a:]

        for k in range(pairs - 2, 0, -1):

            @pl.when((pair_place >= k) & (pair_place < pairs - 1))
            def _():
                to_later(k).wait_recv()
                follow(later_got.at[k - 1])

        if pairs > 1:

            @pl.when(pair_place == pairs - 2)
            def _():
                part = packs[1].astype(jnp.float32)
                factor = part[DV : DV + 1, :]
                pack(
                    2,
                    factor[:, :width_a] * state_a[...] + part[:DV, :width_a],
                    factor[:, width_a:] * state_b[...] + part[:DV, width_a:],
                    factor,
                )
                to_later(1, 2).start()

        line.pump(3)
        if pairs > 1:

            @pl.when(pair_place == pairs - 1)
            def _():
                to_later(1).wait_recv()
                follow(later_got.at[0])

        state_a[...] = jnp.where(is_odd, got_decay[:, :width_a] * state_a[...] + got_a, state_a[...])
        state_b[...] = jnp.where(is_odd, got_decay[:, width_a:] * state_b[...] + got_b, state_b[...])
        for load in loads[10:]:
            load.wait()

        def attend(i):
            here = rows_at(i, CHUNK)
            pieces = []
            for group, (queries, _, _, _, _, state, key_width, start) in enumerate(groups):
                key_lanes = queries.shape[1]
                earlier = (state[...] * starts[i, :, start : start + key_lanes]).astype(jnp.bfloat16)
                scaled = queries[here, :]
                for h in range(key_lanes // key_width):
                    lanes = slice(h * DV, (h + 1) * DV)
                    if key_width % 128 == 0:
                        mine = slice(h * key_width, (h + 1) * key_width)
                        q, s = scaled[:, mine], earlier[:, mine]
                    else:
                        q = jnp.where(lanes_of(h, key_lanes, key_width), scaled, jnp.zeros_like(scaled))
                        s = earlier
                    head = heads[group, here, lanes] + dot(q, s, ((1,), (1,)))
                    inverse = lax.rsqrt(jnp.mean(head * head, axis=-1, keepdims=True) + EPS)
                    gate = gates[group, here, lanes].astype(jnp.float32)
                    silu = gate / (1.0 + jnp.exp(-gate))
                    pieces.append((silu * (head * inverse * gains[group : group + 1, lanes])).astype(jnp.bfloat16))
            return dot(jnp.concatenate(pieces, axis=1), projection[...], ((1,), (0,)))

        @pl.loop(0, chips * units)
        def _(k):
            other, u = chip_at(k // units), k % units
            slot = other * units + u
            terms[slot] = attend((2 * other + 1 - core) * units + u).astype(jnp.bfloat16)
            terms_copy(slot).start()

        @pl.loop(0, (chips - 1) * units)
        def _(k):
            j, u = k // units, k % units
            other = chip_at(j)
            slot = other * units + u
            total = attend((2 * other + core) * units + u)
            terms_copy(slot).wait_recv()
            cross_terms[k] = (total + partner_terms[slot].astype(jnp.float32)).astype(jnp.bfloat16)
            cross_copy(j, u).start()

        @pl.loop(0, units)
        def _(u):
            slot = chip * units + u
            total = attend((2 * chip + core) * units + u)
            terms_copy(slot).wait_recv()
            own_sum[u] = total + partner_terms[slot].astype(jnp.float32)

        line.pump(6)

        for u in range(units):
            here = slice(u * CHUNK, (u + 1) * CHUNK)
            total = residual[here, :].astype(jnp.float32) + own_sum[u]
            for j in range(chips - 1):
                cross_copy(j, u).wait_recv()
                total = total + cross_got[j * units + u].astype(jnp.float32)
            rounded = total.astype(jnp.bfloat16)
            mid[here, :] = rounded
            widened = rounded.astype(jnp.float32)
            inverse = lax.rsqrt(jnp.mean(widened * widened, axis=-1, keepdims=True) + EPS)
            all_rows[rows_at(mine * units + u, CHUNK), :] = (widened * inverse * row_gain[...]).astype(jnp.bfloat16)
            for k in range(len(peers)):
                rows_copy(k, u, mine).start()
            passed_copy(len(peers), u, mine).start()

    pl.run_scoped(
        attention,
        *[pltpu.VMEM(a.shape, a.dtype) for a in in_hbm[:10]],
        pltpu.VMEM((rows, width_a), jnp.float32),
        pltpu.VMEM((rows, width_b), jnp.float32),
        pltpu.VMEM((chunks, DV, width_a), jnp.bfloat16),
        pltpu.VMEM((chunks, DV, width_b), jnp.bfloat16),
        pltpu.VMEM((chunks, 1, width), jnp.float32),
        pltpu.VMEM((2, rows, values_hbm.shape[2]), jnp.float32),
        pltpu.VMEM((units, CHUNK, residual_hbm.shape[1]), jnp.float32),
    )
    line.pump(8)
    for u in range(units):
        for k, peer in enumerate(peers):
            rows_copy(k, u, owner_at(*peer, core)).wait_recv()
            passed_copy(k, u, owner_at(*peer, core)).start()
        line.pump(12 + 2 * u)
    for u in range(units):
        for k, peer in enumerate(peers + [(0, 0)]):
            passed_copy(k, u, owner_at(*peer, 1 - core)).wait_recv()
    line.pump(14)
    ff = hidden.shape[1]
    tile = 256 if ff % 256 == 0 else 128
    tiles = ff // tile
    bands = 2 * chips
    band = 2 * own_rows
    last_pair = line.nth(pairs - 1)
    depth = 2 * shards[0].shape[0]
    late = rows_at(last_pair, depth)
    early = pl.ds(pl.multiple_of(jnp.where(last_pair == 0, depth, 0), depth), (pairs - 1) * depth)

    def first_half(gate_early, up_early):
        def products(n, part):
            lanes, here = rows_at(n // bands, tile), rows_at(n % bands, band)
            gate_sum = dot(all_rows[here, part], gate_full[part, lanes], ((1,), (0,)))
            return lanes, here, gate_sum, dot(all_rows[here, part], up_full[part, lanes], ((1,), (0,)))

        line.arrive_gates(pairs - 2)

        @pl.loop(0, tiles * bands)
        def _(n):
            lanes, here, gate_sum, up_sum = products(n, early)
            gate_early[here, lanes] = gate_sum
            up_early[here, lanes] = up_sum

        line.arrive_gates(pairs - 1)

        @pl.loop(0, tiles * bands)
        def _(n):
            lanes, here, gate_sum, up_sum = products(n, late)
            gate_sum, up_sum = gate_sum + gate_early[here, lanes], up_sum + up_early[here, lanes]
            hidden[here, lanes] = (gate_sum / (1.0 + jnp.exp(-gate_sum)) * up_sum).astype(jnp.bfloat16)

    pl.run_scoped(first_half, *[pltpu.VMEM(hidden.shape, jnp.float32)] * 2)

    columns = shards[2].shape[1]
    direct = columns % 128 == 0
    count = len(peers)

    order = peers[::-1] + [(0, 0)]
    order_bands = [(1 - odd if dy else odd) * chips + (chip + dx) % chips for dy, dx in order]

    blocks = [(b, 0, columns) for b in range(n_sp)]
    if line.split:
        blocks[-1:] = [(n_sp - 1, 0, columns // 2), (n_sp - 1, columns // 2, columns // 2)]
    origins = [2 * line.nth(b // 2) + b % 2 for b in range(n_sp)]

    def lanes_in(b):
        return pl.ds(0, blocks[b][2])

    def half_copy(b, k):
        at = order_bands[k]
        return remote(
            stage.at[b % DEPTH, at, 1 - core, :, lanes_in(b)],
            stage_partner.at[b, at, :, lanes_in(b)],
            half_send.at[b * (count + 1) + k],
            half_receive.at[b * (count + 1) + k],
            partner,
        )

    def last_copy(b, k):
        slot = b * count + k
        return remote(
            stage_cross.at[b % DEPTH * count + k, :, lanes_in(b)],
            stage_got.at[slot, :, lanes_in(b)],
            last_send.at[slot],
            last_receive.at[slot],
            device_at(*order[k]),
        )

    def multiply(b):
        which, start, size = blocks[b]
        for k in range(count + 1):
            if b >= DEPTH:
                half_copy(b - DEPTH, k).wait_send()
            here = rows_at(order_bands[k], band)
            part = down_full[origins[which], :, start : start + size]
            product = dot(hidden[here, :], part, ((1,), (0,))).astype(jnp.bfloat16)
            stage[b % DEPTH, order_bands[k], :, :, :size] = product.reshape(2, own_rows, size)
            half_copy(b, k).start()

    def chip_sum(b, at):
        size = blocks[b][2]
        mine_here = stage[b % DEPTH, at, core, :, :size].astype(jnp.float32)
        return mine_here + stage_partner[b, at, :, :size].astype(jnp.float32)

    def combine(b):
        for k in range(count):
            half_copy(b, k).wait_recv()
            if b >= DEPTH:
                last_copy(b - DEPTH, k).wait_send()
            both = chip_sum(b, order_bands[k]).astype(jnp.bfloat16)
            stage_cross[b % DEPTH * count + k, :, : blocks[b][2]] = both
            last_copy(b, k).start()

    def close(b):
        which, start, size = blocks[b]
        half_copy(b, count).wait_recv()
        total = chip_sum(b, odd * chips + chip)
        for k in range(count):
            last_copy(b, k).wait_recv()
            total = total + stage_got[b * count + k, :, :size].astype(jnp.float32)
        if direct:
            lanes = pl.ds(pl.multiple_of(origins[which] * columns + start, 128), size)
            outs[0][:, lanes] = (mid[:, lanes].astype(jnp.float32) + total).astype(jnp.bfloat16)
        else:
            outs[1][origins[which]] = total

    for b, (which, start, _) in enumerate(blocks):
        hop = which // 2
        if hop:
            piece = which % 2
            if piece and 2 in line.pieces(1, hop):
                piece = 3 if start else 2
            line.arrive(0, 1, hop, piece)
            line.arrive(1, 1, hop, piece)
        multiply(b)
        if b >= 1:
            combine(b - 1)
        line.pump({0: 15, 1: 16, 3: 17, 4: 18}.get(b * 8 // n_sp, 0))
        if b >= 3:
            close(b - 3)
    line.pump(18)
    combine(len(blocks) - 1)
    for b in range(len(blocks) - 3, len(blocks)):
        close(b)
    if not direct:
        outs[0][...] = mid[...]

    line.finish()
    pair_copy().wait_send()
    for k in range(1, pairs):

        @pl.when(pair_place + k < pairs - 1)
        def _():
            to_later(k).wait_send()

    if pairs > 1:

        @pl.when(pair_place == pairs - 2)
        def _():
            to_later(1, 2).wait_send()

    for slot in range(chips * units):
        terms_copy(slot).wait_send()
    for u in range(units):
        for j in range(chips - 1):
            cross_copy(j, u).wait_send()
        for k in range(count):
            rows_copy(k, u, mine).wait_send()
        for k in range(count + 1):
            passed_copy(k, u, mine).wait_send()
    for b in range(len(blocks) - DEPTH, len(blocks)):
        for k in range(count + 1):
            half_copy(b, k).wait_send()
        for k in range(count):
            last_copy(b, k).wait_send()


def per_device(
    residual,
    first_group_queries,
    first_group_keys,
    second_group_queries,
    second_group_keys,
    primary_retain_switch_inputs,
    secondary_retain_switch_inputs,
    timestep_fading_exponent,
    values,
    output_gate_logits,
    head_norm_gains,
    output_projection,
    feedforward_norm_gain,
    gate_projection,
    up_projection,
    down_projection,
):
    n_sp, n_tp = lax.axis_size("sp"), lax.axis_size("tp")
    rows, own_rows = first_group_queries.shape[0], residual.shape[0]
    features = residual.shape[1]
    chunks, units, chips = rows // CHUNK, own_rows // CHUNK, n_tp // 2
    width_a, width_b = first_group_keys.shape[1], second_group_keys.shape[1]
    width = width_a + width_b
    inner, ff = gate_projection.shape
    columns = down_projection.shape[1]
    pairs, crossings, peers = n_sp // 2, max(chips - 1, 1), 2 * chips - 1
    direct = columns % 128 == 0
    blocks = n_sp + 1 if columns % 256 == 0 else n_sp
    projection = output_projection.reshape(-1, features)
    in_hbm = [
        residual,
        first_group_queries,
        second_group_queries,
        first_group_keys,
        second_group_keys,
        primary_retain_switch_inputs,
        secondary_retain_switch_inputs,
        values,
        output_gate_logits,
        projection,
        gate_projection,
        up_projection,
        down_projection,
    ]
    in_vmem = [
        timestep_fading_exponent.reshape(chunks, 1, CHUNK),
        head_norm_gains,
        feedforward_norm_gain.reshape(1, features),
    ]

    def bf16(*shape):
        return pltpu.VMEM(shape, jnp.bfloat16)

    def f32(*shape):
        return pltpu.VMEM(shape, jnp.float32)

    def sems(*shape):
        return pltpu.SemaphoreType.DMA(shape)

    scratch = [bf16(n_sp * inner, ff // 2)] * 2 + [bf16(n_sp, ff // 2, columns)]
    scratch += [f32(DV, width_a), f32(DV, width_b), f32(8, width)]
    scratch += [bf16(3, DV + PAD, width), bf16(DV + PAD, width), bf16(max(n_sp // 2 - 1, 1), DV + PAD, width)]
    scratch += [bf16(chips * units, CHUNK, features)] * 2
    scratch += [bf16(crossings * units, CHUNK, features)] * 2
    scratch += [bf16(2 * rows, features), bf16(2 * rows, ff // 2)]
    scratch += [bf16(DEPTH, 2 * chips, 2, own_rows, columns), bf16(blocks, 2 * chips, own_rows, columns)]
    scratch += [bf16(DEPTH * peers, own_rows, columns), bf16(blocks * peers, own_rows, columns)]
    scratch += [bf16(own_rows, features)]
    scratch += [sems(len(in_hbm)), sems(3), sems(3)]
    scratch += [sems(2, max(pairs - 1, 1), 4)] * 4
    scratch += [sems(2), sems(max(n_sp // 2 - 1, 1)), sems(max(n_sp // 2 - 1, 1))]
    scratch += [sems(chips * units)] * 2
    scratch += [sems(crossings * units)] * 2
    scratch += [sems(peers * units)] * 2
    scratch += [sems((peers + 1) * units)] * 2
    scratch += [sems(blocks * (peers + 1))] * 2
    scratch += [sems(blocks * peers)] * 2
    outs = [bf16(own_rows, features)] if direct else [bf16(own_rows, features), f32(n_sp, own_rows, columns)]
    outs = pl.pallas_call(
        functools.partial(layer_kernel, n_sp, n_tp),
        in_specs=[pl.BlockSpec(memory_space=pl.ANY)] * len(in_hbm)
        + [pl.BlockSpec(memory_space=pltpu.VMEM)] * len(in_vmem),
        out_specs=[pl.BlockSpec(memory_space=pltpu.VMEM)] * len(outs),
        out_shape=outs,
        scratch_shapes=scratch,
        compiler_params=pltpu.CompilerParams(
            collective_id=0, has_side_effects=True, vmem_limit_bytes=VMEM_BYTES
        ),
        name="layer",
    )(*in_hbm, *in_vmem)
    if direct:
        return outs[0]
    added = outs[1].transpose(1, 0, 2).reshape(own_rows, features)
    return (outs[0].astype(jnp.float32) + added).astype(jnp.bfloat16)


def solution(mesh):
    return jax.shard_map(
        per_device,
        mesh=mesh,
        in_specs=(
            P(("sp", "tp"), None),
            P("sp", "tp"),
            P("sp", "tp"),
            P("sp", "tp"),
            P("sp", "tp"),
            P("sp", "tp"),
            P("sp", "tp"),
            P("sp"),
            P(None, "sp", "tp"),
            P(None, "sp", "tp"),
            P(None, "tp"),
            P(None, "tp", None),
            P(),
            P("sp", "tp"),
            P("sp", "tp"),
            P("tp", "sp"),
        ),
        out_specs=P(("sp", "tp"), None),
        check_vma=False,
    )
```

```python
import functools

import jax
import jax.numpy as jnp
from jax import lax
from jax.experimental import pallas as pl
from jax.experimental.pallas import tpu as pltpu
from jax.sharding import PartitionSpec as P

FIRST_KEY_SIZE = 128
SECOND_KEY_SIZE = 64
DV = 128
CHUNK = 128
MIDDLE = CHUNK // 2 - 1
PAD = 16
MESH = pl.DeviceIdType.MESH

EPS = 1e-06
SOFTNESS_SCALE = 16.0
VMEM_BYTES = 62_000_000
DEPTH = 4

def dot(a, b, dims):
    return lax.dot_general(a, b, (dims, ((), ())), preferred_element_type=jnp.float32)


def positions():
    row = lax.broadcasted_iota(jnp.int32, (CHUNK, CHUNK), 0)
    column = lax.broadcasted_iota(jnp.int32, (CHUNK, CHUNK), 1)
    return row, column


def fading_sums(fading_row):
    row, column = positions()
    as_column = jnp.sum(jnp.where(row == column, fading_row, 0.0), axis=1, keepdims=True)
    column_sums = jnp.sum(jnp.where(column <= row, fading_row, 0.0), axis=1, keepdims=True)
    row_sums = jnp.sum(jnp.where(row <= column, as_column, 0.0), axis=0, keepdims=True)
    return column_sums, row_sums


def channel_sums(switches):
    row, column = positions()
    x = switches.astype(jnp.float32)
    logs = (jnp.minimum(x, 0.0) - jnp.log1p(jnp.exp(-jnp.abs(x)))) * (1.0 / SOFTNESS_SCALE)
    lower = (column <= row).astype(jnp.bfloat16)
    high = logs.astype(jnp.bfloat16)
    low = (logs - high.astype(jnp.float32)).astype(jnp.bfloat16)
    return dot(lower, high, ((1,), (0,))) + dot(lower, low, ((1,), (0,)))


def lanes_of(head, width, key_width):
    lane = lax.broadcasted_iota(jnp.int32, (1, width), 1)
    return (lane >= head * key_width) & (lane < (head + 1) * key_width)


def advanced(state, inverse_keys, weighted, sums, total_fading, key_width):
    width = state.shape[1]
    end, middle = sums[CHUNK - 1 :, :], sums[MIDDLE : MIDDLE + 1, :]
    head_count = width // key_width
    if key_width % 128 == 0:
        added = jnp.concatenate(
            [
                dot(
                    weighted[:, h * DV : (h + 1) * DV],
                    inverse_keys[:, h * key_width : (h + 1) * key_width],
                    ((0,), (0,)),
                )
                for h in range(head_count)
            ],
            axis=1,
        )
    else:
        added = jnp.zeros((DV, width), jnp.float32)
        for h in range(head_count):
            product = dot(weighted[:, h * DV : (h + 1) * DV], inverse_keys, ((0,), (0,)))
            added = jnp.where(lanes_of(h, width, key_width), product, added)
    return jnp.exp(end + total_fading) * state + jnp.exp(end - middle) * added


def remote(source, target, send, receive, device):
    return pltpu.make_async_remote_copy(
        src_ref=source,
        dst_ref=target,
        send_sem=send,
        recv_sem=receive,
        device_id=device,
        device_id_type=MESH,
    )


def rows_at(index, count):
    return pl.ds(pl.multiple_of(index * count, count), count)


class Line:
    def __init__(self, pairs, place, tp_place, whole, shards, sems, mate_sems):
        self.pairs, self.place, self.tp_place = pairs, place, tp_place
        self.pair, self.side = place // 2, place % 2
        self.gate, self.up, self.down = whole
        self.shards = shards
        self.sems, self.mate_sems = sems, mate_sems
        self.inner, self.half = shards[0].shape[0], shards[2].shape[0] // 2
        self.waited = set()
        self.issued = [0, 0]
        self.split = self.down.shape[2] % 256 == 0
        self.events = [
            (matrix, hop, piece)
            for matrix in (0, 1)
            for hop in range(1, pairs)
            for piece in self.pieces(matrix, hop)
        ]

    def pieces(self, matrix, hop):
        if not matrix:
            return range(4)
        return (0, 2, 3) if hop == self.pairs - 1 and self.split else (0, 1)

    def shard(self, kind, side):
        half = rows_at(side, self.half)
        return self.shards[kind].at[half, :] if kind == 2 else self.shards[kind].at[:, half]

    def landing(self, kind, origin):
        if kind == 2:
            return self.down.at[origin]
        return (self.up if kind else self.gate).at[rows_at(origin, self.inner), :]

    def own(self, kind):
        return self.shard(kind, self.side), self.landing(kind, self.place)

    def mate_copy(self, kind):
        return remote(
            self.shard(kind, 1 - self.side),
            self.landing(kind, self.place),
            self.mate_sems[0].at[kind],
            self.mate_sems[1].at[kind],
            (self.place + 1 - 2 * self.side, self.tp_place),
        )

    def arrive_mate(self, kind):
        if ("mate", kind) not in self.waited:
            self.waited.add(("mate", kind))
            self.mate_copy(kind).wait_recv()

    def reaches(self, way, distance):
        return self.pair + distance < self.pairs if way else self.pair >= distance

    def copy(self, way, matrix, hop, piece, distance):
        pair = (self.pair + (distance if way else -distance) + self.pairs) % self.pairs
        if matrix and piece >= 2:
            half = self.down.shape[2] // 2
            ref = self.down.at[2 * pair + 1, :, pl.ds((piece - 2) * half, half)]
        elif matrix:
            ref = self.landing(2, 2 * pair + piece)
        else:
            ref = self.landing(piece % 2, 2 * pair + (self.side if piece < 2 else 1 - self.side))
        send, receive = self.sems[matrix]
        at = (way, hop - 1, piece)
        beyond = (self.place + (-2 if way else 2) + 2 * self.pairs) % (2 * self.pairs)
        return remote(ref, ref, send.at[at], receive.at[at], (beyond, self.tp_place))

    def arrive(self, way, matrix, hop, piece):
        if (way, matrix, hop, piece) not in self.waited:
            self.waited.add((way, matrix, hop, piece))

            @pl.when(self.reaches(way, hop))
            def _():
                self.copy(way, matrix, hop, piece, hop).wait_recv()

    def passes(self, way, hop):
        return self.reaches(way, hop - 1) & self.reaches(1 - way, 1)

    def pump(self, until, ways=(0, 1), also=True):
        count = 6 * (self.pairs - 1)
        until = len(self.events) if until >= 18 else (until * count + 17) // 18
        for way in ways:
            for matrix, hop, piece in self.events[self.issued[way] : until]:
                if hop == 1 and (matrix or piece >= 2):
                    self.arrive_mate(2 if matrix else piece % 2)
                if hop > 1:
                    self.arrive(way, matrix, hop - 1, 1 if matrix and piece else piece)

                @pl.when(self.passes(way, hop) & also)
                def _():
                    self.copy(way, matrix, hop, piece, hop - 1).start()

            self.issued[way] = max(until, self.issued[way])

    def arrive_gates(self, until):
        for hop in range(1, until + 1):
            for piece in range(4):
                for way in (0, 1):
                    self.arrive(way, 0, hop, piece)

    def nth(self, q):
        low, high = self.pair, self.pairs - 1 - self.pair
        both = jnp.minimum(low, high)
        near = self.pair + ((q // 2) if q % 2 == 0 else -((q + 1) // 2))
        far = jnp.where(low > high, self.pair - (q - both), self.pair + (q - both))
        return jnp.where(q <= 2 * both, near, far)

    def finish(self):
        for kind in range(3):
            self.mate_copy(kind).wait_send()
        for matrix, hop, piece in self.events:
            for way in (0, 1):

                @pl.when(self.passes(way, hop))
                def _():
                    self.copy(way, matrix, hop, piece, hop - 1).wait_send()


def layer_kernel(
    n_sp,
    n_tp,
    residual_hbm,
    qa_hbm,
    qb_hbm,
    ka_hbm,
    kb_hbm,
    sa_hbm,
    sb_hbm,
    values_hbm,
    gates_hbm,
    projection_hbm,
    gate_hbm,
    up_hbm,
    down_hbm,
    fading,
    gains,
    row_gain,
    *others,
):
    outs, scratch = (others[:1], others[1:]) if down_hbm.shape[1] % 128 == 0 else (others[:2], others[2:])
    layer_body(
        n_sp,
        n_tp,
        (
            residual_hbm,
            qa_hbm,
            qb_hbm,
            ka_hbm,
            kb_hbm,
            sa_hbm,
            sb_hbm,
            values_hbm,
            gates_hbm,
            projection_hbm,
            gate_hbm,
            up_hbm,
            down_hbm,
        ),
        fading,
        gains,
        row_gain,
        outs,
        *scratch,
    )


def layer_body(
    n_sp,
    n_tp,
    in_hbm,
    fading,
    gains,
    row_gain,
    outs,
    gate_full,
    up_full,
    down_full,
    state_a,
    state_b,
    decay,
    packs,
    pair_got,
    later_got,
    terms,
    partner_terms,
    cross_terms,
    cross_got,
    all_rows,
    hidden,
    stage,
    stage_partner,
    stage_cross,
    stage_got,
    mid,
    load_sems,
    mate_send,
    mate_receive,
    gate_send,
    gate_receive,
    down_send,
    down_receive,
    pair_sems,
    later_send,
    later_receive,
    terms_send,
    terms_receive,
    cross_send,
    cross_receive,
    rows_send,
    rows_receive,
    passed_send,
    passed_receive,
    half_send,
    half_receive,
    last_send,
    last_receive,
):
    residual_hbm, qa_hbm, qb_hbm, ka_hbm, kb_hbm, sa_hbm, sb_hbm, values_hbm, gates_hbm, projection_hbm = in_hbm[:10]
    shards = in_hbm[10:]
    place, tp_place = lax.axis_index("sp"), lax.axis_index("tp")
    chip, core = tp_place // 2, tp_place % 2
    chips = n_tp // 2
    partner = (place, 2 * chip + 1 - core)
    rows, own_rows = qa_hbm.shape[0], residual_hbm.shape[0]
    chunks, units = rows // CHUNK, own_rows // CHUNK
    width_a, width_b = ka_hbm.shape[1], kb_hbm.shape[1]
    width = width_a + width_b
    odd = place % 2
    mate = place + 1 - 2 * odd
    pairs, pair_place = n_sp // 2, place // 2
    line = Line(
        pairs,
        place,
        tp_place,
        (gate_full, up_full, down_full),
        shards,
        ((gate_send, gate_receive), (down_send, down_receive)),
        (mate_send, mate_receive),
    )

    barrier = pltpu.get_barrier_semaphore()
    for k in range(1, n_sp):
        pl.semaphore_signal(
            barrier, inc=1, device_id=((place + k) % n_sp, tp_place), device_id_type=MESH
        )
    for k in range(1, n_tp):
        pl.semaphore_signal(
            barrier, inc=1, device_id=(place, (tp_place + k) % n_tp), device_id_type=MESH
        )

    for k in range(1, chips):
        pl.semaphore_signal(
            barrier,
            inc=1,
            device_id=(mate, 2 * ((chip + k) % chips) + core),
            device_id_type=MESH,
        )

    def pair_copy():
        return remote(packs.at[0], pair_got, pair_sems.at[0], pair_sems.at[1], (mate, tp_place))

    def to_later(k, slot=1):
        return remote(
            packs.at[slot],
            later_got.at[k - 1],
            later_send.at[k - 1],
            later_receive.at[k - 1],
            ((place + 2 * k) % n_sp, tp_place),
        )

    def chip_at(k):
        return (chip + 1 + k) % chips

    def terms_copy(slot):
        return remote(
            terms.at[slot], partner_terms.at[slot], terms_send.at[slot], terms_receive.at[slot], partner
        )

    def cross_copy(j, u):
        slot = j * units + u
        return remote(
            cross_terms.at[slot],
            cross_got.at[slot],
            cross_send.at[slot],
            cross_receive.at[slot],
            (place, 2 * chip_at(j) + core),
        )

    peers = [(dy, dx) for dy in (0, 1) for dx in range(chips) if dy or dx]

    def device_at(dy, dx):
        return (mate if dy else place, 2 * ((chip + dx) % chips) + core)

    def owner_at(dy, dx, of_core):
        side = 1 - odd if dy else odd
        return side * n_tp + 2 * ((chip - dx + chips) % chips) + of_core

    def own_at(owner, u):
        return all_rows.at[rows_at(owner * units + u, CHUNK), :]

    def rows_copy(k, u, owner):
        slot = k * units + u
        ref = own_at(owner, u)
        return remote(ref, ref, rows_send.at[slot], rows_receive.at[slot], device_at(*peers[k]))

    def passed_copy(k, u, owner):
        slot = k * units + u
        ref = own_at(owner, u)
        return remote(ref, ref, passed_send.at[slot], passed_receive.at[slot], partner)

    mine = owner_at(0, 0, core)
    def attention(
        residual,
        qa,
        qb,
        ka,
        kb,
        sa,
        sb,
        values,
        gates,
        projection,
        sums_a,
        sums_b,
        before_a,
        before_b,
        starts,
        heads,
        own_sum,
    ):
        groups = (
            (qa, ka, sa, sums_a, before_a, state_a, FIRST_KEY_SIZE, 0),
            (qb, kb, sb, sums_b, before_b, state_b, SECOND_KEY_SIZE, width_a),
        )

        loads = [
            line.own(0),
            line.own(1),
            (ka_hbm, ka),
            (kb_hbm, kb),
            (sa_hbm, sa),
            (sb_hbm, sb),
            (values_hbm, values),
            (qa_hbm, qa),
            (qb_hbm, qb),
            line.own(2),
            (projection_hbm, projection),
            (gates_hbm, gates),
            (residual_hbm, residual),
        ]
        loads = [pltpu.make_async_copy(a, b, load_sems.at[i]) for i, (a, b) in enumerate(loads)]
        for load in loads:
            load.start()
        state_a[...] = jnp.zeros_like(state_a)
        state_b[...] = jnp.zeros_like(state_b)
        decay[...] = jnp.zeros_like(decay)
        loads[0].wait()
        loads[1].wait()
        pl.semaphore_wait(barrier, n_sp + n_tp + chips - 3)
        line.pump(1)
        for load in loads[2:7]:
            load.wait()

        @pl.loop(0, chunks)
        def _(i):
            here = rows_at(i, CHUNK)
            column_sums, _ = fading_sums(fading[i])
            total_fading = column_sums[CHUNK - 1 :, :]
            later = jnp.exp(total_fading - column_sums)
            for group, (_, keys, switches, kept, before, state, key_width, start) in enumerate(groups):
                mine = slice(start, start + keys.shape[1])
                sums = channel_sums(switches[here, :])
                kept[here, :] = sums
                middle = sums[MIDDLE : MIDDLE + 1, :]
                inverse_keys = (keys[here, :].astype(jnp.float32) * jnp.exp(middle - sums)).astype(jnp.bfloat16)
                keys[here, :] = inverse_keys
                before[i] = (state[...] * jnp.exp(middle)).astype(jnp.bfloat16)
                starts[i, :, mine] = jnp.exp(decay[:1, mine] + middle)
                weighted = (values[group, here, :].astype(jnp.float32) * later).astype(jnp.bfloat16)
                state[...] = advanced(state[...], inverse_keys, weighted, sums, total_fading, key_width)
                decay[:, mine] += sums[CHUNK - 1 :, :] + total_fading

        def pack(slot, first, second, factor):
            packs[slot, :DV, :width_a] = first.astype(jnp.bfloat16)
            packs[slot, :DV, width_a:] = second.astype(jnp.bfloat16)
            packs[slot, DV:, :] = jnp.broadcast_to(factor, (PAD, width)).astype(jnp.bfloat16)

        whole_decay = jnp.exp(decay[:1, :])
        pack(0, state_a[...], state_b[...], whole_decay)
        pair_copy().start()
        line.mate_copy(0).start()
        line.mate_copy(1).start()
        line.pump(2, (1,))
        calm = pair_place >= pairs - 2
        line.pump(2, (0,), calm)
        pair_copy().wait_recv()
        got = pair_got[...].astype(jnp.float32)
        got_a, got_b, got_decay = got[:DV, :width_a], got[:DV, width_a:], got[DV : DV + 1, :]
        is_odd = odd == 1
        pair_a = jnp.where(
            is_odd,
            whole_decay[:, :width_a] * got_a + state_a[...],
            got_decay[:, :width_a] * state_a[...] + got_a,
        )
        pair_b = jnp.where(
            is_odd,
            whole_decay[:, width_a:] * got_b + state_b[...],
            got_decay[:, width_a:] * state_b[...] + got_b,
        )
        pack(1, pair_a, pair_b, whole_decay * got_decay)
        for k in range(1, pairs):

            @pl.when(pair_place + k < pairs - 1)
            def _():
                to_later(k).start()

        line.issued[0] = 1
        line.pump(2, (0,), ~calm)
        line.mate_copy(2).start()
        loads[9].wait()
        loads[7].wait()
        loads[8].wait()

        row, column = positions()
        causal = column <= row

        @pl.loop(0, chunks)
        def _(i):
            here = rows_at(i, CHUNK)
            column_sums, row_sums = fading_sums(fading[i])
            since_start = jnp.exp(column_sums)
            between = jnp.where(causal, jnp.exp(jnp.minimum(column_sums - row_sums, 0.0)), 0.0)
            for group, (queries, keys, _, kept, before, _, key_width, _) in enumerate(groups):
                sums = kept[here, :]
                middle = sums[MIDDLE : MIDDLE + 1, :]
                spread = queries[here, :].astype(jnp.float32) * (jnp.exp(sums - middle) * key_width**-0.5)
                scaled = spread.astype(jnp.bfloat16)
                queries[here, :] = (spread * since_start).astype(jnp.bfloat16)
                inverse_keys = keys[here, :]
                local = before[i]
                for h in range(keys.shape[1] // key_width):
                    if key_width % 128 == 0:
                        mine = slice(h * key_width, (h + 1) * key_width)
                        q, k, s = scaled[:, mine], inverse_keys[:, mine], local[:, mine]
                    else:
                        q = jnp.where(lanes_of(h, keys.shape[1], key_width), scaled, jnp.zeros_like(scaled))
                        k, s = inverse_keys, local
                    scores = jnp.where(causal, dot(q, k, ((1,), (1,))) * between, 0.0).astype(jnp.bfloat16)
                    head = dot(scores, values[group, here, h * DV : (h + 1) * DV], ((1,), (0,)))
                    heads[group, here, h * DV : (h + 1) * DV] = head + since_start * dot(q, s, ((1,), (1,)))

        state_a[...] = jnp.zeros_like(state_a)
        state_b[...] = jnp.zeros_like(state_b)

        def follow(slot):
            part = slot[...].astype(jnp.float32)
            factor = part[DV : DV + 1, :]
            state_a[...] = factor[:, :width_a] * state_a[...] + part[:DV, :width_a]
            state_b[...] = factor[:, width_a:] * state_b[...] + part[:DV, width_a:]

        for k in range(pairs - 2, 0, -1):

            @pl.when((pair_place >= k) & (pair_place < pairs - 1))
            def _():
                to_later(k).wait_recv()
                follow(later_got.at[k - 1])

        if pairs > 1:

            @pl.when(pair_place == pairs - 2)
            def _():
                part = packs[1].astype(jnp.float32)
                factor = part[DV : DV + 1, :]
                pack(
                    2,
                    factor[:, :width_a] * state_a[...] + part[:DV, :width_a],
                    factor[:, width_a:] * state_b[...] + part[:DV, width_a:],
                    factor,
                )
                to_later(1, 2).start()

        line.pump(3)
        if pairs > 1:

            @pl.when(pair_place == pairs - 1)
            def _():
                to_later(1).wait_recv()
                follow(later_got.at[0])

        state_a[...] = jnp.where(is_odd, got_decay[:, :width_a] * state_a[...] + got_a, state_a[...])
        state_b[...] = jnp.where(is_odd, got_decay[:, width_a:] * state_b[...] + got_b, state_b[...])
        for load in loads[10:]:
            load.wait()

        def attend(i):
            here = rows_at(i, CHUNK)
            pieces = []
            for group, (queries, _, _, _, _, state, key_width, start) in enumerate(groups):
                key_lanes = queries.shape[1]
                earlier = (state[...] * starts[i, :, start : start + key_lanes]).astype(jnp.bfloat16)
                scaled = queries[here, :]
                for h in range(key_lanes // key_width):
                    lanes = slice(h * DV, (h + 1) * DV)
                    if key_width % 128 == 0:
                        mine = slice(h * key_width, (h + 1) * key_width)
                        q, s = scaled[:, mine], earlier[:, mine]
                    else:
                        q = jnp.where(lanes_of(h, key_lanes, key_width), scaled, jnp.zeros_like(scaled))
                        s = earlier
                    head = heads[group, here, lanes] + dot(q, s, ((1,), (1,)))
                    inverse = lax.rsqrt(jnp.mean(head * head, axis=-1, keepdims=True) + EPS)
                    gate = gates[group, here, lanes].astype(jnp.float32)
                    silu = gate / (1.0 + jnp.exp(-gate))
                    pieces.append((silu * (head * inverse * gains[group : group + 1, lanes])).astype(jnp.bfloat16))
            return dot(jnp.concatenate(pieces, axis=1), projection[...], ((1,), (0,)))

        @pl.loop(0, chips * units)
        def _(k):
            other, u = chip_at(k // units), k % units
            slot = other * units + u
            terms[slot] = attend((2 * other + 1 - core) * units + u).astype(jnp.bfloat16)
            terms_copy(slot).start()

        @pl.loop(0, (chips - 1) * units)
        def _(k):
            j, u = k // units, k % units
            other = chip_at(j)
            slot = other * units + u
            total = attend((2 * other + core) * units + u)
            terms_copy(slot).wait_recv()
            cross_terms[k] = (total + partner_terms[slot].astype(jnp.float32)).astype(jnp.bfloat16)
            cross_copy(j, u).start()

        @pl.loop(0, units)
        def _(u):
            slot = chip * units + u
            total = attend((2 * chip + core) * units + u)
            terms_copy(slot).wait_recv()
            own_sum[u] = total + partner_terms[slot].astype(jnp.float32)

        line.pump(6)

        for u in range(units):
            here = slice(u * CHUNK, (u + 1) * CHUNK)
            total = residual[here, :].astype(jnp.float32) + own_sum[u]
            for j in range(chips - 1):
                cross_copy(j, u).wait_recv()
                total = total + cross_got[j * units + u].astype(jnp.float32)
            rounded = total.astype(jnp.bfloat16)
            mid[here, :] = rounded
            widened = rounded.astype(jnp.float32)
            inverse = lax.rsqrt(jnp.mean(widened * widened, axis=-1, keepdims=True) + EPS)
            all_rows[rows_at(mine * units + u, CHUNK), :] = (widened * inverse * row_gain[...]).astype(jnp.bfloat16)
            for k in range(len(peers)):
                rows_copy(k, u, mine).start()
            passed_copy(len(peers), u, mine).start()

    pl.run_scoped(
        attention,
        *[pltpu.VMEM(a.shape, a.dtype) for a in in_hbm[:10]],
        pltpu.VMEM((rows, width_a), jnp.float32),
        pltpu.VMEM((rows, width_b), jnp.float32),
        pltpu.VMEM((chunks, DV, width_a), jnp.bfloat16),
        pltpu.VMEM((chunks, DV, width_b), jnp.bfloat16),
        pltpu.VMEM((chunks, 1, width), jnp.float32),
        pltpu.VMEM((2, rows, values_hbm.shape[2]), jnp.float32),
        pltpu.VMEM((units, CHUNK, residual_hbm.shape[1]), jnp.float32),
    )
    line.pump(10)
    for u in range(units):
        for k, peer in enumerate(peers):
            rows_copy(k, u, owner_at(*peer, core)).wait_recv()
            passed_copy(k, u, owner_at(*peer, core)).start()
        line.pump(12 + 2 * u)
    for u in range(units):
        for k, peer in enumerate(peers + [(0, 0)]):
            passed_copy(k, u, owner_at(*peer, 1 - core)).wait_recv()
    line.pump(14)
    ff = hidden.shape[1]
    tile = 256 if ff % 256 == 0 else 128
    tiles = ff // tile
    bands = 2 * chips
    band = 2 * own_rows
    last_pair = line.nth(pairs - 1)
    depth = 2 * shards[0].shape[0]
    late = rows_at(last_pair, depth)
    early = pl.ds(pl.multiple_of(jnp.where(last_pair == 0, depth, 0), depth), (pairs - 1) * depth)

    def first_half(gate_early, up_early):
        def products(n, part):
            lanes, here = rows_at(n // bands, tile), rows_at(n % bands, band)
            gate_sum = dot(all_rows[here, part], gate_full[part, lanes], ((1,), (0,)))
            return lanes, here, gate_sum, dot(all_rows[here, part], up_full[part, lanes], ((1,), (0,)))

        line.arrive_gates(pairs - 2)

        @pl.loop(0, tiles * bands)
        def _(n):
            lanes, here, gate_sum, up_sum = products(n, early)
            gate_early[here, lanes] = gate_sum
            up_early[here, lanes] = up_sum

        line.arrive_gates(pairs - 1)

        @pl.loop(0, tiles * bands)
        def _(n):
            lanes, here, gate_sum, up_sum = products(n, late)
            gate_sum, up_sum = gate_sum + gate_early[here, lanes], up_sum + up_early[here, lanes]
            hidden[here, lanes] = (gate_sum / (1.0 + jnp.exp(-gate_sum)) * up_sum).astype(jnp.bfloat16)

    pl.run_scoped(first_half, *[pltpu.VMEM(hidden.shape, jnp.float32)] * 2)

    columns = shards[2].shape[1]
    direct = columns % 128 == 0
    count = len(peers)

    order = peers[::-1] + [(0, 0)]
    order_bands = [(1 - odd if dy else odd) * chips + (chip + dx) % chips for dy, dx in order]

    blocks = [(b, 0, columns) for b in range(n_sp)]
    if line.split:
        blocks[-1:] = [(n_sp - 1, 0, columns // 2), (n_sp - 1, columns // 2, columns // 2)]
    origins = [2 * line.nth(b // 2) + b % 2 for b in range(n_sp)]

    def lanes_in(b):
        return pl.ds(0, blocks[b][2])

    def half_copy(b, k):
        at = order_bands[k]
        return remote(
            stage.at[b % DEPTH, at, 1 - core, :, lanes_in(b)],
            stage_partner.at[b, at, :, lanes_in(b)],
            half_send.at[b * (count + 1) + k],
            half_receive.at[b * (count + 1) + k],
            partner,
        )

    def last_copy(b, k):
        slot = b * count + k
        return remote(
            stage_cross.at[b % DEPTH * count + k, :, lanes_in(b)],
            stage_got.at[slot, :, lanes_in(b)],
            last_send.at[slot],
            last_receive.at[slot],
            device_at(*order[k]),
        )

    def multiply(b):
        which, start, size = blocks[b]
        for k in range(count + 1):
            if b >= DEPTH:
                half_copy(b - DEPTH, k).wait_send()
            here = rows_at(order_bands[k], band)
            part = down_full[origins[which], :, start : start + size]
            product = dot(hidden[here, :], part, ((1,), (0,))).astype(jnp.bfloat16)
            stage[b % DEPTH, order_bands[k], :, :, :size] = product.reshape(2, own_rows, size)
            half_copy(b, k).start()
            if k >= 2:
                combine(b, k - 2)
        combine(b, count - 1)

    def chip_sum(b, at):
        size = blocks[b][2]
        mine_here = stage[b % DEPTH, at, core, :, :size].astype(jnp.float32)
        return mine_here + stage_partner[b, at, :, :size].astype(jnp.float32)

    def combine(b, k):
        half_copy(b, k).wait_recv()
        if b >= DEPTH:
            last_copy(b - DEPTH, k).wait_send()
        both = chip_sum(b, order_bands[k]).astype(jnp.bfloat16)
        stage_cross[b % DEPTH * count + k, :, : blocks[b][2]] = both
        last_copy(b, k).start()

    def close(b):
        which, start, size = blocks[b]
        half_copy(b, count).wait_recv()
        total = chip_sum(b, odd * chips + chip)
        for k in range(count):
            last_copy(b, k).wait_recv()
            total = total + stage_got[b * count + k, :, :size].astype(jnp.float32)
        if direct:
            lanes = pl.ds(pl.multiple_of(origins[which] * columns + start, 128), size)
            outs[0][:, lanes] = (mid[:, lanes].astype(jnp.float32) + total).astype(jnp.bfloat16)
        else:
            outs[1][origins[which]] = total

    for b, (which, start, _) in enumerate(blocks):
        hop = which // 2
        if hop:
            piece = which % 2
            if piece and 2 in line.pieces(1, hop):
                piece = 3 if start else 2
            line.arrive(0, 1, hop, piece)
            line.arrive(1, 1, hop, piece)
        multiply(b)
        line.pump({0: 15, 1: 16, 3: 17, 4: 18}.get(b * 8 // n_sp, 0))
        if b >= 3:
            close(b - 3)
    line.pump(18)
    for b in range(len(blocks) - 3, len(blocks)):
        close(b)
    if not direct:
        outs[0][...] = mid[...]

    line.finish()
    pair_copy().wait_send()
    for k in range(1, pairs):

        @pl.when(pair_place + k < pairs - 1)
        def _():
            to_later(k).wait_send()

    if pairs > 1:

        @pl.when(pair_place == pairs - 2)
        def _():
            to_later(1, 2).wait_send()

    for slot in range(chips * units):
        terms_copy(slot).wait_send()
    for u in range(units):
        for j in range(chips - 1):
            cross_copy(j, u).wait_send()
        for k in range(count):
            rows_copy(k, u, mine).wait_send()
        for k in range(count + 1):
            passed_copy(k, u, mine).wait_send()
    for b in range(len(blocks) - DEPTH, len(blocks)):
        for k in range(count + 1):
            half_copy(b, k).wait_send()
        for k in range(count):
            last_copy(b, k).wait_send()


def per_device(
    residual,
    first_group_queries,
    first_group_keys,
    second_group_queries,
    second_group_keys,
    primary_retain_switch_inputs,
    secondary_retain_switch_inputs,
    timestep_fading_exponent,
    values,
    output_gate_logits,
    head_norm_gains,
    output_projection,
    feedforward_norm_gain,
    gate_projection,
    up_projection,
    down_projection,
):
    n_sp, n_tp = lax.axis_size("sp"), lax.axis_size("tp")
    rows, own_rows = first_group_queries.shape[0], residual.shape[0]
    features = residual.shape[1]
    chunks, units, chips = rows // CHUNK, own_rows // CHUNK, n_tp // 2
    width_a, width_b = first_group_keys.shape[1], second_group_keys.shape[1]
    width = width_a + width_b
    inner, ff = gate_projection.shape
    columns = down_projection.shape[1]
    pairs, crossings, peers = n_sp // 2, max(chips - 1, 1), 2 * chips - 1
    direct = columns % 128 == 0
    blocks = n_sp + 1 if columns % 256 == 0 else n_sp
    projection = output_projection.reshape(-1, features)
    in_hbm = [
        residual,
        first_group_queries,
        second_group_queries,
        first_group_keys,
        second_group_keys,
        primary_retain_switch_inputs,
        secondary_retain_switch_inputs,
        values,
        output_gate_logits,
        projection,
        gate_projection,
        up_projection,
        down_projection,
    ]
    in_vmem = [
        timestep_fading_exponent.reshape(chunks, 1, CHUNK),
        head_norm_gains,
        feedforward_norm_gain.reshape(1, features),
    ]

    def bf16(*shape):
        return pltpu.VMEM(shape, jnp.bfloat16)

    def f32(*shape):
        return pltpu.VMEM(shape, jnp.float32)

    def sems(*shape):
        return pltpu.SemaphoreType.DMA(shape)

    scratch = [bf16(n_sp * inner, ff // 2)] * 2 + [bf16(n_sp, ff // 2, columns)]
    scratch += [f32(DV, width_a), f32(DV, width_b), f32(8, width)]
    scratch += [bf16(3, DV + PAD, width), bf16(DV + PAD, width), bf16(max(n_sp // 2 - 1, 1), DV + PAD, width)]
    scratch += [bf16(chips * units, CHUNK, features)] * 2
    scratch += [bf16(crossings * units, CHUNK, features)] * 2
    scratch += [bf16(2 * rows, features), bf16(2 * rows, ff // 2)]
    scratch += [bf16(DEPTH, 2 * chips, 2, own_rows, columns), bf16(blocks, 2 * chips, own_rows, columns)]
    scratch += [bf16(DEPTH * peers, own_rows, columns), bf16(blocks * peers, own_rows, columns)]
    scratch += [bf16(own_rows, features)]
    scratch += [sems(len(in_hbm)), sems(3), sems(3)]
    scratch += [sems(2, max(pairs - 1, 1), 4)] * 4
    scratch += [sems(2), sems(max(n_sp // 2 - 1, 1)), sems(max(n_sp // 2 - 1, 1))]
    scratch += [sems(chips * units)] * 2
    scratch += [sems(crossings * units)] * 2
    scratch += [sems(peers * units)] * 2
    scratch += [sems((peers + 1) * units)] * 2
    scratch += [sems(blocks * (peers + 1))] * 2
    scratch += [sems(blocks * peers)] * 2
    outs = [bf16(own_rows, features)] if direct else [bf16(own_rows, features), f32(n_sp, own_rows, columns)]
    outs = pl.pallas_call(
        functools.partial(layer_kernel, n_sp, n_tp),
        in_specs=[pl.BlockSpec(memory_space=pl.ANY)] * len(in_hbm)
        + [pl.BlockSpec(memory_space=pltpu.VMEM)] * len(in_vmem),
        out_specs=[pl.BlockSpec(memory_space=pltpu.VMEM)] * len(outs),
        out_shape=outs,
        scratch_shapes=scratch,
        compiler_params=pltpu.CompilerParams(
            collective_id=0, has_side_effects=True, vmem_limit_bytes=VMEM_BYTES
        ),
        name="layer",
    )(*in_hbm, *in_vmem)
    if direct:
        return outs[0]
    added = outs[1].transpose(1, 0, 2).reshape(own_rows, features)
    return (outs[0].astype(jnp.float32) + added).astype(jnp.bfloat16)


def solution(mesh):
    return jax.shard_map(
        per_device,
        mesh=mesh,
        in_specs=(
            P(("sp", "tp"), None),
            P("sp", "tp"),
            P("sp", "tp"),
            P("sp", "tp"),
            P("sp", "tp"),
            P("sp", "tp"),
            P("sp", "tp"),
            P("sp"),
            P(None, "sp", "tp"),
            P(None, "sp", "tp"),
            P(None, "tp"),
            P(None, "tp", None),
            P(),
            P("sp", "tp"),
            P("sp", "tp"),
            P("tp", "sp"),
        ),
        out_specs=P(("sp", "tp"), None),
        check_vma=False,
    )
```

```python
import functools

import jax
import jax.numpy as jnp
from jax import lax
from jax.experimental import pallas as pl
from jax.experimental.pallas import tpu as pltpu
from jax.sharding import PartitionSpec as P

FIRST_KEY_SIZE = 128
SECOND_KEY_SIZE = 64
DV = 128
CHUNK = 128
MIDDLE = CHUNK // 2 - 1
PAD = 16
MESH = pl.DeviceIdType.MESH

EPS = 1e-06
SOFTNESS_SCALE = 16.0
VMEM_BYTES = 62_000_000
DEPTH = 4
QUEUE = 8

def dot(a, b, dims):
    return lax.dot_general(a, b, (dims, ((), ())), preferred_element_type=jnp.float32)


def positions():
    row = lax.broadcasted_iota(jnp.int32, (CHUNK, CHUNK), 0)
    column = lax.broadcasted_iota(jnp.int32, (CHUNK, CHUNK), 1)
    return row, column


def fading_sums(fading_row):
    row, column = positions()
    as_column = jnp.sum(jnp.where(row == column, fading_row, 0.0), axis=1, keepdims=True)
    column_sums = jnp.sum(jnp.where(column <= row, fading_row, 0.0), axis=1, keepdims=True)
    row_sums = jnp.sum(jnp.where(row <= column, as_column, 0.0), axis=0, keepdims=True)
    return column_sums, row_sums


def channel_sums(switches):
    row, column = positions()
    x = switches.astype(jnp.float32)
    logs = (jnp.minimum(x, 0.0) - jnp.log1p(jnp.exp(-jnp.abs(x)))) * (1.0 / SOFTNESS_SCALE)
    lower = (column <= row).astype(jnp.bfloat16)
    high = logs.astype(jnp.bfloat16)
    low = (logs - high.astype(jnp.float32)).astype(jnp.bfloat16)
    return dot(lower, high, ((1,), (0,))) + dot(lower, low, ((1,), (0,)))


def lanes_of(head, width, key_width):
    lane = lax.broadcasted_iota(jnp.int32, (1, width), 1)
    return (lane >= head * key_width) & (lane < (head + 1) * key_width)


def advanced(state, inverse_keys, weighted, sums, total_fading, key_width):
    width = state.shape[1]
    end, middle = sums[CHUNK - 1 :, :], sums[MIDDLE : MIDDLE + 1, :]
    head_count = width // key_width
    if key_width % 128 == 0:
        added = jnp.concatenate(
            [
                dot(
                    weighted[:, h * DV : (h + 1) * DV],
                    inverse_keys[:, h * key_width : (h + 1) * key_width],
                    ((0,), (0,)),
                )
                for h in range(head_count)
            ],
            axis=1,
        )
    else:
        added = jnp.zeros((DV, width), jnp.float32)
        for h in range(head_count):
            product = dot(weighted[:, h * DV : (h + 1) * DV], inverse_keys, ((0,), (0,)))
            added = jnp.where(lanes_of(h, width, key_width), product, added)
    return jnp.exp(end + total_fading) * state + jnp.exp(end - middle) * added


def remote(source, target, send, receive, device):
    return pltpu.make_async_remote_copy(
        src_ref=source,
        dst_ref=target,
        send_sem=send,
        recv_sem=receive,
        device_id=device,
        device_id_type=MESH,
    )


def rows_at(index, count):
    return pl.ds(pl.multiple_of(index * count, count), count)


class Line:
    def __init__(self, pairs, place, tp_place, whole, shards, sems, mate_sems):
        self.pairs, self.place, self.tp_place = pairs, place, tp_place
        self.pair, self.side = place // 2, place % 2
        self.gate, self.up, self.down = whole
        self.shards = shards
        self.sems, self.mate_sems = sems, mate_sems
        self.inner, self.half = shards[0].shape[0], shards[2].shape[0] // 2
        self.waited = set()
        self.issued = [0, 0]
        self.split = self.down.shape[2] % 256 == 0
        self.events = [
            (matrix, hop, piece)
            for matrix in (0, 1)
            for hop in range(1, pairs)
            for piece in self.pieces(matrix, hop)
        ]

    def pieces(self, matrix, hop):
        if not matrix:
            return range(4)
        return (0, 2, 3) if hop == self.pairs - 1 and self.split else (0, 1)

    def shard(self, kind, side):
        half = rows_at(side, self.half)
        return self.shards[kind].at[half, :] if kind == 2 else self.shards[kind].at[:, half]

    def landing(self, kind, origin):
        if kind == 2:
            return self.down.at[origin]
        return (self.up if kind else self.gate).at[rows_at(origin, self.inner), :]

    def own(self, kind):
        return self.shard(kind, self.side), self.landing(kind, self.place)

    def mate_copy(self, kind):
        return remote(
            self.shard(kind, 1 - self.side),
            self.landing(kind, self.place),
            self.mate_sems[0].at[kind],
            self.mate_sems[1].at[kind],
            (self.place + 1 - 2 * self.side, self.tp_place),
        )

    def arrive_mate(self, kind):
        if ("mate", kind) not in self.waited:
            self.waited.add(("mate", kind))
            self.mate_copy(kind).wait_recv()

    def reaches(self, way, distance):
        return self.pair + distance < self.pairs if way else self.pair >= distance

    def copy(self, way, matrix, hop, piece, distance):
        pair = (self.pair + (distance if way else -distance) + self.pairs) % self.pairs
        if matrix and piece >= 2:
            half = self.down.shape[2] // 2
            ref = self.down.at[2 * pair + 1, :, pl.ds((piece - 2) * half, half)]
        elif matrix:
            ref = self.landing(2, 2 * pair + piece)
        else:
            ref = self.landing(piece % 2, 2 * pair + (self.side if piece < 2 else 1 - self.side))
        number = self.events.index((matrix, hop, piece))
        send, receive = self.sems[0].at[way, number % QUEUE], self.sems[1].at[way, number]
        beyond = (self.place + (-2 if way else 2) + 2 * self.pairs) % (2 * self.pairs)
        return remote(ref, ref, send, receive, (beyond, self.tp_place))

    def arrive(self, way, matrix, hop, piece):
        if (way, matrix, hop, piece) not in self.waited:
            self.waited.add((way, matrix, hop, piece))

            @pl.when(self.reaches(way, hop))
            def _():
                self.copy(way, matrix, hop, piece, hop).wait_recv()

    def passes(self, way, hop):
        return self.reaches(way, hop - 1) & self.reaches(1 - way, 1)

    def pump(self, until, ways=(0, 1), also=True):
        count = 6 * (self.pairs - 1)
        until = len(self.events) if until >= 18 else (until * count + 17) // 18
        for way in ways:
            for number in range(self.issued[way], until):
                matrix, hop, piece = self.events[number]
                if hop == 1 and (matrix or piece >= 2):
                    self.arrive_mate(2 if matrix else piece % 2)
                if hop > 1:
                    self.arrive(way, matrix, hop - 1, 1 if matrix and piece else piece)

                self.left(way, number - QUEUE)

                @pl.when(self.passes(way, hop) & also)
                def _():
                    self.copy(way, matrix, hop, piece, hop - 1).start()

            self.issued[way] = max(until, self.issued[way])

    def arrive_gates(self, until):
        for hop in range(1, until + 1):
            for piece in range(4):
                for way in (0, 1):
                    self.arrive(way, 0, hop, piece)

    def nth(self, q):
        low, high = self.pair, self.pairs - 1 - self.pair
        both = jnp.minimum(low, high)
        near = self.pair + ((q // 2) if q % 2 == 0 else -((q + 1) // 2))
        far = jnp.where(low > high, self.pair - (q - both), self.pair + (q - both))
        return jnp.where(q <= 2 * both, near, far)

    def finish(self):
        for kind in range(3):
            self.mate_copy(kind).wait_send()
        for number in range(len(self.events)):
            for way in (0, 1):
                self.left(way, number)

    def left(self, way, number):
        if number >= 0 and ("left", way, number) not in self.waited:
            self.waited.add(("left", way, number))
            matrix, hop, piece = self.events[number]

            @pl.when(self.passes(way, hop))
            def _():
                self.copy(way, matrix, hop, piece, hop - 1).wait_send()


def layer_kernel(n_sp, n_tp, in_count, out_count, *refs):
    layer_body(n_sp, n_tp, refs[:in_count], refs[in_count : in_count + out_count], *refs[in_count + out_count :])


def layer_body(
    n_sp,
    n_tp,
    in_hbm,
    outs,
    gate_full,
    up_full,
    down_full,
    state_a,
    state_b,
    decay,
    packs,
    pair_got,
    later_got,
    terms,
    partner_terms,
    cross_terms,
    cross_got,
    all_rows,
    hidden,
    stage,
    stage_partner,
    stage_cross,
    stage_got,
    mid,
    load_sems,
    mate_send,
    mate_receive,
    line_send,
    line_receive,
    pair_sems,
    later_send,
    later_receive,
    terms_send,
    terms_receive,
    cross_send,
    cross_receive,
    rows_send,
    rows_receive,
    passed_send,
    passed_receive,
    half_send,
    half_receive,
    last_send,
    last_receive,
):
    residual_hbm, qa_hbm, qb_hbm, ka_hbm, kb_hbm, sa_hbm, sb_hbm, values_hbm, gates_hbm, projection_hbm = in_hbm[:10]
    shards = in_hbm[10:13]
    fading_hbm, gains_hbm, row_gain_hbm = in_hbm[13:]
    place, tp_place = lax.axis_index("sp"), lax.axis_index("tp")
    chip, core = tp_place // 2, tp_place % 2
    chips = n_tp // 2
    partner = (place, 2 * chip + 1 - core)
    rows, own_rows = qa_hbm.shape[0], residual_hbm.shape[0]
    chunks, units = rows // CHUNK, own_rows // CHUNK
    width_a, width_b = ka_hbm.shape[1], kb_hbm.shape[1]
    width = width_a + width_b
    odd = place % 2
    mate = place + 1 - 2 * odd
    pairs, pair_place = n_sp // 2, place // 2
    line = Line(
        pairs,
        place,
        tp_place,
        (gate_full, up_full, down_full),
        shards,
        (line_send, line_receive),
        (mate_send, mate_receive),
    )

    barrier = pltpu.get_barrier_semaphore()
    for k in range(1, n_sp):
        pl.semaphore_signal(
            barrier, inc=1, device_id=((place + k) % n_sp, tp_place), device_id_type=MESH
        )
    for k in range(1, n_tp):
        pl.semaphore_signal(
            barrier, inc=1, device_id=(place, (tp_place + k) % n_tp), device_id_type=MESH
        )

    for k in range(1, chips):
        pl.semaphore_signal(
            barrier,
            inc=1,
            device_id=(mate, 2 * ((chip + k) % chips) + core),
            device_id_type=MESH,
        )

    def pair_copy():
        return remote(packs.at[0], pair_got, pair_sems.at[0], pair_sems.at[1], (mate, tp_place))

    def to_later(k, slot=1):
        return remote(
            packs.at[slot],
            later_got.at[k - 1],
            later_send.at[k - 1],
            later_receive.at[k - 1],
            ((place + 2 * k) % n_sp, tp_place),
        )

    def chip_at(k):
        return (chip + 1 + k) % chips

    def terms_copy(slot):
        return remote(
            terms.at[slot], partner_terms.at[slot], terms_send.at[slot], terms_receive.at[slot], partner
        )

    def cross_copy(j, u):
        slot = j * units + u
        return remote(
            cross_terms.at[slot],
            cross_got.at[slot],
            cross_send.at[slot],
            cross_receive.at[slot],
            (place, 2 * chip_at(j) + core),
        )

    peers = [(dy, dx) for dy in (0, 1) for dx in range(chips) if dy or dx]

    def device_at(dy, dx):
        return (mate if dy else place, 2 * ((chip + dx) % chips) + core)

    def owner_at(dy, dx, of_core):
        side = 1 - odd if dy else odd
        return side * n_tp + 2 * ((chip - dx + chips) % chips) + of_core

    def own_at(owner, u):
        return all_rows.at[rows_at(owner * units + u, CHUNK), :]

    def rows_copy(k, u, owner):
        slot = k * units + u
        ref = own_at(owner, u)
        return remote(ref, ref, rows_send.at[slot], rows_receive.at[slot], device_at(*peers[k]))

    def passed_copy(k, u, owner):
        slot = k * units + u
        ref = own_at(owner, u)
        return remote(ref, ref, passed_send.at[slot], passed_receive.at[slot], partner)

    mine = owner_at(0, 0, core)
    def attention(
        residual,
        qa,
        qb,
        ka,
        kb,
        sa,
        sb,
        values,
        gates,
        projection,
        sums_a,
        sums_b,
        before_a,
        before_b,
        starts,
        heads,
        own_sum,
        fading,
        gains,
        row_gain,
    ):
        groups = (
            (qa, ka, sa, sums_a, before_a, state_a, FIRST_KEY_SIZE, 0),
            (qb, kb, sb, sums_b, before_b, state_b, SECOND_KEY_SIZE, width_a),
        )

        loads = [
            line.own(0),
            line.own(1),
            (fading_hbm, fading),
            (ka_hbm, ka),
            (kb_hbm, kb),
            (sa_hbm, sa),
            (sb_hbm, sb),
            (values_hbm, values),
            (qa_hbm, qa),
            (qb_hbm, qb),
            line.own(2),
            (projection_hbm, projection),
            (gates_hbm, gates),
            (residual_hbm, residual),
            (gains_hbm, gains),
            (row_gain_hbm, row_gain),
        ]
        loads = [pltpu.make_async_copy(a, b, load_sems.at[i]) for i, (a, b) in enumerate(loads)]
        for load in loads:
            load.start()
        state_a[...] = jnp.zeros_like(state_a)
        state_b[...] = jnp.zeros_like(state_b)
        decay[...] = jnp.zeros_like(decay)
        loads[0].wait()
        loads[1].wait()
        pl.semaphore_wait(barrier, n_sp + n_tp + chips - 3)
        line.pump(1)
        for load in loads[2:8]:
            load.wait()

        @pl.loop(0, chunks)
        def _(i):
            here = rows_at(i, CHUNK)
            column_sums, _ = fading_sums(fading[i])
            total_fading = column_sums[CHUNK - 1 :, :]
            later = jnp.exp(total_fading - column_sums)
            for group, (_, keys, switches, kept, before, state, key_width, start) in enumerate(groups):
                mine = slice(start, start + keys.shape[1])
                sums = channel_sums(switches[here, :])
                kept[here, :] = sums
                middle = sums[MIDDLE : MIDDLE + 1, :]
                inverse_keys = (keys[here, :].astype(jnp.float32) * jnp.exp(middle - sums)).astype(jnp.bfloat16)
                keys[here, :] = inverse_keys
                before[i] = (state[...] * jnp.exp(middle)).astype(jnp.bfloat16)
                starts[i, :, mine] = jnp.exp(decay[:1, mine] + middle)
                weighted = (values[group, here, :].astype(jnp.float32) * later).astype(jnp.bfloat16)
                state[...] = advanced(state[...], inverse_keys, weighted, sums, total_fading, key_width)
                decay[:, mine] += sums[CHUNK - 1 :, :] + total_fading

        def pack(slot, first, second, factor):
            packs[slot, :DV, :width_a] = first.astype(jnp.bfloat16)
            packs[slot, :DV, width_a:] = second.astype(jnp.bfloat16)
            packs[slot, DV:, :] = jnp.broadcast_to(factor, (PAD, width)).astype(jnp.bfloat16)

        whole_decay = jnp.exp(decay[:1, :])
        pack(0, state_a[...], state_b[...], whole_decay)
        pair_copy().start()
        line.mate_copy(0).start()
        line.mate_copy(1).start()
        line.pump(2, (1,))
        calm = pair_place >= pairs - 2
        line.pump(2, (0,), calm)
        pair_copy().wait_recv()
        got = pair_got[...].astype(jnp.float32)
        got_a, got_b, got_decay = got[:DV, :width_a], got[:DV, width_a:], got[DV : DV + 1, :]
        is_odd = odd == 1
        pair_a = jnp.where(
            is_odd,
            whole_decay[:, :width_a] * got_a + state_a[...],
            got_decay[:, :width_a] * state_a[...] + got_a,
        )
        pair_b = jnp.where(
            is_odd,
            whole_decay[:, width_a:] * got_b + state_b[...],
            got_decay[:, width_a:] * state_b[...] + got_b,
        )
        pack(1, pair_a, pair_b, whole_decay * got_decay)
        for k in range(1, pairs):

            @pl.when(pair_place + k < pairs - 1)
            def _():
                to_later(k).start()

        line.issued[0] = 1
        line.pump(2, (0,), ~calm)
        line.mate_copy(2).start()
        loads[10].wait()
        loads[8].wait()
        loads[9].wait()

        row, column = positions()
        causal = column <= row

        @pl.loop(0, chunks)
        def _(i):
            here = rows_at(i, CHUNK)
            column_sums, row_sums = fading_sums(fading[i])
            since_start = jnp.exp(column_sums)
            between = jnp.where(causal, jnp.exp(jnp.minimum(column_sums - row_sums, 0.0)), 0.0)
            for group, (queries, keys, _, kept, before, _, key_width, _) in enumerate(groups):
                sums = kept[here, :]
                middle = sums[MIDDLE : MIDDLE + 1, :]
                spread = queries[here, :].astype(jnp.float32) * (jnp.exp(sums - middle) * key_width**-0.5)
                scaled = spread.astype(jnp.bfloat16)
                queries[here, :] = (spread * since_start).astype(jnp.bfloat16)
                inverse_keys = keys[here, :]
                local = before[i]
                for h in range(keys.shape[1] // key_width):
                    if key_width % 128 == 0:
                        mine = slice(h * key_width, (h + 1) * key_width)
                        q, k, s = scaled[:, mine], inverse_keys[:, mine], local[:, mine]
                    else:
                        q = jnp.where(lanes_of(h, keys.shape[1], key_width), scaled, jnp.zeros_like(scaled))
                        k, s = inverse_keys, local
                    scores = jnp.where(causal, dot(q, k, ((1,), (1,))) * between, 0.0).astype(jnp.bfloat16)
                    head = dot(scores, values[group, here, h * DV : (h + 1) * DV], ((1,), (0,)))
                    heads[group, here, h * DV : (h + 1) * DV] = head + since_start * dot(q, s, ((1,), (1,)))

        state_a[...] = jnp.zeros_like(state_a)
        state_b[...] = jnp.zeros_like(state_b)

        def follow(slot):
            part = slot[...].astype(jnp.float32)
            factor = part[DV : DV + 1, :]
            state_a[...] = factor[:, :width_a] * state_a[...] + part[:DV, :width_a]
            state_b[...] = factor[:, width_a:] * state_b[...] + part[:DV, width_a:]

        for k in range(pairs - 2, 0, -1):

            @pl.when((pair_place >= k) & (pair_place < pairs - 1))
            def _():
                to_later(k).wait_recv()
                follow(later_got.at[k - 1])

        if pairs > 1:

            @pl.when(pair_place == pairs - 2)
            def _():
                part = packs[1].astype(jnp.float32)
                factor = part[DV : DV + 1, :]
                pack(
                    2,
                    factor[:, :width_a] * state_a[...] + part[:DV, :width_a],
                    factor[:, width_a:] * state_b[...] + part[:DV, width_a:],
                    factor,
                )
                to_later(1, 2).start()

        line.pump(3)
        if pairs > 1:

            @pl.when(pair_place == pairs - 1)
            def _():
                to_later(1).wait_recv()
                follow(later_got.at[0])

        state_a[...] = jnp.where(is_odd, got_decay[:, :width_a] * state_a[...] + got_a, state_a[...])
        state_b[...] = jnp.where(is_odd, got_decay[:, width_a:] * state_b[...] + got_b, state_b[...])
        for load in loads[11:]:
            load.wait()

        def attend(i):
            here = rows_at(i, CHUNK)
            pieces = []
            for group, (queries, _, _, _, _, state, key_width, start) in enumerate(groups):
                key_lanes = queries.shape[1]
                earlier = (state[...] * starts[i, :, start : start + key_lanes]).astype(jnp.bfloat16)
                scaled = queries[here, :]
                for h in range(key_lanes // key_width):
                    lanes = slice(h * DV, (h + 1) * DV)
                    if key_width % 128 == 0:
                        mine = slice(h * key_width, (h + 1) * key_width)
                        q, s = scaled[:, mine], earlier[:, mine]
                    else:
                        q = jnp.where(lanes_of(h, key_lanes, key_width), scaled, jnp.zeros_like(scaled))
                        s = earlier
                    head = heads[group, here, lanes] + dot(q, s, ((1,), (1,)))
                    inverse = lax.rsqrt(jnp.mean(head * head, axis=-1, keepdims=True) + EPS)
                    gate = gates[group, here, lanes].astype(jnp.float32)
                    silu = gate / (1.0 + jnp.exp(-gate))
                    pieces.append((silu * (head * inverse * gains[group : group + 1, lanes])).astype(jnp.bfloat16))
            return dot(jnp.concatenate(pieces, axis=1), projection[...], ((1,), (0,)))

        @pl.loop(0, chips * units)
        def _(k):
            other, u = chip_at(k // units), k % units
            slot = other * units + u
            terms[slot] = attend((2 * other + 1 - core) * units + u).astype(jnp.bfloat16)
            terms_copy(slot).start()

        @pl.loop(0, (chips - 1) * units)
        def _(k):
            j, u = k // units, k % units
            other = chip_at(j)
            slot = other * units + u
            total = attend((2 * other + core) * units + u)
            terms_copy(slot).wait_recv()
            cross_terms[k] = (total + partner_terms[slot].astype(jnp.float32)).astype(jnp.bfloat16)
            cross_copy(j, u).start()

        @pl.loop(0, units)
        def _(u):
            slot = chip * units + u
            total = attend((2 * chip + core) * units + u)
            terms_copy(slot).wait_recv()
            own_sum[u] = total + partner_terms[slot].astype(jnp.float32)

        line.pump(6)

        for u in range(units):
            here = slice(u * CHUNK, (u + 1) * CHUNK)
            total = residual[here, :].astype(jnp.float32) + own_sum[u]
            for j in range(chips - 1):
                cross_copy(j, u).wait_recv()
                total = total + cross_got[j * units + u].astype(jnp.float32)
            rounded = total.astype(jnp.bfloat16)
            mid[here, :] = rounded
            widened = rounded.astype(jnp.float32)
            inverse = lax.rsqrt(jnp.mean(widened * widened, axis=-1, keepdims=True) + EPS)
            all_rows[rows_at(mine * units + u, CHUNK), :] = (widened * inverse * row_gain[...]).astype(jnp.bfloat16)
            for k in range(len(peers)):
                rows_copy(k, u, mine).start()
            passed_copy(len(peers), u, mine).start()

    pl.run_scoped(
        attention,
        *[pltpu.VMEM(a.shape, a.dtype) for a in in_hbm[:10]],
        pltpu.VMEM((rows, width_a), jnp.float32),
        pltpu.VMEM((rows, width_b), jnp.float32),
        pltpu.VMEM((chunks, DV, width_a), jnp.bfloat16),
        pltpu.VMEM((chunks, DV, width_b), jnp.bfloat16),
        pltpu.VMEM((chunks, 1, width), jnp.float32),
        pltpu.VMEM((2, rows, values_hbm.shape[2]), jnp.float32),
        pltpu.VMEM((units, CHUNK, residual_hbm.shape[1]), jnp.float32),
        *[pltpu.VMEM(a.shape, a.dtype) for a in in_hbm[13:]],
    )
    line.pump(10)
    for u in range(units):
        for k, peer in enumerate(peers):
            rows_copy(k, u, owner_at(*peer, core)).wait_recv()
            passed_copy(k, u, owner_at(*peer, core)).start()
        line.pump(12 + 2 * u)
    for u in range(units):
        for k, peer in enumerate(peers + [(0, 0)]):
            passed_copy(k, u, owner_at(*peer, 1 - core)).wait_recv()
    line.pump(14)
    ff = hidden.shape[1]
    tile = 256 if ff % 256 == 0 else 128
    tiles = ff // tile
    bands = 2 * chips
    band = 2 * own_rows
    last_pair = line.nth(pairs - 1)
    depth = 2 * shards[0].shape[0]
    late = rows_at(last_pair, depth)
    early = pl.ds(pl.multiple_of(jnp.where(last_pair == 0, depth, 0), depth), (pairs - 1) * depth)

    def first_half(gate_early, up_early):
        def products(n, part):
            lanes, here = rows_at(n // bands, tile), rows_at(n % bands, band)
            gate_sum = dot(all_rows[here, part], gate_full[part, lanes], ((1,), (0,)))
            return lanes, here, gate_sum, dot(all_rows[here, part], up_full[part, lanes], ((1,), (0,)))

        line.arrive_gates(pairs - 2)

        @pl.loop(0, tiles * bands)
        def _(n):
            lanes, here, gate_sum, up_sum = products(n, early)
            gate_early[here, lanes] = gate_sum
            up_early[here, lanes] = up_sum

        line.arrive_gates(pairs - 1)

        @pl.loop(0, tiles * bands)
        def _(n):
            lanes, here, gate_sum, up_sum = products(n, late)
            gate_sum, up_sum = gate_sum + gate_early[here, lanes], up_sum + up_early[here, lanes]
            hidden[here, lanes] = (gate_sum / (1.0 + jnp.exp(-gate_sum)) * up_sum).astype(jnp.bfloat16)

    pl.run_scoped(first_half, *[pltpu.VMEM(hidden.shape, jnp.float32)] * 2)

    columns = shards[2].shape[1]
    direct = columns % 128 == 0
    count = len(peers)

    order = peers[::-1] + [(0, 0)]
    order_bands = [(1 - odd if dy else odd) * chips + (chip + dx) % chips for dy, dx in order]

    blocks = [(b, 0, columns) for b in range(n_sp)]
    if line.split:
        blocks[-1:] = [(n_sp - 1, 0, columns // 2), (n_sp - 1, columns // 2, columns // 2)]
    origins = [2 * line.nth(b // 2) + b % 2 for b in range(n_sp)]

    def lanes_in(b):
        return pl.ds(0, blocks[b][2])

    def half_copy(b, k):
        at = order_bands[k]
        return remote(
            stage.at[b % DEPTH, at, 1 - core, :, lanes_in(b)],
            stage_partner.at[b, at, :, lanes_in(b)],
            half_send.at[b % DEPTH * (count + 1) + k],
            half_receive.at[b % (DEPTH + 1) * (count + 1) + k],
            partner,
        )

    def last_copy(b, k):
        slot = b * count + k
        return remote(
            stage_cross.at[b % DEPTH * count + k, :, lanes_in(b)],
            stage_got.at[slot, :, lanes_in(b)],
            last_send.at[b % DEPTH * count + k],
            last_receive.at[slot],
            device_at(*order[k]),
        )

    def multiply(b):
        which, start, size = blocks[b]
        for k in range(count + 1):
            if b >= DEPTH:
                half_copy(b - DEPTH, k).wait_send()
            here = rows_at(order_bands[k], band)
            part = down_full[origins[which], :, start : start + size]
            product = dot(hidden[here, :], part, ((1,), (0,))).astype(jnp.bfloat16)
            stage[b % DEPTH, order_bands[k], :, :, :size] = product.reshape(2, own_rows, size)
            half_copy(b, k).start()
            if k >= 2:
                combine(b, k - 2)
        combine(b, count - 1)

    def chip_sum(b, at):
        size = blocks[b][2]
        mine_here = stage[b % DEPTH, at, core, :, :size].astype(jnp.float32)
        return mine_here + stage_partner[b, at, :, :size].astype(jnp.float32)

    def combine(b, k):
        half_copy(b, k).wait_recv()
        if b >= DEPTH:
            last_copy(b - DEPTH, k).wait_send()
        both = chip_sum(b, order_bands[k]).astype(jnp.bfloat16)
        stage_cross[b % DEPTH * count + k, :, : blocks[b][2]] = both
        last_copy(b, k).start()

    def close(b):
        which, start, size = blocks[b]
        half_copy(b, count).wait_recv()
        total = chip_sum(b, odd * chips + chip)
        for k in range(count):
            last_copy(b, k).wait_recv()
            total = total + stage_got[b * count + k, :, :size].astype(jnp.float32)
        if direct:
            lanes = pl.ds(pl.multiple_of(origins[which] * columns + start, 128), size)
            outs[0][:, lanes] = (mid[:, lanes].astype(jnp.float32) + total).astype(jnp.bfloat16)
        else:
            outs[1][origins[which]] = total

    for b, (which, start, _) in enumerate(blocks):
        hop = which // 2
        if hop:
            piece = which % 2
            if piece and 2 in line.pieces(1, hop):
                piece = 3 if start else 2
            line.arrive(0, 1, hop, piece)
            line.arrive(1, 1, hop, piece)
        multiply(b)
        line.pump({0: 15, 1: 16, 3: 17}.get(b * 8 // n_sp, 0))
        if b * 8 // n_sp == 4:
            held = line.issued[0]
            line.pump(18, also=core == 0)
        if b >= 3:
            close(b - 3)
        if b == n_sp - 1:
            line.issued = [held, held]
            line.pump(18, also=core == 1)
    for b in range(len(blocks) - 3, len(blocks)):
        close(b)
    if not direct:
        outs[0][...] = mid[...]

    line.finish()
    pair_copy().wait_send()
    for k in range(1, pairs):

        @pl.when(pair_place + k < pairs - 1)
        def _():
            to_later(k).wait_send()

    if pairs > 1:

        @pl.when(pair_place == pairs - 2)
        def _():
            to_later(1, 2).wait_send()

    for slot in range(chips * units):
        terms_copy(slot).wait_send()
    for u in range(units):
        for j in range(chips - 1):
            cross_copy(j, u).wait_send()
        for k in range(count):
            rows_copy(k, u, mine).wait_send()
        for k in range(count + 1):
            passed_copy(k, u, mine).wait_send()
    for b in range(len(blocks) - DEPTH, len(blocks)):
        for k in range(count + 1):
            half_copy(b, k).wait_send()
        for k in range(count):
            last_copy(b, k).wait_send()


def per_device(
    residual,
    first_group_queries,
    first_group_keys,
    second_group_queries,
    second_group_keys,
    primary_retain_switch_inputs,
    secondary_retain_switch_inputs,
    timestep_fading_exponent,
    values,
    output_gate_logits,
    head_norm_gains,
    output_projection,
    feedforward_norm_gain,
    gate_projection,
    up_projection,
    down_projection,
):
    n_sp, n_tp = lax.axis_size("sp"), lax.axis_size("tp")
    rows, own_rows = first_group_queries.shape[0], residual.shape[0]
    features = residual.shape[1]
    chunks, units, chips = rows // CHUNK, own_rows // CHUNK, n_tp // 2
    width_a, width_b = first_group_keys.shape[1], second_group_keys.shape[1]
    width = width_a + width_b
    inner, ff = gate_projection.shape
    columns = down_projection.shape[1]
    pairs, crossings, peers = n_sp // 2, max(chips - 1, 1), 2 * chips - 1
    direct = columns % 128 == 0
    blocks = n_sp + 1 if columns % 256 == 0 else n_sp
    projection = output_projection.reshape(-1, features)
    in_hbm = [
        residual,
        first_group_queries,
        second_group_queries,
        first_group_keys,
        second_group_keys,
        primary_retain_switch_inputs,
        secondary_retain_switch_inputs,
        values,
        output_gate_logits,
        projection,
        gate_projection,
        up_projection,
        down_projection,
        timestep_fading_exponent.reshape(chunks, 1, CHUNK),
        head_norm_gains,
        feedforward_norm_gain.reshape(1, features),
    ]

    def bf16(*shape):
        return pltpu.VMEM(shape, jnp.bfloat16)

    def f32(*shape):
        return pltpu.VMEM(shape, jnp.float32)

    def sems(*shape):
        return pltpu.SemaphoreType.DMA(shape)

    scratch = [bf16(n_sp * inner, ff // 2)] * 2 + [bf16(n_sp, ff // 2, columns)]
    scratch += [f32(DV, width_a), f32(DV, width_b), f32(8, width)]
    scratch += [bf16(3, DV + PAD, width), bf16(DV + PAD, width), bf16(max(n_sp // 2 - 1, 1), DV + PAD, width)]
    scratch += [bf16(chips * units, CHUNK, features)] * 2
    scratch += [bf16(crossings * units, CHUNK, features)] * 2
    scratch += [bf16(2 * rows, features), bf16(2 * rows, ff // 2)]
    scratch += [bf16(DEPTH, 2 * chips, 2, own_rows, columns), bf16(blocks, 2 * chips, own_rows, columns)]
    scratch += [bf16(DEPTH * peers, own_rows, columns), bf16(blocks * peers, own_rows, columns)]
    scratch += [bf16(own_rows, features)]
    scratch += [sems(len(in_hbm)), sems(3), sems(3)]
    scratch += [sems(2, QUEUE), sems(2, max(6 * pairs - 5, 1))]
    scratch += [sems(2), sems(max(n_sp // 2 - 1, 1)), sems(max(n_sp // 2 - 1, 1))]
    scratch += [sems(chips * units)] * 2
    scratch += [sems(crossings * units)] * 2
    scratch += [sems(peers * units)] * 2
    scratch += [sems((peers + 1) * units)] * 2
    scratch += [sems(DEPTH * (peers + 1)), sems((DEPTH + 1) * (peers + 1))]
    scratch += [sems(DEPTH * peers), sems(blocks * peers)]
    outs = [bf16(own_rows, features)] if direct else [bf16(own_rows, features), f32(n_sp, own_rows, columns)]
    outs = pl.pallas_call(
        functools.partial(layer_kernel, n_sp, n_tp, len(in_hbm), len(outs)),
        in_specs=[pl.BlockSpec(memory_space=pl.ANY)] * len(in_hbm),
        out_specs=[pl.BlockSpec(memory_space=pltpu.VMEM)] * len(outs),
        out_shape=outs,
        scratch_shapes=scratch,
        compiler_params=pltpu.CompilerParams(
            collective_id=0, has_side_effects=True, vmem_limit_bytes=VMEM_BYTES
        ),
        name="layer",
    )(*in_hbm)
    if direct:
        return outs[0]
    added = outs[1].transpose(1, 0, 2).reshape(own_rows, features)
    return (outs[0].astype(jnp.float32) + added).astype(jnp.bfloat16)


def solution(mesh):
    return jax.shard_map(
        per_device,
        mesh=mesh,
        in_specs=(
            P(("sp", "tp"), None),
            P("sp", "tp"),
            P("sp", "tp"),
            P("sp", "tp"),
            P("sp", "tp"),
            P("sp", "tp"),
            P("sp", "tp"),
            P("sp"),
            P(None, "sp", "tp"),
            P(None, "sp", "tp"),
            P(None, "tp"),
            P(None, "tp", None),
            P(),
            P("sp", "tp"),
            P("sp", "tp"),
            P("tp", "sp"),
        ),
        out_specs=P(("sp", "tp"), None),
        check_vma=False,
    )
```

```python
import functools

import jax
import jax.numpy as jnp
from jax import lax
from jax.experimental import pallas as pl
from jax.experimental.pallas import tpu as pltpu
from jax.sharding import PartitionSpec as P

FIRST_KEY_SIZE = 128
SECOND_KEY_SIZE = 64
DV = 128
CHUNK = 128
MIDDLE = CHUNK // 2 - 1
PAD = 16
MESH = pl.DeviceIdType.MESH

EPS = 1e-06
SOFTNESS_SCALE = 16.0
VMEM_BYTES = 62_000_000
DEPTH = 4
QUEUE = 8

def dot(a, b, dims):
    return lax.dot_general(a, b, (dims, ((), ())), preferred_element_type=jnp.float32)


def positions():
    row = lax.broadcasted_iota(jnp.int32, (CHUNK, CHUNK), 0)
    column = lax.broadcasted_iota(jnp.int32, (CHUNK, CHUNK), 1)
    return row, column


def fading_sums(fading_row):
    row, column = positions()
    as_column = jnp.sum(jnp.where(row == column, fading_row, 0.0), axis=1, keepdims=True)
    column_sums = jnp.sum(jnp.where(column <= row, fading_row, 0.0), axis=1, keepdims=True)
    row_sums = jnp.sum(jnp.where(row <= column, as_column, 0.0), axis=0, keepdims=True)
    return column_sums, row_sums


def channel_sums(switches):
    row, column = positions()
    x = switches.astype(jnp.float32)
    logs = (jnp.minimum(x, 0.0) - jnp.log1p(jnp.exp(-jnp.abs(x)))) * (1.0 / SOFTNESS_SCALE)
    lower = (column <= row).astype(jnp.bfloat16)
    high = logs.astype(jnp.bfloat16)
    low = (logs - high.astype(jnp.float32)).astype(jnp.bfloat16)
    return dot(lower, high, ((1,), (0,))) + dot(lower, low, ((1,), (0,)))


def lanes_of(head, width, key_width):
    lane = lax.broadcasted_iota(jnp.int32, (1, width), 1)
    return (lane >= head * key_width) & (lane < (head + 1) * key_width)


def advanced(state, inverse_keys, weighted, sums, total_fading, key_width):
    width = state.shape[1]
    end, middle = sums[CHUNK - 1 :, :], sums[MIDDLE : MIDDLE + 1, :]
    head_count = width // key_width
    if key_width % 128 == 0:
        added = jnp.concatenate(
            [
                dot(
                    weighted[:, h * DV : (h + 1) * DV],
                    inverse_keys[:, h * key_width : (h + 1) * key_width],
                    ((0,), (0,)),
                )
                for h in range(head_count)
            ],
            axis=1,
        )
    else:
        added = jnp.zeros((DV, width), jnp.float32)
        for h in range(head_count):
            product = dot(weighted[:, h * DV : (h + 1) * DV], inverse_keys, ((0,), (0,)))
            added = jnp.where(lanes_of(h, width, key_width), product, added)
    return jnp.exp(end + total_fading) * state + jnp.exp(end - middle) * added


def remote(source, target, send, receive, device):
    return pltpu.make_async_remote_copy(
        src_ref=source,
        dst_ref=target,
        send_sem=send,
        recv_sem=receive,
        device_id=device,
        device_id_type=MESH,
    )


def rows_at(index, count):
    return pl.ds(pl.multiple_of(index * count, count), count)


class Line:
    def __init__(self, pairs, place, tp_place, whole, shards, sems, mate_sems):
        self.pairs, self.place, self.tp_place = pairs, place, tp_place
        self.pair, self.side = place // 2, place % 2
        self.gate, self.up, self.down = whole
        self.shards = shards
        self.sems, self.mate_sems = sems, mate_sems
        self.inner, self.half = shards[0].shape[0], shards[2].shape[0] // 2
        self.waited = set()
        self.issued = [0, 0]
        self.split = self.down.shape[2] % 256 == 0
        self.events = [
            (matrix, hop, piece)
            for matrix in (0, 1)
            for hop in range(1, pairs)
            for piece in self.pieces(matrix, hop)
        ]

    def pieces(self, matrix, hop):
        if not matrix:
            return range(4)
        return (0, 2, 3) if hop == self.pairs - 1 and self.split else (0, 1)

    def shard(self, kind, side):
        half = rows_at(side, self.half)
        return self.shards[kind].at[half, :] if kind == 2 else self.shards[kind].at[:, half]

    def landing(self, kind, origin):
        if kind == 2:
            return self.down.at[origin]
        return (self.up if kind else self.gate).at[rows_at(origin, self.inner), :]

    def own(self, kind):
        return self.shard(kind, self.side), self.landing(kind, self.place)

    def mate_copy(self, kind):
        return remote(
            self.shard(kind, 1 - self.side),
            self.landing(kind, self.place),
            self.mate_sems[0].at[kind],
            self.mate_sems[1].at[kind],
            (self.place + 1 - 2 * self.side, self.tp_place),
        )

    def arrive_mate(self, kind):
        if ("mate", kind) not in self.waited:
            self.waited.add(("mate", kind))
            self.mate_copy(kind).wait_recv()

    def reaches(self, way, distance):
        return self.pair + distance < self.pairs if way else self.pair >= distance

    def copy(self, way, matrix, hop, piece, distance):
        pair = (self.pair + (distance if way else -distance) + self.pairs) % self.pairs
        if matrix and piece >= 2:
            half = self.down.shape[2] // 2
            ref = self.down.at[2 * pair + 1, :, pl.ds((piece - 2) * half, half)]
        elif matrix:
            ref = self.landing(2, 2 * pair + piece)
        else:
            ref = self.landing(piece % 2, 2 * pair + (self.side if piece < 2 else 1 - self.side))
        number = self.events.index((matrix, hop, piece))
        send, receive = self.sems[0].at[way, number % QUEUE], self.sems[1].at[way, number]
        beyond = (self.place + (-2 if way else 2) + 2 * self.pairs) % (2 * self.pairs)
        return remote(ref, ref, send, receive, (beyond, self.tp_place))

    def arrive(self, way, matrix, hop, piece):
        if (way, matrix, hop, piece) not in self.waited:
            self.waited.add((way, matrix, hop, piece))

            @pl.when(self.reaches(way, hop))
            def _():
                self.copy(way, matrix, hop, piece, hop).wait_recv()

    def passes(self, way, hop):
        return self.reaches(way, hop - 1) & self.reaches(1 - way, 1)

    def pump(self, until, ways=(0, 1), also=True):
        count = 6 * (self.pairs - 1)
        until = len(self.events) if until >= 18 else (until * count + 17) // 18
        for way in ways:
            for number in range(self.issued[way], until):
                matrix, hop, piece = self.events[number]
                if hop == 1 and (matrix or piece >= 2):
                    self.arrive_mate(2 if matrix else piece % 2)
                if hop > 1:
                    self.arrive(way, matrix, hop - 1, 1 if matrix and piece else piece)

                self.left(way, number - QUEUE)

                @pl.when(self.passes(way, hop) & also)
                def _():
                    self.copy(way, matrix, hop, piece, hop - 1).start()

            self.issued[way] = max(until, self.issued[way])

    def arrive_gates(self, until):
        for hop in range(1, until + 1):
            for piece in range(4):
                for way in (0, 1):
                    self.arrive(way, 0, hop, piece)

    def nth(self, q):
        low, high = self.pair, self.pairs - 1 - self.pair
        both = jnp.minimum(low, high)
        near = self.pair + ((q // 2) if q % 2 == 0 else -((q + 1) // 2))
        far = jnp.where(low > high, self.pair - (q - both), self.pair + (q - both))
        return jnp.where(q <= 2 * both, near, far)

    def finish(self):
        for kind in range(3):
            self.mate_copy(kind).wait_send()
        for number in range(len(self.events)):
            for way in (0, 1):
                self.left(way, number)

    def left(self, way, number):
        if number >= 0 and ("left", way, number) not in self.waited:
            self.waited.add(("left", way, number))
            matrix, hop, piece = self.events[number]

            @pl.when(self.passes(way, hop))
            def _():
                self.copy(way, matrix, hop, piece, hop - 1).wait_send()


def layer_kernel(n_sp, n_tp, in_count, out_count, *refs):
    layer_body(n_sp, n_tp, refs[:in_count], refs[in_count : in_count + out_count], *refs[in_count + out_count :])


def layer_body(
    n_sp,
    n_tp,
    in_hbm,
    outs,
    gate_full,
    up_full,
    down_full,
    state_a,
    state_b,
    decay,
    packs,
    pair_got,
    later_got,
    terms,
    partner_terms,
    cross_terms,
    cross_got,
    all_rows,
    hidden,
    stage,
    stage_partner,
    stage_cross,
    stage_got,
    mid,
    load_sems,
    mate_send,
    mate_receive,
    line_send,
    line_receive,
    pair_sems,
    later_send,
    later_receive,
    terms_send,
    terms_receive,
    cross_send,
    cross_receive,
    rows_send,
    rows_receive,
    passed_send,
    passed_receive,
    half_send,
    half_receive,
    last_send,
    last_receive,
):
    residual_hbm, qa_hbm, qb_hbm, ka_hbm, kb_hbm, sa_hbm, sb_hbm, values_hbm, gates_hbm, projection_hbm = in_hbm[:10]
    shards = in_hbm[10:13]
    fading_hbm, gains_hbm, row_gain_hbm = in_hbm[13:]
    place, tp_place = lax.axis_index("sp"), lax.axis_index("tp")
    chip, core = tp_place // 2, tp_place % 2
    chips = n_tp // 2
    partner = (place, 2 * chip + 1 - core)
    rows, own_rows = qa_hbm.shape[0], residual_hbm.shape[0]
    chunks, units = rows // CHUNK, own_rows // CHUNK
    width_a, width_b = ka_hbm.shape[1], kb_hbm.shape[1]
    width = width_a + width_b
    odd = place % 2
    mate = place + 1 - 2 * odd
    pairs, pair_place = n_sp // 2, place // 2
    line = Line(
        pairs,
        place,
        tp_place,
        (gate_full, up_full, down_full),
        shards,
        (line_send, line_receive),
        (mate_send, mate_receive),
    )

    barrier = pltpu.get_barrier_semaphore()
    for k in range(1, n_sp):
        pl.semaphore_signal(
            barrier, inc=1, device_id=((place + k) % n_sp, tp_place), device_id_type=MESH
        )
    for k in range(1, n_tp):
        pl.semaphore_signal(
            barrier, inc=1, device_id=(place, (tp_place + k) % n_tp), device_id_type=MESH
        )

    for k in range(1, chips):
        pl.semaphore_signal(
            barrier,
            inc=1,
            device_id=(mate, 2 * ((chip + k) % chips) + core),
            device_id_type=MESH,
        )

    def pair_copy():
        return remote(packs.at[0], pair_got, pair_sems.at[0], pair_sems.at[1], (mate, tp_place))

    def to_later(k, slot=1):
        return remote(
            packs.at[slot],
            later_got.at[k - 1],
            later_send.at[k - 1],
            later_receive.at[k - 1],
            ((place + 2 * k) % n_sp, tp_place),
        )

    def chip_at(k):
        return (chip + 1 + k) % chips

    def terms_copy(slot):
        return remote(
            terms.at[slot], partner_terms.at[slot], terms_send.at[slot], terms_receive.at[slot], partner
        )

    def cross_copy(j, u):
        slot = j * units + u
        return remote(
            cross_terms.at[slot],
            cross_got.at[slot],
            cross_send.at[slot],
            cross_receive.at[slot],
            (place, 2 * chip_at(j) + core),
        )

    peers = [(dy, dx) for dy in (0, 1) for dx in range(chips) if dy or dx]

    def device_at(dy, dx):
        return (mate if dy else place, 2 * ((chip + dx) % chips) + core)

    def owner_at(dy, dx, of_core):
        side = 1 - odd if dy else odd
        return side * n_tp + 2 * ((chip - dx + chips) % chips) + of_core

    def own_at(owner, u):
        return all_rows.at[rows_at(u * 2 * n_tp + owner, CHUNK), :]

    def rows_copy(k, u, owner):
        slot = k * units + u
        ref = own_at(owner, u)
        return remote(ref, ref, rows_send.at[slot], rows_receive.at[slot], device_at(*peers[k]))

    def passed_copy(k, u, owner):
        slot = k * units + u
        ref = own_at(owner, u)
        return remote(ref, ref, passed_send.at[slot], passed_receive.at[slot], partner)

    mine = owner_at(0, 0, core)
    def attention(
        residual,
        qa,
        qb,
        ka,
        kb,
        sa,
        sb,
        values,
        gates,
        projection,
        sums_a,
        sums_b,
        before_a,
        before_b,
        starts,
        heads,
        own_sum,
        fading,
        gains,
        row_gain,
    ):
        groups = (
            (qa, ka, sa, sums_a, before_a, state_a, FIRST_KEY_SIZE, 0),
            (qb, kb, sb, sums_b, before_b, state_b, SECOND_KEY_SIZE, width_a),
        )

        loads = [
            line.own(0),
            line.own(1),
            (fading_hbm, fading),
            (ka_hbm, ka),
            (kb_hbm, kb),
            (sa_hbm, sa),
            (sb_hbm, sb),
            (values_hbm, values),
            (qa_hbm, qa),
            (qb_hbm, qb),
            line.own(2),
            (projection_hbm, projection),
            (gates_hbm, gates),
            (residual_hbm, residual),
            (gains_hbm, gains),
            (row_gain_hbm, row_gain),
        ]
        loads = [pltpu.make_async_copy(a, b, load_sems.at[i]) for i, (a, b) in enumerate(loads)]
        for load in loads:
            load.start()
        state_a[...] = jnp.zeros_like(state_a)
        state_b[...] = jnp.zeros_like(state_b)
        decay[...] = jnp.zeros_like(decay)
        loads[0].wait()
        loads[1].wait()
        pl.semaphore_wait(barrier, n_sp + n_tp + chips - 3)
        line.pump(1)
        for load in loads[2:8]:
            load.wait()

        @pl.loop(0, chunks)
        def _(i):
            here = rows_at(i, CHUNK)
            column_sums, _ = fading_sums(fading[i])
            total_fading = column_sums[CHUNK - 1 :, :]
            later = jnp.exp(total_fading - column_sums)
            for group, (_, keys, switches, kept, before, state, key_width, start) in enumerate(groups):
                mine = slice(start, start + keys.shape[1])
                sums = channel_sums(switches[here, :])
                kept[here, :] = sums
                middle = sums[MIDDLE : MIDDLE + 1, :]
                inverse_keys = (keys[here, :].astype(jnp.float32) * jnp.exp(middle - sums)).astype(jnp.bfloat16)
                keys[here, :] = inverse_keys
                before[i] = (state[...] * jnp.exp(middle)).astype(jnp.bfloat16)
                starts[i, :, mine] = jnp.exp(decay[:1, mine] + middle)
                weighted = (values[group, here, :].astype(jnp.float32) * later).astype(jnp.bfloat16)
                state[...] = advanced(state[...], inverse_keys, weighted, sums, total_fading, key_width)
                decay[:, mine] += sums[CHUNK - 1 :, :] + total_fading

        def pack(slot, first, second, factor):
            packs[slot, :DV, :width_a] = first.astype(jnp.bfloat16)
            packs[slot, :DV, width_a:] = second.astype(jnp.bfloat16)
            packs[slot, DV:, :] = jnp.broadcast_to(factor, (PAD, width)).astype(jnp.bfloat16)

        whole_decay = jnp.exp(decay[:1, :])
        pack(0, state_a[...], state_b[...], whole_decay)
        pair_copy().start()
        line.mate_copy(0).start()
        line.mate_copy(1).start()
        line.pump(2, (1,))
        calm = pair_place >= pairs - 2
        line.pump(2, (0,), calm)
        pair_copy().wait_recv()
        got = pair_got[...].astype(jnp.float32)
        got_a, got_b, got_decay = got[:DV, :width_a], got[:DV, width_a:], got[DV : DV + 1, :]
        is_odd = odd == 1
        pair_a = jnp.where(
            is_odd,
            whole_decay[:, :width_a] * got_a + state_a[...],
            got_decay[:, :width_a] * state_a[...] + got_a,
        )
        pair_b = jnp.where(
            is_odd,
            whole_decay[:, width_a:] * got_b + state_b[...],
            got_decay[:, width_a:] * state_b[...] + got_b,
        )
        pack(1, pair_a, pair_b, whole_decay * got_decay)
        for k in range(1, pairs):

            @pl.when(pair_place + k < pairs - 1)
            def _():
                to_later(k).start()

        line.issued[0] = 1
        line.pump(2, (0,), ~calm)
        line.mate_copy(2).start()
        loads[10].wait()
        loads[8].wait()
        loads[9].wait()

        row, column = positions()
        causal = column <= row

        @pl.loop(0, chunks)
        def _(i):
            here = rows_at(i, CHUNK)
            column_sums, row_sums = fading_sums(fading[i])
            since_start = jnp.exp(column_sums)
            between = jnp.where(causal, jnp.exp(jnp.minimum(column_sums - row_sums, 0.0)), 0.0)
            for group, (queries, keys, _, kept, before, _, key_width, _) in enumerate(groups):
                sums = kept[here, :]
                middle = sums[MIDDLE : MIDDLE + 1, :]
                spread = queries[here, :].astype(jnp.float32) * (jnp.exp(sums - middle) * key_width**-0.5)
                scaled = spread.astype(jnp.bfloat16)
                queries[here, :] = (spread * since_start).astype(jnp.bfloat16)
                inverse_keys = keys[here, :]
                local = before[i]
                for h in range(keys.shape[1] // key_width):
                    if key_width % 128 == 0:
                        mine = slice(h * key_width, (h + 1) * key_width)
                        q, k, s = scaled[:, mine], inverse_keys[:, mine], local[:, mine]
                    else:
                        q = jnp.where(lanes_of(h, keys.shape[1], key_width), scaled, jnp.zeros_like(scaled))
                        k, s = inverse_keys, local
                    scores = jnp.where(causal, dot(q, k, ((1,), (1,))) * between, 0.0).astype(jnp.bfloat16)
                    head = dot(scores, values[group, here, h * DV : (h + 1) * DV], ((1,), (0,)))
                    heads[group, here, h * DV : (h + 1) * DV] = head + since_start * dot(q, s, ((1,), (1,)))

        state_a[...] = jnp.zeros_like(state_a)
        state_b[...] = jnp.zeros_like(state_b)

        def follow(slot):
            part = slot[...].astype(jnp.float32)
            factor = part[DV : DV + 1, :]
            state_a[...] = factor[:, :width_a] * state_a[...] + part[:DV, :width_a]
            state_b[...] = factor[:, width_a:] * state_b[...] + part[:DV, width_a:]

        for k in range(pairs - 2, 0, -1):

            @pl.when((pair_place >= k) & (pair_place < pairs - 1))
            def _():
                to_later(k).wait_recv()
                follow(later_got.at[k - 1])

        if pairs > 1:

            @pl.when(pair_place == pairs - 2)
            def _():
                part = packs[1].astype(jnp.float32)
                factor = part[DV : DV + 1, :]
                pack(
                    2,
                    factor[:, :width_a] * state_a[...] + part[:DV, :width_a],
                    factor[:, width_a:] * state_b[...] + part[:DV, width_a:],
                    factor,
                )
                to_later(1, 2).start()

        line.pump(3)
        if pairs > 1:

            @pl.when(pair_place == pairs - 1)
            def _():
                to_later(1).wait_recv()
                follow(later_got.at[0])

        state_a[...] = jnp.where(is_odd, got_decay[:, :width_a] * state_a[...] + got_a, state_a[...])
        state_b[...] = jnp.where(is_odd, got_decay[:, width_a:] * state_b[...] + got_b, state_b[...])
        for load in loads[11:]:
            load.wait()

        def attend(i):
            here = rows_at(i, CHUNK)
            pieces = []
            for group, (queries, _, _, _, _, state, key_width, start) in enumerate(groups):
                key_lanes = queries.shape[1]
                earlier = (state[...] * starts[i, :, start : start + key_lanes]).astype(jnp.bfloat16)
                scaled = queries[here, :]
                for h in range(key_lanes // key_width):
                    lanes = slice(h * DV, (h + 1) * DV)
                    if key_width % 128 == 0:
                        mine = slice(h * key_width, (h + 1) * key_width)
                        q, s = scaled[:, mine], earlier[:, mine]
                    else:
                        q = jnp.where(lanes_of(h, key_lanes, key_width), scaled, jnp.zeros_like(scaled))
                        s = earlier
                    head = heads[group, here, lanes] + dot(q, s, ((1,), (1,)))
                    inverse = lax.rsqrt(jnp.mean(head * head, axis=-1, keepdims=True) + EPS)
                    gate = gates[group, here, lanes].astype(jnp.float32)
                    silu = gate / (1.0 + jnp.exp(-gate))
                    pieces.append((silu * (head * inverse * gains[group : group + 1, lanes])).astype(jnp.bfloat16))
            return dot(jnp.concatenate(pieces, axis=1), projection[...], ((1,), (0,)))

        @pl.loop(0, chips * units)
        def _(k):
            other, u = chip_at(k // units), k % units
            slot = other * units + u
            terms[slot] = attend((2 * other + 1 - core) * units + u).astype(jnp.bfloat16)
            terms_copy(slot).start()

        @pl.loop(0, (chips - 1) * units)
        def _(k):
            j, u = k // units, k % units
            other = chip_at(j)
            slot = other * units + u
            total = attend((2 * other + core) * units + u)
            terms_copy(slot).wait_recv()
            cross_terms[k] = (total + partner_terms[slot].astype(jnp.float32)).astype(jnp.bfloat16)
            cross_copy(j, u).start()

        @pl.loop(0, units)
        def _(u):
            slot = chip * units + u
            total = attend((2 * chip + core) * units + u)
            terms_copy(slot).wait_recv()
            own_sum[u] = total + partner_terms[slot].astype(jnp.float32)

        line.pump(6)

        for u in range(units):
            here = slice(u * CHUNK, (u + 1) * CHUNK)
            total = residual[here, :].astype(jnp.float32) + own_sum[u]
            for j in range(chips - 1):
                cross_copy(j, u).wait_recv()
                total = total + cross_got[j * units + u].astype(jnp.float32)
            rounded = total.astype(jnp.bfloat16)
            mid[here, :] = rounded
            widened = rounded.astype(jnp.float32)
            inverse = lax.rsqrt(jnp.mean(widened * widened, axis=-1, keepdims=True) + EPS)
            all_rows[rows_at(u * 2 * n_tp + mine, CHUNK), :] = (widened * inverse * row_gain[...]).astype(jnp.bfloat16)
            for k in range(len(peers)):
                rows_copy(k, u, mine).start()
            passed_copy(len(peers), u, mine).start()

    pl.run_scoped(
        attention,
        *[pltpu.VMEM(a.shape, a.dtype) for a in in_hbm[:10]],
        pltpu.VMEM((rows, width_a), jnp.float32),
        pltpu.VMEM((rows, width_b), jnp.float32),
        pltpu.VMEM((chunks, DV, width_a), jnp.bfloat16),
        pltpu.VMEM((chunks, DV, width_b), jnp.bfloat16),
        pltpu.VMEM((chunks, 1, width), jnp.float32),
        pltpu.VMEM((2, rows, values_hbm.shape[2]), jnp.float32),
        pltpu.VMEM((units, CHUNK, residual_hbm.shape[1]), jnp.float32),
        *[pltpu.VMEM(a.shape, a.dtype) for a in in_hbm[13:]],
    )
    line.pump(10)
    ff = hidden.shape[1]
    tile = 256 if ff % 256 == 0 else 128
    tiles = ff // tile
    bands = 2 * chips
    part_rows = 2 * n_tp * CHUNK
    wide = min(512, part_rows)
    wides = part_rows // wide
    last_pair = line.nth(pairs - 1)
    depth = 2 * shards[0].shape[0]
    late = rows_at(last_pair, depth)
    early = pl.ds(pl.multiple_of(jnp.where(last_pair == 0, depth, 0), depth), (pairs - 1) * depth)

    def first_half(gate_early, up_early):
        def products(n, u, part):
            lanes, here = rows_at(n // wides, tile), rows_at(u * wides + n % wides, wide)
            gate_sum = dot(all_rows[here, part], gate_full[part, lanes], ((1,), (0,)))
            return lanes, here, gate_sum, dot(all_rows[here, part], up_full[part, lanes], ((1,), (0,)))

        for u in range(units):
            for k, peer in enumerate(peers):
                rows_copy(k, u, owner_at(*peer, core)).wait_recv()
                passed_copy(k, u, owner_at(*peer, core)).start()
            line.pump(12 + 2 * u)
            for k, peer in enumerate(peers + [(0, 0)]):
                passed_copy(k, u, owner_at(*peer, 1 - core)).wait_recv()
            line.arrive_gates(pairs - 2)

            @pl.loop(0, tiles * wides)
            def _(n):
                lanes, here, gate_sum, up_sum = products(n, u, early)
                gate_early[here, lanes] = gate_sum
                up_early[here, lanes] = up_sum

        line.pump(14)
        line.arrive_gates(pairs - 1)

        @pl.loop(0, tiles * wides * units)
        def _(n):
            lanes, here, gate_sum, up_sum = products(n % (tiles * wides), n // (tiles * wides), late)
            gate_sum, up_sum = gate_sum + gate_early[here, lanes], up_sum + up_early[here, lanes]
            hidden[here, lanes] = (gate_sum / (1.0 + jnp.exp(-gate_sum)) * up_sum).astype(jnp.bfloat16)

    pl.run_scoped(first_half, *[pltpu.VMEM(hidden.shape, jnp.float32)] * 2)

    columns = shards[2].shape[1]
    direct = columns % 128 == 0
    count = len(peers)

    order = peers[::-1] + [(0, 0)]
    order_bands = [(1 - odd if dy else odd) * chips + (chip + dx) % chips for dy, dx in order]

    blocks = [(b, 0, columns) for b in range(n_sp)]
    if line.split:
        blocks[-1:] = [(n_sp - 1, 0, columns // 2), (n_sp - 1, columns // 2, columns // 2)]
    origins = [2 * line.nth(b // 2) + b % 2 for b in range(n_sp)]

    def lanes_in(b):
        return pl.ds(0, blocks[b][2])

    def half_copy(b, k):
        at = order_bands[k]
        return remote(
            stage.at[b % DEPTH, at, 1 - core, :, lanes_in(b)],
            stage_partner.at[b, at, :, lanes_in(b)],
            half_send.at[b % DEPTH * (count + 1) + k],
            half_receive.at[b % (DEPTH + 1) * (count + 1) + k],
            partner,
        )

    def last_copy(b, k):
        slot = b * count + k
        return remote(
            stage_cross.at[b % DEPTH * count + k, :, lanes_in(b)],
            stage_got.at[slot, :, lanes_in(b)],
            last_send.at[b % DEPTH * count + k],
            last_receive.at[slot],
            device_at(*order[k]),
        )

    def multiply(b):
        which, start, size = blocks[b]
        for k in range(count + 1):
            if b >= DEPTH:
                half_copy(b - DEPTH, k).wait_send()
            part = down_full[origins[which], :, start : start + size]
            for u in range(units):
                here = rows_at(u * bands + order_bands[k], 2 * CHUNK)
                product = dot(hidden[here, :], part, ((1,), (0,))).astype(jnp.bfloat16)
                lines = slice(u * CHUNK, (u + 1) * CHUNK)
                stage[b % DEPTH, order_bands[k], :, lines, :size] = product.reshape(2, CHUNK, size)
            half_copy(b, k).start()
            if k >= 2:
                combine(b, k - 2)
        combine(b, count - 1)

    def chip_sum(b, at):
        size = blocks[b][2]
        mine_here = stage[b % DEPTH, at, core, :, :size].astype(jnp.float32)
        return mine_here + stage_partner[b, at, :, :size].astype(jnp.float32)

    def combine(b, k):
        half_copy(b, k).wait_recv()
        if b >= DEPTH:
            last_copy(b - DEPTH, k).wait_send()
        both = chip_sum(b, order_bands[k]).astype(jnp.bfloat16)
        stage_cross[b % DEPTH * count + k, :, : blocks[b][2]] = both
        last_copy(b, k).start()

    def close(b):
        which, start, size = blocks[b]
        half_copy(b, count).wait_recv()
        total = chip_sum(b, odd * chips + chip)
        for k in range(count):
            last_copy(b, k).wait_recv()
            total = total + stage_got[b * count + k, :, :size].astype(jnp.float32)
        if direct:
            lanes = pl.ds(pl.multiple_of(origins[which] * columns + start, 128), size)
            outs[0][:, lanes] = (mid[:, lanes].astype(jnp.float32) + total).astype(jnp.bfloat16)
        else:
            outs[1][origins[which]] = total

    for b, (which, start, _) in enumerate(blocks):
        hop = which // 2
        if hop:
            piece = which % 2
            if piece and 2 in line.pieces(1, hop):
                piece = 3 if start else 2
            line.arrive(0, 1, hop, piece)
            line.arrive(1, 1, hop, piece)
        multiply(b)
        line.pump({0: 15, 1: 16, 3: 17}.get(b * 8 // n_sp, 0))
        if b * 8 // n_sp == 4:
            held = line.issued[0]
            line.pump(18, also=core == 0)
        if b >= 3:
            close(b - 3)
    line.issued = [held, held]
    line.pump(18, also=core == 1)
    for b in range(len(blocks) - 3, len(blocks)):
        close(b)
    if not direct:
        outs[0][...] = mid[...]

    line.finish()
    pair_copy().wait_send()
    for k in range(1, pairs):

        @pl.when(pair_place + k < pairs - 1)
        def _():
            to_later(k).wait_send()

    if pairs > 1:

        @pl.when(pair_place == pairs - 2)
        def _():
            to_later(1, 2).wait_send()

    for slot in range(chips * units):
        terms_copy(slot).wait_send()
    for u in range(units):
        for j in range(chips - 1):
            cross_copy(j, u).wait_send()
        for k in range(count):
            rows_copy(k, u, mine).wait_send()
        for k in range(count + 1):
            passed_copy(k, u, mine).wait_send()
    for b in range(len(blocks) - DEPTH, len(blocks)):
        for k in range(count + 1):
            half_copy(b, k).wait_send()
        for k in range(count):
            last_copy(b, k).wait_send()


def per_device(
    residual,
    first_group_queries,
    first_group_keys,
    second_group_queries,
    second_group_keys,
    primary_retain_switch_inputs,
    secondary_retain_switch_inputs,
    timestep_fading_exponent,
    values,
    output_gate_logits,
    head_norm_gains,
    output_projection,
    feedforward_norm_gain,
    gate_projection,
    up_projection,
    down_projection,
):
    n_sp, n_tp = lax.axis_size("sp"), lax.axis_size("tp")
    rows, own_rows = first_group_queries.shape[0], residual.shape[0]
    features = residual.shape[1]
    chunks, units, chips = rows // CHUNK, own_rows // CHUNK, n_tp // 2
    width_a, width_b = first_group_keys.shape[1], second_group_keys.shape[1]
    width = width_a + width_b
    inner, ff = gate_projection.shape
    columns = down_projection.shape[1]
    pairs, crossings, peers = n_sp // 2, max(chips - 1, 1), 2 * chips - 1
    direct = columns % 128 == 0
    blocks = n_sp + 1 if columns % 256 == 0 else n_sp
    projection = output_projection.reshape(-1, features)
    in_hbm = [
        residual,
        first_group_queries,
        second_group_queries,
        first_group_keys,
        second_group_keys,
        primary_retain_switch_inputs,
        secondary_retain_switch_inputs,
        values,
        output_gate_logits,
        projection,
        gate_projection,
        up_projection,
        down_projection,
        timestep_fading_exponent.reshape(chunks, 1, CHUNK),
        head_norm_gains,
        feedforward_norm_gain.reshape(1, features),
    ]

    def bf16(*shape):
        return pltpu.VMEM(shape, jnp.bfloat16)

    def f32(*shape):
        return pltpu.VMEM(shape, jnp.float32)

    def sems(*shape):
        return pltpu.SemaphoreType.DMA(shape)

    scratch = [bf16(n_sp * inner, ff // 2)] * 2 + [bf16(n_sp, ff // 2, columns)]
    scratch += [f32(DV, width_a), f32(DV, width_b), f32(8, width)]
    scratch += [bf16(3, DV + PAD, width), bf16(DV + PAD, width), bf16(max(n_sp // 2 - 1, 1), DV + PAD, width)]
    scratch += [bf16(chips * units, CHUNK, features)] * 2
    scratch += [bf16(crossings * units, CHUNK, features)] * 2
    scratch += [bf16(2 * rows, features), bf16(2 * rows, ff // 2)]
    scratch += [bf16(DEPTH, 2 * chips, 2, own_rows, columns), bf16(blocks, 2 * chips, own_rows, columns)]
    scratch += [bf16(DEPTH * peers, own_rows, columns), bf16(blocks * peers, own_rows, columns)]
    scratch += [bf16(own_rows, features)]
    scratch += [sems(len(in_hbm)), sems(3), sems(3)]
    scratch += [sems(2, QUEUE), sems(2, max(6 * pairs - 5, 1))]
    scratch += [sems(2), sems(max(n_sp // 2 - 1, 1)), sems(max(n_sp // 2 - 1, 1))]
    scratch += [sems(chips * units)] * 2
    scratch += [sems(crossings * units)] * 2
    scratch += [sems(peers * units)] * 2
    scratch += [sems((peers + 1) * units)] * 2
    scratch += [sems(DEPTH * (peers + 1)), sems((DEPTH + 1) * (peers + 1))]
    scratch += [sems(DEPTH * peers), sems(blocks * peers)]
    outs = [bf16(own_rows, features)] if direct else [bf16(own_rows, features), f32(n_sp, own_rows, columns)]
    outs = pl.pallas_call(
        functools.partial(layer_kernel, n_sp, n_tp, len(in_hbm), len(outs)),
        in_specs=[pl.BlockSpec(memory_space=pl.ANY)] * len(in_hbm),
        out_specs=[pl.BlockSpec(memory_space=pltpu.VMEM)] * len(outs),
        out_shape=outs,
        scratch_shapes=scratch,
        compiler_params=pltpu.CompilerParams(
            collective_id=0, has_side_effects=True, vmem_limit_bytes=VMEM_BYTES
        ),
        name="layer",
    )(*in_hbm)
    if direct:
        return outs[0]
    added = outs[1].transpose(1, 0, 2).reshape(own_rows, features)
    return (outs[0].astype(jnp.float32) + added).astype(jnp.bfloat16)


def solution(mesh):
    return jax.shard_map(
        per_device,
        mesh=mesh,
        in_specs=(
            P(("sp", "tp"), None),
            P("sp", "tp"),
            P("sp", "tp"),
            P("sp", "tp"),
            P("sp", "tp"),
            P("sp", "tp"),
            P("sp", "tp"),
            P("sp"),
            P(None, "sp", "tp"),
            P(None, "sp", "tp"),
            P(None, "tp"),
            P(None, "tp", None),
            P(),
            P("sp", "tp"),
            P("sp", "tp"),
            P("tp", "sp"),
        ),
        out_specs=P(("sp", "tp"), None),
        check_vma=False,
    )
```
